128 devices in a mesh: ep: 128 (over z, y, x, core).
Axes of the slice: x: 4, y: 4, z: 4, core: 2. Of those that a mesh axis runs over, the one named last changes fastest.
Arguments:
- tokens: bfloat16 [2048, 2048], P('ep'), may hold values from -6 to 6
- recurrent_state: float32 [2048, 16, 4096], P('ep'), may hold values from -8 to 8
- first_gain: float32 [2048], replicated, may hold values from 0.1 to 1.9
- w_receptance: bfloat16 [2048, 1024], P('ep'), may hold values from -0.125 to 0.125
- w_key: bfloat16 [2048, 1024], P('ep'), may hold values from -0.125 to 0.125
- w_value: bfloat16 [2048, 1024], P('ep'), may hold values from -0.125 to 0.125
- decay_down: bfloat16 [2048, 64], replicated, may hold values from -0.125 to 0.125
- decay_up: bfloat16 [64, 1024], replicated, may hold values from -0.75 to 0.75
- decay_base: float32 [1024], replicated, may hold values from -4 to 1
- rate_down: bfloat16 [2048, 64], replicated, may hold values from -0.125 to 0.125
- rate_up: bfloat16 [64, 1024], replicated, may hold values from -0.75 to 0.75
- rate_base: float32 [1024], replicated, may hold values from -5 to 5
- key_scale: float32 [1024], replicated, may hold values from 0.25 to 4
- head_gain: float32 [1024], replicated, may hold values from 0.1 to 1.9
- w_output: bfloat16 [1024, 2048], replicated, may hold values from -0.1875 to 0.1875
- second_gain: float32 [2048], replicated, may hold values from 0.1 to 1.9
- shared_gate: bfloat16 [2048, 512], replicated, may hold values from -0.125 to 0.125
- shared_up: bfloat16 [2048, 512], replicated, may hold values from -0.125 to 0.125
- shared_down: bfloat16 [512, 2048], replicated, may hold values from -0.25 to 0.25
- expert_gate: bfloat16 [128, 2048, 512], P('ep'), may hold values from -0.125 to 0.125
- expert_up: bfloat16 [128, 2048, 512], P('ep'), may hold values from -0.125 to 0.125
- expert_down: bfloat16 [128, 512, 2048], P('ep'), may hold values from -0.25 to 0.25
- routes: int32 [2048, 4], replicated, may hold values from 0 to 127, all different within a row; in each aligned block of 16 rows (0 to 15, 16 to 31, ...) at most 4 rows name the same one
- route_weights: float32 [2048, 4], replicated, may hold values from 0.1 to 1
Outputs:
- new_tokens: bfloat16 [2048, 2048], P('ep')
- new_state: float32 [2048, 16, 4096], P('ep')
The draws below stay inside these ranges and needn't reach their ends.
Inputs may be any that keep to these rules, and one draw needn't show every extreme that they name: `routes`: each row names 4 different experts. In the rows of one device no expert is named by more than 4 rows, a bound that some block reaches of them.
All inputs are finite; a program needn't handle non-finite values.
Results may differ from the reference program's by a relative error of at most 0.015.
Values may be sent and summed in bfloat16 or wider, within the bound.
A program may use at most 128 MiB of HBM per device.

```python
import math
import jax
import jax.numpy as jnp
import numpy as np
from jax import lax

D = 2048
HEADS = 16
HEAD = 64
DECAY_RANK = 64
RATE_RANK = 64
EXPERT_W = 512
SHARED_W = 512
TOPK = 4
MOST = 4
SEQ_DEV = 16
MIX = 1024
STATE = 4096
EXPERTS = 128
TOKENS = 2048
N_EP = 128


def block_levels(key, dims, split, least, largest):
    def one(position, blocks):
        heights = jax.random.uniform(jax.random.fold_in(jax.random.fold_in(key, 6), position), (blocks,), jnp.float32, least / len(split), largest / len(split))
        return jnp.repeat(jnp.exp(heights), dims[position] // blocks).reshape((-1,) + (1,) * (len(dims) - position - 1))

    level = one(*split[0])
    for cut in split[1:]:
        level = level * one(*cut)
    return level


def assign_block(rng, own, number, rows, count, top, most, skew):
    sequence = jax.random.permutation(rng, count)
    heavy_load, common = load_shares(count, rows * top, most, skew, True), load_shares(count, rows * top, most, skew, False)
    places = jnp.arange(count)

    def named(sizes, rotation):
        used = int((sizes > 0).sum())
        fixed = max(1, used // 4)
        shifted = fixed + (places - fixed + rotation * (used - fixed)) % max(1, count - fixed)
        return jnp.zeros((count,), jnp.int32).at[sequence[jnp.where(places < fixed, places, shifted)]].set(jnp.asarray(sizes, jnp.int32))

    sizes = jnp.where(number % 4 == 0, named(heavy_load, number // 4), named(common, number - number // 4 - 1))
    mixed = jax.random.permutation(jax.random.fold_in(own, 3), count)
    donor, sink = mixed[0:count // 2 * 2:2], mixed[1:count // 2 * 2:2]
    slack = jnp.minimum(sizes[donor] - 1, most - sizes[sink]) // 2
    slack = jnp.where((donor == sequence[0]) | (sink == sequence[0]) | (sizes[sink] == 0), 0, jnp.maximum(slack, 0))
    shifted = jax.random.randint(jax.random.fold_in(own, 4), (count // 2,), 0, 1 << 20) % (slack + 1)
    sizes = sizes.at[donor].add(-shifted).at[sink].add(shifted)
    labels = jnp.searchsorted(jnp.cumsum(sizes), jnp.arange(rows * top), side="right").astype(jnp.int32)
    listing = labels.reshape(top, rows).T
    listing = listing[jax.random.permutation(jax.random.fold_in(own, 1), rows)]
    rotation = jax.random.randint(jax.random.fold_in(own, 2), (rows, 1), 0, top)
    return jnp.take_along_axis(listing, (jnp.arange(top)[None, :] + rotation) % top, axis=1)


def load_shares(amount, total, bound, skew, full):
    loads = [(1 << 20) // math.isqrt(rank ** skew) + 1 for rank in range(1, amount + 1)]
    largest = bound if full else min(bound, max(-(-total // amount), total * loads[0] // sum(loads)))
    least = 1 if total - largest >= amount - 1 else 0
    given, surplus = [largest] + [least] * (amount - 1), total - largest - least * (amount - 1)
    while surplus > 0:
        candidates = [i for i in range(1, amount) if given[i] < largest] or [i for i in range(1, amount) if given[i] < bound]
        pool, left = sum([loads[i] for i in candidates]), surplus
        for i in candidates:
            addition = min(bound - given[i], max(1, left * loads[i] // pool), surplus)
            given[i] = given[i] + addition
            surplus = surplus - addition
    return np.array(given)


def bell_draw(own_key, dims, scale, most, split=(), kind=jnp.bfloat16):
    factor_of = block_levels(own_key, dims, split, -0.22, 0.18) if split else 1.0
    values = jax.random.normal(own_key, dims, jnp.float32) * scale * factor_of
    return jnp.minimum(jnp.maximum(values, -most), most).astype(kind)


def setup_inputs(seed: int = 0) -> dict:
    arg_keys = jax.random.split(jax.random.key(seed), 25)
    tokens = bell_draw(arg_keys[0], (TOKENS, D), 1.0, 6.0, ((0, 128),))
    recurrent_state = bell_draw(arg_keys[1], (TOKENS, HEADS, STATE), 2.0, 8.0, ((0, 128),), jnp.float32)
    first_gain = jnp.clip(1.0 + 0.18 * jax.random.normal(arg_keys[2], (D,), jnp.float32), 0.1, 1.9)
    w_receptance = bell_draw(arg_keys[3], (D, MIX), D ** -0.5, 0.125, ((0, 128),))
    w_key = bell_draw(arg_keys[4], (D, MIX), D ** -0.5, 0.125, ((0, 128),))
    w_value = bell_draw(arg_keys[5], (D, MIX), D ** -0.5, 0.125, ((0, 128),))
    decay_down = bell_draw(arg_keys[6], (D, DECAY_RANK), D ** -0.5, 0.125)
    decay_up = bell_draw(arg_keys[7], (DECAY_RANK, MIX), DECAY_RANK ** -0.5, 0.75)
    decay_base = jnp.clip(jax.random.uniform(arg_keys[8], (MIX,), jnp.float32, -4.0, 1.0), -4.0, 1.0)
    rate_down = bell_draw(arg_keys[9], (D, RATE_RANK), D ** -0.5, 0.125)
    rate_up = bell_draw(arg_keys[10], (RATE_RANK, MIX), RATE_RANK ** -0.5, 0.75)
    rate_base = bell_draw(arg_keys[11], (MIX,), 2.0, 5.0, (), jnp.float32)
    key_scale = jnp.clip(jnp.exp(jax.random.uniform(arg_keys[12], (MIX,), jnp.float32, math.log(0.25), math.log(4.0))), 0.25, 4.0)
    head_gain = jnp.clip(1.0 + 0.18 * jax.random.normal(arg_keys[13], (MIX,), jnp.float32), 0.1, 1.9)
    w_output = bell_draw(arg_keys[14], (MIX, D), MIX ** -0.5, 0.1875)
    second_gain = jnp.clip(1.0 + 0.18 * jax.random.normal(arg_keys[15], (D,), jnp.float32), 0.1, 1.9)
    shared_gate = bell_draw(arg_keys[16], (D, SHARED_W), D ** -0.5, 0.125)
    shared_up = bell_draw(arg_keys[17], (D, SHARED_W), D ** -0.5, 0.125)
    shared_down = bell_draw(arg_keys[18], (SHARED_W, D), SHARED_W ** -0.5, 0.25)
    expert_gate = bell_draw(arg_keys[19], (EXPERTS, D, EXPERT_W), D ** -0.5, 0.125, ((0, 128),))
    expert_up = bell_draw(arg_keys[20], (EXPERTS, D, EXPERT_W), D ** -0.5, 0.125, ((0, 128),))
    expert_down = bell_draw(arg_keys[21], (EXPERTS, EXPERT_W, D), EXPERT_W ** -0.5, 0.25, ((0, 128),))
    routes_keys = jax.random.split(jax.random.fold_in(arg_keys[22], 1), TOKENS // SEQ_DEV)
    routes_turns = jax.random.permutation(jax.random.fold_in(arg_keys[22], 3), TOKENS // SEQ_DEV)
    routes = jax.vmap(lambda own, number: assign_block(jax.random.fold_in(arg_keys[22], 2), own, number, SEQ_DEV, EXPERTS, TOPK, MOST, 2))(routes_keys, routes_turns).reshape((TOKENS, TOPK))
    route_weights = jnp.clip(jax.random.uniform(arg_keys[23], (TOKENS, TOPK), jnp.float32, 0.1, 1.0), 0.1, 1.0)
    return {"tokens": tokens, "recurrent_state": recurrent_state, "first_gain": first_gain, "w_receptance": w_receptance, "w_key": w_key, "w_value": w_value, "decay_down": decay_down, "decay_up": decay_up, "decay_base": decay_base, "rate_down": rate_down, "rate_up": rate_up, "rate_base": rate_base, "key_scale": key_scale, "head_gain": head_gain, "w_output": w_output, "second_gain": second_gain, "shared_gate": shared_gate, "shared_up": shared_up, "shared_down": shared_down, "expert_gate": expert_gate, "expert_up": expert_up, "expert_down": expert_down, "routes": routes, "route_weights": route_weights}


NORM_EPS = 1e-06
GROUP_EPS = 0.00064

def rms_scale(inputs, gain):
    widened = inputs.astype(jnp.float32)
    return widened * lax.rsqrt(lax.optimization_barrier(jnp.mean(widened * widened, axis=-1, keepdims=True)) + NORM_EPS) * gain

def gated_units(inputs, gate_weight, up_weight):
    gate_part = jnp.dot(inputs, gate_weight, preferred_element_type=jnp.float32)
    up_part = jnp.dot(inputs, up_weight, preferred_element_type=jnp.float32)
    return (jax.nn.silu(gate_part) * up_part).astype(jnp.bfloat16)

def mix_heads(normed, receptance, key_rows, value_rows, state_old, decay_down, decay_up, decay_base, rate_down, rate_up, rate_base, key_scale, head_gain):
    count_rows = normed.shape[0]
    heads_count = state_old.shape[1]
    decay_low = jnp.tanh(jnp.dot(normed, decay_down, preferred_element_type=jnp.float32)).astype(jnp.bfloat16)
    decay_pre = decay_base + jnp.dot(decay_low, decay_up, preferred_element_type=jnp.float32)
    decay_rate = jnp.exp(-jnp.exp(-jax.nn.softplus(-decay_pre) - 0.5))
    rate_low = jnp.dot(normed, rate_down, preferred_element_type=jnp.float32).astype(jnp.bfloat16)
    learn_rate = jax.nn.sigmoid(rate_base + jnp.dot(rate_low, rate_up, preferred_element_type=jnp.float32))

    def by_head(inputs):
        return inputs.astype(jnp.float32).reshape(count_rows, heads_count, HEAD)
    reader = by_head(receptance)
    key_heads = by_head(key_rows)
    value_heads = by_head(value_rows)
    decay_heads = by_head(decay_rate)
    learn_heads = by_head(learn_rate)
    scaled = key_heads * key_scale.reshape(heads_count, HEAD)
    direction = scaled / jnp.sqrt(lax.optimization_barrier(jnp.sum(scaled * scaled, axis=-1, keepdims=True)) + 1.0)
    state_prev = state_old.reshape(count_rows, heads_count, HEAD, HEAD)
    removed = lax.optimization_barrier(jnp.sum(state_prev * direction[:, :, None, :], axis=-1))
    state_next = state_prev * decay_heads[:, :, None, :] - removed[..., None] * (direction * learn_heads)[:, :, None, :] + value_heads[..., None] * key_heads[:, :, None, :]
    readout = lax.optimization_barrier(jnp.sum(state_next * reader[:, :, None, :], axis=-1))
    centre = lax.optimization_barrier(jnp.mean(readout, axis=-1, keepdims=True))
    spread = lax.optimization_barrier(jnp.mean(jnp.square(readout - centre), axis=-1, keepdims=True))
    normalized = ((readout - centre) * lax.rsqrt(spread + GROUP_EPS)).reshape(count_rows, heads_count * HEAD)
    normalized = normalized * head_gain
    return (normalized.astype(jnp.bfloat16), state_next.reshape(count_rows, heads_count, HEAD * HEAD))

def routed_mix(second, routes, route_weights, expert_gate, expert_up, expert_down):
    span_rows = 64
    count_rows = second.shape[0]
    width = second.shape[1]
    experts_all = expert_gate.shape[0]
    flat_expert = routes.reshape(-1).astype(jnp.int32)
    assigned = flat_expert.shape[0]
    flat_token = jnp.arange(assigned, dtype=jnp.int32) // TOPK
    flat_weight = route_weights.reshape(-1)
    ordering = jnp.argsort(flat_expert, stable=True)
    sorted_expert = flat_expert[ordering]
    counts = lax.optimization_barrier(jnp.sum((flat_expert[None, :] == jnp.arange(experts_all, dtype=jnp.int32)[:, None]).astype(jnp.int32), axis=1)).astype(jnp.int32)
    padded = (counts + span_rows - 1) // span_rows * span_rows
    start_sorted = (jnp.cumsum(counts) - counts).astype(jnp.int32)
    end_padded = jnp.cumsum(padded).astype(jnp.int32)
    start_padded = (end_padded - padded).astype(jnp.int32)
    target = (start_padded[sorted_expert] + (jnp.arange(assigned, dtype=jnp.int32) - start_sorted[sorted_expert])).astype(jnp.int32)
    total_rows = (assigned + experts_all * (span_rows - 1) + span_rows - 1) // span_rows * span_rows
    total_spans = total_rows // span_rows
    row_token = jnp.full((total_rows,), count_rows, jnp.int32).at[target].set(flat_token[ordering])
    row_weight = jnp.zeros((total_rows,), jnp.float32).at[target].set(flat_weight[ordering])
    span_expert = jnp.minimum(jnp.searchsorted(end_padded, jnp.arange(total_spans, dtype=jnp.int32) * span_rows, side='right'), experts_all - 1).astype(jnp.int32)
    table = jnp.concatenate([second, jnp.zeros((1, width), second.dtype)], axis=0)

    def one_span(inputs):
        which, token_ids, weights = inputs
        picked = table[token_ids]
        hidden = gated_units(picked, expert_gate[which], expert_up[which])
        result = jnp.dot(hidden, expert_down[which], preferred_element_type=jnp.float32).astype(jnp.bfloat16)
        return result.astype(jnp.float32) * weights[:, None]
    span_out = lax.map(one_span, (span_expert, row_token.reshape(total_spans, span_rows), row_weight.reshape(total_spans, span_rows)))
    summed = jnp.zeros((count_rows + 1, width), jnp.float32).at[row_token].add(span_out.reshape(total_rows, width))
    return summed[:count_rows]

def reference(tokens, recurrent_state, first_gain, w_receptance, w_key, w_value, decay_down, decay_up, decay_base, rate_down, rate_up, rate_base, key_scale, head_gain, w_output, second_gain, shared_gate, shared_up, shared_down, expert_gate, expert_up, expert_down, routes, route_weights):
    normed = rms_scale(tokens, first_gain).astype(jnp.bfloat16)
    receptance = jnp.dot(normed, w_receptance, preferred_element_type=jnp.float32).astype(jnp.bfloat16)
    key_rows = jnp.dot(normed, w_key, preferred_element_type=jnp.float32).astype(jnp.bfloat16)
    value_rows = jnp.dot(normed, w_value, preferred_element_type=jnp.float32).astype(jnp.bfloat16)

    def per_block(group):
        return mix_heads(group[0], group[1], group[2], group[3], group[4], decay_down, decay_up, decay_base, rate_down, rate_up, rate_base, key_scale, head_gain)
    grouped = (normed.reshape(N_EP, SEQ_DEV, D), receptance.reshape(N_EP, SEQ_DEV, MIX), key_rows.reshape(N_EP, SEQ_DEV, MIX), value_rows.reshape(N_EP, SEQ_DEV, MIX), recurrent_state.reshape(N_EP, SEQ_DEV, HEADS, STATE))
    mixed, new_state = lax.map(per_block, grouped)
    mixed = mixed.reshape(TOKENS, MIX)
    new_state = new_state.reshape(TOKENS, HEADS, STATE)
    residual = (tokens.astype(jnp.float32) + jnp.dot(mixed, w_output, preferred_element_type=jnp.float32)).astype(jnp.bfloat16)
    second = rms_scale(residual, second_gain).astype(jnp.bfloat16)
    shared = jnp.dot(gated_units(second, shared_gate, shared_up), shared_down, preferred_element_type=jnp.float32)
    routed = routed_mix(second, routes, route_weights, expert_gate, expert_up, expert_down)
    new_tokens = (residual.astype(jnp.float32) + shared + routed).astype(jnp.bfloat16)
    return (new_tokens, new_state)
```

```python
import functools

import jax
import jax.numpy as jnp
from jax import lax
from jax.experimental import pallas as pl
from jax.experimental.pallas import tpu as pltpu
from jax.sharding import PartitionSpec as P

HEAD = 64
TOPK = 4
MOST = 4
GROUP = 8
NORM_EPS = 1e-06
GROUP_EPS = 0.00064
MESH = pl.DeviceIdType.MESH
F32 = jnp.float32
BF16 = jnp.bfloat16
VMEM_BYTES = 60 * 1024 * 1024


def dot(a, b):
    return jnp.dot(a, b, preferred_element_type=F32)


def rms_scale(inputs, gain):
    widened = inputs.astype(F32)
    return (
        widened * lax.rsqrt(jnp.mean(widened * widened, axis=-1, keepdims=True) + NORM_EPS) * gain
    )


def project_kernel(
    devices,
    tokens,
    gain,
    w_r,
    w_k,
    w_v,
    decay_down,
    decay_up,
    decay_base,
    rate_down,
    rate_up,
    rate_base,
    key_scale,
    out,
    stage,
    wbuf,
    nsend,
    xbuf,
    psend,
    precv,
    local_sem,
    wsend_sem,
    wrecv_sem,
    xsend_sem,
    xrecv_sem,
    psend_sem,
    precv_sem,
):
    rows, mix = w_r.shape
    half = mix // 2
    count = tokens.shape[0]
    groups = devices // GROUP
    members = 2 * groups
    depth = tokens.shape[1] // groups
    me = lax.axis_index("ep")
    base = (me // GROUP) * GROUP
    place = me % GROUP
    core = me % 2
    column = place // 2
    member = (me // GROUP) * 2 + core
    chip = me - core
    x_bit = (place // 2) % 2
    y_bit = place // 4
    x_chip = chip + 2 - 4 * x_bit
    y_chip = chip + 4 - 8 * y_bit
    diag_chip = x_chip + 4 - 8 * y_bit
    partner = chip + 1 - core

    def peer_of(offset):
        which = (member + offset) % members
        return which, (which // 2) * GROUP + column * 2 + which % 2

    local = []
    weights = (w_r, w_k, w_v)
    for number, weight in enumerate(weights):
        for side in range(2):
            local.append(
                pltpu.make_async_copy(
                    weight.at[:, pl.ds(side * half, half)],
                    stage.at[number, side],
                    local_sem.at[number * 2 + side],
                )
            )
    for copy in local:
        copy.start()

    barrier = pltpu.get_barrier_semaphore()
    greet = [partner, x_chip, x_chip + 1, y_chip, y_chip + 1]
    greet = greet + [peer_of(offset)[1] for offset in range(1, members)]
    for peer in greet:
        pl.semaphore_signal(barrier, inc=1, device_id=(peer,), device_id_type=MESH)

    normed = rms_scale(tokens[...], gain[...]).astype(BF16)
    for number in range(groups):
        nsend[number] = normed[:, number * depth : (number + 1) * depth]
    for copy in local:
        copy.wait()
    pl.semaphore_wait(barrier, len(greet))

    def slot(number, device):
        return wbuf.at[number, pl.ds(pl.multiple_of((device - base) * rows, rows), rows), :]

    def weight_copy(number, source, landing, send, receive, target):
        return pltpu.make_async_remote_copy(
            src_ref=source,
            dst_ref=slot(number, landing),
            send_sem=wsend_sem.at[number * 7 + send],
            recv_sem=wrecv_sem.at[number * 7 + receive],
            device_id=(target,),
            device_id_type=MESH,
        )

    sends = []

    def launch(copy):
        copy.start()
        sends.append(copy)

    def direct(number):
        for side in range(2):
            source = stage.at[number, side]
            launch(weight_copy(number, source, me, 1 + side, 1 + core, x_chip + side))
            launch(weight_copy(number, source, me, 3 + side, 3 + core, y_chip + side))
        launch(weight_copy(number, stage.at[number, 1 - core], me, 0, 0, partner))

    def arrived(number, source, receive):
        weight_copy(number, stage.at[0, 0], source, 0, receive, partner).wait_recv()

    def relay(number):
        arrived(number, y_chip, 3)
        launch(weight_copy(number, slot(number, y_chip), y_chip, 5, 5, x_chip + core))
        arrived(number, x_chip + 1, 2)
        launch(weight_copy(number, slot(number, x_chip + 1), x_chip + 1, 6, 6, y_chip + core))

    direct(0)
    for offset in range(1, members):
        which, device = peer_of(offset)
        launch(
            pltpu.make_async_remote_copy(
                src_ref=nsend.at[which // 2],
                dst_ref=xbuf.at[member],
                send_sem=xsend_sem.at[offset],
                recv_sem=xrecv_sem.at[offset],
                device_id=(device,),
                device_id_type=MESH,
            )
        )
    direct(1)

    for number in range(3):
        own = stage[number, core]
        wbuf[number, pl.ds(pl.multiple_of(place * rows, rows), rows), :] = own
    xbuf[member] = nsend[me // GROUP]
    relay(0)
    direct(2)

    def put(number, values, first):
        for head in range(values.shape[1] // HEAD):
            out[number, :, first + head, :] = values[:, head * HEAD : (head + 1) * HEAD]

    heads = mix // HEAD
    flip = (((1,), (1,)), ((), ()))

    def down(matrix):
        return lax.dot_general(normed, matrix, flip, preferred_element_type=F32)

    decay_low = jnp.tanh(down(decay_down[...])).astype(BF16)
    decay_pre = decay_base[...] + dot(decay_low, decay_up[...])
    put(3, jnp.exp(-jnp.exp(-jax.nn.softplus(-decay_pre) - 0.5)), 0)
    rate_low = down(rate_down[...]).astype(BF16)
    put(4, jax.nn.sigmoid(rate_base[...] + dot(rate_low, rate_up[...])), 0)

    for offset in range(1, members):
        source = (member + members - offset) % members
        pltpu.make_async_remote_copy(
            src_ref=nsend.at[0],
            dst_ref=xbuf.at[source],
            send_sem=xsend_sem.at[offset],
            recv_sem=xrecv_sem.at[offset],
            device_id=(partner,),
            device_id_type=MESH,
        ).wait_recv()
    stacked = xbuf[...].reshape(members * count, depth)

    def part_copy(number, source, landing, offset, target):
        return pltpu.make_async_remote_copy(
            src_ref=psend.at[number, source],
            dst_ref=precv.at[number, landing],
            send_sem=psend_sem.at[number * members + offset],
            recv_sem=precv_sem.at[number * members + offset],
            device_id=(target,),
            device_id_type=MESH,
        )

    def multiply(number):
        arrived(number, partner, 0)
        arrived(number, x_chip, 1)
        arrived(number, y_chip + 1, 4)
        arrived(number, diag_chip, 5)
        arrived(number, diag_chip + 1, 6)
        part = dot(stacked, wbuf[number]).astype(BF16)
        psend[number] = part.reshape(members, count, half)
        for offset in range(1, members):
            which, device = peer_of(offset)
            launch(part_copy(number, which, member, offset, device))
        precv[number, member] = psend[number, member]

    def finish(number):
        for offset in range(1, members):
            source = (member + members - offset) % members
            part_copy(number, 0, source, offset, partner).wait_recv()
        for side in range(2):
            total = precv[number, side].astype(F32)
            for which in range(1, groups):
                total = total + precv[number, which * 2 + side].astype(F32)
            total = total.astype(BF16).astype(F32)
            put(number, total, side * (heads // 2))
            if number == 1:
                scale = key_scale[:, side * half : (side + 1) * half]
                put(5, total * scale, side * (heads // 2))

    relay(1)
    multiply(0)
    relay(2)
    multiply(1)
    finish(0)
    multiply(2)
    finish(1)
    finish(2)
    for copy in sends:
        copy.wait_send()


def project(devices, tokens, gain, w_r, w_k, w_v, dd, du, db, rd, ru, rb, scale):
    count, width = tokens.shape
    rows, mix = w_r.shape
    groups = devices // GROUP
    members = 2 * groups
    half = mix // 2
    vmem = pl.BlockSpec(memory_space=pltpu.VMEM)
    hbm = pl.BlockSpec(memory_space=pl.ANY)
    dma = pltpu.SemaphoreType.DMA
    return pl.pallas_call(
        functools.partial(project_kernel, devices),
        out_shape=jax.ShapeDtypeStruct((6, count, mix // HEAD, HEAD), F32),
        in_specs=[vmem, vmem, hbm, hbm, hbm] + [vmem] * 7,
        out_specs=vmem,
        scratch_shapes=[
            pltpu.VMEM((3, 2, rows, half), BF16),
            pltpu.VMEM((3, GROUP * rows, half), BF16),
            pltpu.VMEM((groups, count, width // groups), BF16),
            pltpu.VMEM((members, count, width // groups), BF16),
            pltpu.VMEM((3, members, count, half), BF16),
            pltpu.VMEM((3, members, count, half), BF16),
            dma((6,)),
            dma((21,)),
            dma((21,)),
            dma((members,)),
            dma((members,)),
            dma((3 * members,)),
            dma((3 * members,)),
        ],
        compiler_params=pltpu.CompilerParams(
            collective_id=0, has_side_effects=True, vmem_limit_bytes=VMEM_BYTES
        ),
        name="project",
    )(tokens, gain, w_r, w_k, w_v, dd, du, db, rd, ru, rb, scale)


def split_sum(values, ones):
    high = values.astype(BF16)
    low = (values - high.astype(F32)).astype(BF16)
    return dot(high, ones) + dot(low, ones)


def mixer_kernel(
    steps,
    vectors,
    state,
    head_gain,
    tokens,
    w_output,
    second_gain,
    new_state,
    residual,
    second,
    wbuf,
    mixed,
    sem,
):
    step = pl.program_id(0)
    _, per_step, heads, _ = vectors.shape
    entries = state.shape[2]
    span = 256
    tiles = entries // span
    copies = span // HEAD
    copy = pltpu.make_async_copy(w_output, wbuf, sem)

    @pl.when(step == 0)
    def _():
        copy.start()

    row = lax.broadcasted_iota(jnp.int32, (span, span), 0)
    col = lax.broadcasted_iota(jnp.int32, (span, span), 1)
    ones = (row // HEAD == col // HEAD).astype(F32).astype(BF16)
    lane = lax.broadcasted_iota(jnp.int32, (heads, span), 1)

    def widen(inputs):
        return jnp.concatenate([inputs] * copies, axis=1)

    for number in range(per_step):
        reader, keys, values, decay, learn, scaled = [vectors[w, number] for w in range(6)]
        direction = scaled / jnp.sqrt(jnp.sum(scaled * scaled, axis=-1, keepdims=True) + 1.0)
        wide_direction = widen(direction)
        wide_decay = widen(decay)
        wide_learn = widen(direction * learn)
        wide_keys = widen(keys)
        wide_reader = widen(reader)
        wide_values = widen(values)
        blocks = [state[number, :, i * span : (i + 1) * span] for i in range(tiles)]
        picks = [(lane % HEAD) == i * copies + lane // HEAD for i in range(tiles)]
        removed = dot(
            jnp.concatenate([(b * wide_direction).astype(BF16) for b in blocks], 0), ones
        )
        spread_values = dot(
            jnp.concatenate([jnp.where(p, wide_values, 0.0) for p in picks], 0).astype(BF16), ones
        )
        later = []
        for i in range(tiles):
            part = slice(i * heads, (i + 1) * heads)
            fresh = (
                blocks[i] * wide_decay
                - removed[part] * wide_learn
                + spread_values[part] * wide_keys
            )
            new_state[number, :, i * span : (i + 1) * span] = fresh
            later.append(fresh * wide_reader)
        read = split_sum(jnp.concatenate(later, 0), ones)
        gathered = jnp.where(picks[0], read[:heads], 0.0)
        for i in range(1, tiles):
            gathered = gathered + jnp.where(picks[i], read[i * heads : (i + 1) * heads], 0.0)
        readout = gathered[:, :HEAD]
        for i in range(1, copies):
            readout = readout + gathered[:, i * HEAD : (i + 1) * HEAD]
        centre = jnp.mean(readout, axis=-1, keepdims=True)
        spread = jnp.mean(jnp.square(readout - centre), axis=-1, keepdims=True)
        mixed[step * per_step + number] = (
            readout - centre
        ) * lax.rsqrt(spread + GROUP_EPS)

    @pl.when(step == steps - 1)
    def _():
        count = mixed.shape[0]
        channels = heads * HEAD
        flat = mixed[...].reshape(count * heads, HEAD)
        source = lax.broadcasted_iota(jnp.int32, (HEAD, channels), 0)
        target = lax.broadcasted_iota(jnp.int32, (HEAD, channels), 1)
        tiled = split_sum(flat, (target % HEAD == source).astype(F32).astype(BF16))
        head = lax.broadcasted_iota(jnp.int32, (count * heads, channels), 0) % heads
        channel = lax.broadcasted_iota(jnp.int32, (count * heads, channels), 1) // HEAD
        kept = (jnp.where(head == channel, tiled, 0.0) * head_gain[...]).astype(BF16)
        owner = lax.broadcasted_iota(jnp.int32, (count, count * heads), 1) // heads
        token = lax.broadcasted_iota(jnp.int32, (count, count * heads), 0)
        rows = dot((owner == token).astype(F32).astype(BF16), kept).astype(BF16)
        copy.wait()
        after = (tokens[...].astype(F32) + dot(rows, wbuf[...])).astype(BF16)
        residual[...] = after
        second[...] = rms_scale(after, second_gain[...]).astype(BF16)


def mixer(vectors, state, head_gain, tokens, w_output, second_gain):
    _, count, heads, _ = vectors.shape
    width = tokens.shape[1]
    entries = state.shape[2]
    per_step = 2 if count % 2 == 0 else 1
    steps = count // per_step
    whole = lambda array: pl.BlockSpec(array.shape, lambda i: (0,) * array.ndim)
    block = pl.BlockSpec((per_step, heads, entries), lambda i: (i, 0, 0))
    flat = pl.BlockSpec((count, width), lambda i: (0, 0))
    return pl.pallas_call(
        functools.partial(mixer_kernel, steps),
        grid=(steps,),
        out_shape=[
            jax.ShapeDtypeStruct(state.shape, F32),
            jax.ShapeDtypeStruct((count, width), BF16),
            jax.ShapeDtypeStruct((count, width), BF16),
        ],
        in_specs=[
            pl.BlockSpec((6, per_step, heads, HEAD), lambda i: (0, i, 0, 0)),
            block,
            whole(head_gain),
            flat,
            pl.BlockSpec(memory_space=pl.ANY),
            whole(second_gain),
        ],
        out_specs=[block, flat, flat],
        scratch_shapes=[
            pltpu.VMEM(w_output.shape, BF16),
            pltpu.VMEM((count, heads, HEAD), F32),
            pltpu.SemaphoreType.DMA,
        ],
        compiler_params=pltpu.CompilerParams(
            dimension_semantics=("arbitrary",), vmem_limit_bytes=VMEM_BYTES
        ),
        name="mixer",
    )(vectors, state, head_gain, tokens, w_output, second_gain)


def onehot(flags):
    return flags.astype(F32).astype(BF16)


def onehot_values(values):
    return values.astype(F32).astype(BF16)


RING = 4
STRIDES = ((2, 8, 32), (8, 32, 2), (32, 2, 8))


def part_widths(width):
    tiles = width // 128
    counts = [tiles // 3 + (1 if number < tiles % 3 else 0) for number in range(3)]
    return [number * 128 for number in counts]


def experts_kernel(
    widths,
    second,
    residual,
    routes,
    route_weights,
    shared_gate,
    shared_up,
    shared_down,
    expert_gate,
    expert_up,
    expert_down,
    out,
    sg,
    su,
    sd,
    eg,
    eu,
    ed,
    *rest,
):
    near, chosen, inbox, answer, back, total, gather, line, final = [
        rest[3 * i : 3 * i + 3] for i in range(9)
    ]
    local_sem = rest[27]
    s1, r1, s2, r2, s3, r3, t3, u3, t2, u2, t1, u1 = rest[28:40]
    count = second.shape[0]
    tokens = routes.shape[1]
    starts = [sum(widths[:p]) for p in range(3)]
    cuts = [slice(starts[p], starts[p] + widths[p]) for p in range(3)]
    blocks = RING * RING
    plane = blocks * count
    note = blocks * MOST
    me = lax.axis_index("ep")
    core = me % 2
    partner = me + 1 - 2 * core

    def place(stride):
        return (me // stride) % RING

    def peer(stride, offset):
        return me + ((place(stride) + offset) % RING - place(stride)) * stride

    spots = [[place(stride) for stride in STRIDES[p]] for p in range(3)]
    barrier = pltpu.get_barrier_semaphore()
    greet = [partner]
    for stride in STRIDES[0]:
        for offset in range(1, RING):
            mate = peer(stride, offset)
            greet = greet + [mate, mate + 1 - 2 * core]
    for mate in greet:
        pl.semaphore_signal(barrier, inc=1, device_id=(mate,), device_id_type=MESH)
    loads = [
        pltpu.make_async_copy(source, target, local_sem.at[number])
        for number, (source, target) in enumerate(
            (
                (shared_gate, sg),
                (shared_up, su),
                (expert_gate.at[0], eg),
                (expert_up.at[0], eu),
                (shared_down, sd),
                (expert_down.at[0], ed),
            )
        )
    ]
    for load in loads:
        load.start()
    pl.semaphore_wait(barrier, len(greet))

    sends = []

    def copy(source, target, send, receive, device):
        return pltpu.make_async_remote_copy(
            src_ref=source,
            dst_ref=target,
            send_sem=send,
            recv_sem=receive,
            device_id=(device,),
            device_id_type=MESH,
        )

    def launch(*args):
        made = copy(*args)
        made.start()
        sends.append(made)

    mine = [second.at[:, pl.ds(starts[p], widths[p])] for p in range(3)]

    def onward(p, step, source):
        a1, a2, _ = spots[p]
        for offset in (1, 3, 2):
            index = p * 16 + offset * 4 + step
            launch(
                source,
                near[p].at[a2, (a1 + RING - step) % RING],
                s2.at[index],
                r2.at[index],
                peer(STRIDES[p][1], offset),
            )

    for p in range(3):
        a1, a2, _ = spots[p]
        for offset in (1, 3, 2):
            launch(
                mine[p],
                near[p].at[a2, a1],
                s1.at[p * 4 + offset],
                r1.at[p * 4 + offset],
                peer(STRIDES[p][0], offset),
            )
    for p in range(3):
        onward(p, 0, mine[p])
    rows = second[...]
    for p in range(3):
        a1, a2, _ = spots[p]
        near[p][a2, a1] = rows[:, cuts[p]]

    def iota(shape, dim):
        return lax.broadcasted_iota(jnp.int32, shape, dim)

    def token_of(p, number):
        first, second_stride, third = STRIDES[p]
        device = (
            spots[p][2] * third
            + core
            + number // (RING * count) * second_stride
            + number // count % RING * first
        )
        return device * count + number % count

    def expert_of(p, number):
        third = STRIDES[p][2]
        return me - spots[p][2] * third - core + number // 2 * third + number % 2

    routes_low = onehot_values(routes[...])
    weights_low = route_weights[...].astype(BF16)
    up_row = iota((plane, plane), 0)
    up_col = iota((plane, plane), 1)
    same = up_row // count == up_col // count
    upper = onehot(same & (up_row < up_col))
    lower = onehot(same & (up_col < up_row))
    slot_row = iota((note, plane), 0)
    slot_col = iota((note, plane), 1)
    wanted = jnp.where(slot_col // count == slot_row // MOST, slot_row % MOST, -2).astype(F32)
    peers = 2 * RING

    def selector(p):
        pick = onehot(iota((tokens, plane), 0) == token_of(p, iota((tokens, plane), 1)))
        here = dot(routes_low, pick)
        names = expert_of(p, iota((peers, plane), 0)).astype(F32)
        named = names < 0.0
        for j in range(TOPK):
            named = named | (here[j : j + 1, :] == names)
        before = dot(onehot(named), upper)
        rank = jnp.where(named, before, -1.0)
        parts = [
            onehot(jnp.broadcast_to(rank[i : i + 1, :], (note, plane)) == wanted)
            for i in range(peers)
        ]
        return jnp.concatenate(parts, 0)

    selectors = [selector(p) for p in range(3)]

    for offset in (1, 3, 2):
        for p in range(3):
            a1, a2, _ = spots[p]
            slot = near[p].at[a2, (a1 + RING - offset) % RING]
            copy(mine[p], slot, s1.at[p * 4 + offset], r1.at[p * 4 + offset], partner).wait_recv()
            onward(p, offset, slot)

    for p in (1, 2, 0):
        a1, a2, a3 = spots[p]
        for offset in (1, 3, 2):
            for step in (0, 1, 3, 2):
                slot = near[p].at[(a2 + RING - offset) % RING, (a1 + RING - step) % RING]
                index = p * 16 + offset * 4 + step
                copy(mine[p], slot, s2.at[index], r2.at[index], partner).wait_recv()
        held = near[p][...].reshape(plane, widths[p])
        picked = dot(selectors[p], held).astype(BF16)
        chosen[p][...] = picked.reshape(peers, note, widths[p])
        for offset in (1, 3, 2):
            chip = peer(STRIDES[p][2], offset) - core
            for side in range(2):
                launch(
                    chosen[p].at[(a3 + offset) % RING * 2 + side],
                    inbox[p].at[core, a3],
                    s3.at[p * 8 + offset * 2 + side],
                    r3.at[p * 8 + offset * 2 + core],
                    chip + side,
                )
        launch(
            chosen[p].at[a3 * 2 + 1 - core],
            inbox[p].at[core, a3],
            s3.at[p * 8],
            r3.at[p * 8 + core],
            partner,
        )
        inbox[p][core, a3] = chosen[p][a3 * 2 + core]

    def gated(gate_part, up_part):
        return (jax.nn.silu(gate_part) * up_part).astype(BF16)

    loads[0].wait()
    loads[1].wait()
    shared_hidden = gated(dot(rows, sg[...]), dot(rows, su[...]))
    loads[4].wait()
    kept = residual[...].astype(F32) + dot(shared_hidden, sd[...])

    turned = (((1,), (1,)), ((), ()))
    tall_row = iota((plane, peers * note), 0)
    tall_col = iota((plane, peers * note), 1)
    expand = onehot(iota((128, peers * note), 0) == iota((128, peers * note), 1) // note)
    wanted_t = jnp.where(
        tall_row // count == tall_col % note // MOST, tall_col % MOST, -2
    ).astype(F32)

    def mixing(p):
        pick = onehot(iota((plane, tokens), 1) == token_of(p, iota((plane, tokens), 0)))
        here = lax.dot_general(pick, routes_low, turned, preferred_element_type=F32)
        weigh = lax.dot_general(pick, weights_low, turned, preferred_element_type=F32)
        number = iota((plane, 128), 1)
        names = jnp.where(number < peers, expert_of(p, number), -1).astype(F32)
        named = names < -2.0
        weight = jnp.zeros((plane, 128), F32)
        for j in range(TOPK):
            hit = here[:, j : j + 1] == names
            named = named | hit
            weight = weight + jnp.where(hit, weigh[:, j : j + 1], 0.0)
        before = dot(lower, onehot(named))
        rank = dot(jnp.where(named, before, -1.0).astype(BF16), expand)
        spread = dot(weight.astype(BF16), expand)
        return jnp.where(rank == wanted_t, spread, 0.0).astype(BF16)

    mixers = [mixing(p) for p in range(3)]

    each = RING * note
    turn_row = iota((each, each), 0)
    turn_col = iota((each, each), 1)

    def digits(number):
        return number // 64, number // 16 % 4, number // 4 % 4, number % 4

    def joined(a, b, c, d):
        return ((a * RING + b) * RING + c) * MOST + d

    def orders(number):
        z, y, x, s = digits(number)
        return [None, joined(x, z, y, s), joined(y, x, z, s)]

    def restored(number):
        first, middle, last, s = digits(number)
        return [None, joined(middle, last, first, s), joined(last, first, middle, s)]

    turns = [None] + [onehot(turn_col == orders(turn_row)[p]) for p in (1, 2)]
    returns = [None] + [onehot(turn_col == restored(turn_row)[p]) for p in (1, 2)]

    gate_part = None
    up_part = None
    loads[2].wait()
    loads[3].wait()
    for p in (1, 2, 0):
        a3 = spots[p][2]
        for offset in (0, 1, 3, 2):
            for side in range(2):
                if offset == 0 and side == 1:
                    continue
                which = side if offset else 1 - core
                slot = inbox[p].at[which, (a3 + RING - offset) % RING]
                index = p * 8 + offset * 2 + which
                copy(chosen[p].at[0], slot, s3.at[index], r3.at[index], partner).wait_recv()
        if p == 0:
            inputs = inbox[p][...].reshape(2 * each, widths[p])
        else:
            inputs = jnp.concatenate(
                [
                    dot(turns[p], inbox[p][side].reshape(each, widths[p])).astype(BF16)
                    for side in range(2)
                ],
                0,
            )
        gate_more = dot(inputs, eg[cuts[p], :])
        up_more = dot(inputs, eu[cuts[p], :])
        gate_part = gate_more if gate_part is None else gate_part + gate_more
        up_part = up_more if up_part is None else up_part + up_more
    hidden = gated(gate_part, up_part)
    loads[5].wait()

    for p in range(3):
        a3 = spots[p][2]
        if p == 0:
            inputs = hidden
        else:
            inputs = jnp.concatenate(
                [
                    dot(returns[p], hidden[side * each : (side + 1) * each]).astype(BF16)
                    for side in range(2)
                ],
                0,
            )
        result = dot(inputs, ed[:, cuts[p]]).astype(BF16)
        answer[p][...] = result.reshape(2, RING, note, widths[p])
        for offset in (1, 3, 2):
            chip = peer(STRIDES[p][2], offset) - core
            for side in range(2):
                launch(
                    answer[p].at[side, (a3 + offset) % RING],
                    back[p].at[a3, core],
                    t3.at[p * 8 + offset * 2 + side],
                    u3.at[p * 8 + offset * 2 + core],
                    chip + side,
                )
        launch(
            answer[p].at[1 - core, a3],
            back[p].at[a3, core],
            t3.at[p * 8],
            u3.at[p * 8 + core],
            partner,
        )
        back[p][a3, core] = answer[p][core, a3]

    for p in (1, 2, 0):
        a1, a2, a3 = spots[p]
        for offset in (0, 1, 3, 2):
            for side in range(2):
                if offset == 0 and side == 1:
                    continue
                which = side if offset else 1 - core
                slot = back[p].at[(a3 + RING - offset) % RING, which]
                index = p * 8 + offset * 2 + which
                copy(chosen[p].at[0], slot, t3.at[index], u3.at[index], partner).wait_recv()
        summed = dot(mixers[p], back[p][...].reshape(peers * note, widths[p])).astype(BF16)
        total[p][...] = summed.reshape(RING, RING, count, widths[p])
        for offset in (1, 3, 2):
            launch(
                total[p].at[(a2 + offset) % RING],
                gather[p].at[offset],
                t2.at[p * 4 + offset],
                u2.at[p * 4 + offset],
                peer(STRIDES[p][1], offset),
            )
    for p in (1, 2, 0):
        a1, a2, a3 = spots[p]
        summed = total[p][a2].astype(F32)
        for offset in (1, 3, 2):
            index = p * 4 + offset
            slot = gather[p].at[offset]
            copy(total[p].at[0], slot, t2.at[index], u2.at[index], partner).wait_recv()
            summed = summed + gather[p][offset].astype(F32)
        line[p][...] = summed.astype(BF16)
        for offset in (1, 3, 2):
            launch(
                line[p].at[(a1 + offset) % RING],
                final[p].at[offset],
                t1.at[p * 4 + offset],
                u1.at[p * 4 + offset],
                peer(STRIDES[p][0], offset),
            )
    for p in (1, 2, 0):
        a1 = spots[p][0]
        summed = line[p][a1].astype(F32)
        for offset in (1, 3, 2):
            index = p * 4 + offset
            slot = final[p].at[offset]
            copy(line[p].at[0], slot, t1.at[index], u1.at[index], partner).wait_recv()
            summed = summed + final[p][offset].astype(F32)
        out[:, cuts[p]] = (kept[:, cuts[p]] + summed).astype(BF16)
    for made in sends:
        made.wait_send()


def experts(second, residual, routes, weights, *matrices):
    count, width = second.shape
    widths = part_widths(width)
    vmem = pl.BlockSpec(memory_space=pltpu.VMEM)
    hbm = pl.BlockSpec(memory_space=pl.ANY)
    dma = pltpu.SemaphoreType.DMA
    blocks = RING * RING
    note = blocks * MOST
    shapes = (
        (RING, RING, count),
        (2 * RING, note),
        (2, RING, note),
        (2, RING, note),
        (RING, 2, note),
        (RING, RING, count),
        (RING, RING, count),
        (RING, count),
        (RING, count),
    )
    shapes = [pltpu.VMEM(shape + (w,), BF16) for shape in shapes for w in widths]
    sizes = (6, 12, 12, 48, 48, 24, 24, 24, 24, 12, 12, 12, 12)
    return pl.pallas_call(
        functools.partial(experts_kernel, widths),
        out_shape=jax.ShapeDtypeStruct((count, width), BF16),
        in_specs=[vmem] * 4 + [hbm] * 6,
        out_specs=vmem,
        scratch_shapes=[pltpu.VMEM(m.shape[-2:], BF16) for m in matrices]
        + shapes
        + [dma((size,)) for size in sizes],
        compiler_params=pltpu.CompilerParams(
            collective_id=1, has_side_effects=True, vmem_limit_bytes=VMEM_BYTES
        ),
        name="experts",
    )(second, residual, routes, weights, *matrices)


def per_device(
    tokens,
    recurrent_state,
    first_gain,
    w_receptance,
    w_key,
    w_value,
    decay_down,
    decay_up,
    decay_base,
    rate_down,
    rate_up,
    rate_base,
    key_scale,
    head_gain,
    w_output,
    second_gain,
    shared_gate,
    shared_up,
    shared_down,
    expert_gate,
    expert_up,
    expert_down,
    routes,
    route_weights,
):
    devices = lax.axis_size("ep")
    vectors = project(
        devices,
        tokens,
        first_gain[None, :],
        w_receptance,
        w_key,
        w_value,
        decay_down.T,
        decay_up,
        decay_base[None, :],
        rate_down.T,
        rate_up,
        rate_base[None, :],
        key_scale[None, :],
    )
    new_state, residual, second = mixer(
        vectors,
        recurrent_state,
        head_gain[None, :],
        tokens,
        w_output,
        second_gain[None, :],
    )
    new_tokens = experts(
        second,
        residual,
        routes.T,
        route_weights.T,
        shared_gate,
        shared_up,
        shared_down,
        expert_gate,
        expert_up,
        expert_down,
    )
    return (new_tokens, new_state)


def solution(mesh):
    in_specs = (
        P("ep", None),
        P("ep", None, None),
        P(),
        P("ep", None),
        P("ep", None),
        P("ep", None),
        P(),
        P(),
        P(),
        P(),
        P(),
        P(),
        P(),
        P(),
        P(),
        P(),
        P(),
        P(),
        P(),
        P("ep", None, None),
        P("ep", None, None),
        P("ep", None, None),
        P(),
        P(),
    )
    out_specs = (P("ep", None), P("ep", None, None))
    return jax.shard_map(
        per_device, mesh=mesh, in_specs=in_specs, out_specs=out_specs, check_vma=False
    )
```

```python
import functools

import jax
import jax.numpy as jnp
from jax import lax
from jax.experimental import pallas as pl
from jax.experimental.pallas import tpu as pltpu
from jax.sharding import PartitionSpec as P

HEAD = 64
TOPK = 4
MOST = 4
RING = 4
STRIDES = ((2, 8, 32), (8, 32, 2), (32, 2, 8))
NORM_EPS = 1e-06
GROUP_EPS = 0.00064
MESH = pl.DeviceIdType.MESH
F32 = jnp.float32
BF16 = jnp.bfloat16
VMEM_BYTES = 60 * 1024 * 1024


def dot(a, b):
    return jnp.dot(a, b, preferred_element_type=F32)


def rms_scale(inputs, gain):
    widened = inputs.astype(F32)
    return (
        widened * lax.rsqrt(jnp.mean(widened * widened, axis=-1, keepdims=True) + NORM_EPS) * gain
    )


def project_kernel(
    tokens,
    gain,
    w_r,
    w_k,
    w_v,
    decay_down,
    decay_up,
    decay_base,
    rate_down,
    rate_up,
    rate_base,
    key_scale,
    out,
    stage,
    wbuf,
    nsend,
    xbuf,
    psend,
    precv,
    local_sem,
    wsend_sem,
    wrecv_sem,
    xsend_sem,
    xrecv_sem,
    psend_sem,
    precv_sem,
):
    rows, mix = w_r.shape
    half = mix // 2
    count, width = tokens.shape
    pair = 2 * rows
    depth = width // RING
    me = lax.axis_index("ep")
    core = me % 2
    partner = me + 1 - 2 * core

    def place(stride):
        return (me // stride) % RING

    def peer(stride, offset):
        return me + ((place(stride) + offset) % RING - place(stride)) * stride

    spots = [[place(stride) for stride in STRIDES[p]] for p in range(3)]
    local = []
    for p, weight in enumerate((w_r, w_k, w_v)):
        for side in range(2):
            local.append(
                pltpu.make_async_copy(
                    weight.at[:, pl.ds(side * half, half)],
                    stage.at[p, side],
                    local_sem.at[p * 2 + side],
                )
            )
    for copy in local:
        copy.start()

    barrier = pltpu.get_barrier_semaphore()
    greet = [partner]
    for stride in STRIDES[0]:
        for offset in range(1, RING):
            mate = peer(stride, offset)
            greet = greet + [mate, mate + 1 - 2 * core]
    for mate in greet:
        pl.semaphore_signal(barrier, inc=1, device_id=(mate,), device_id_type=MESH)

    normed = rms_scale(tokens[...], gain[...]).astype(BF16)
    for q in range(RING):
        nsend[0, q] = normed[:, q * depth : (q + 1) * depth]
        chunks = [z * depth + y * RING * pair + q * pair for z in range(RING) for y in range(RING)]
        nsend[1, q] = jnp.concatenate([normed[:, s : s + pair] for s in chunks], axis=1)
        chunks = [z * depth + q * RING * pair for z in range(RING)]
        nsend[2, q] = jnp.concatenate([normed[:, s : s + RING * pair] for s in chunks], axis=1)
    for copy in local:
        copy.wait()
    pl.semaphore_wait(barrier, len(greet))

    sends = []

    def remote(source, target, send, receive, device):
        return pltpu.make_async_remote_copy(
            src_ref=source,
            dst_ref=target,
            send_sem=send,
            recv_sem=receive,
            device_id=(device,),
            device_id_type=MESH,
        )

    def launch(*args):
        made = remote(*args)
        made.start()
        sends.append(made)

    def chip_slot(p, first, second):
        return wbuf.at[p, first, second] if p == 2 else wbuf.at[p, second, first]

    def row_slot(p, first, second, which):
        return chip_slot(p, first, second).at[which]

    for p in range(3):
        a1, a2, _ = spots[p]
        for offset in (1, 3, 2):
            chip = peer(STRIDES[p][0], offset) - core
            for side in range(2):
                launch(
                    stage.at[p, side],
                    row_slot(p, a1, a2, core),
                    wsend_sem.at[p * 32 + offset * 2 + side],
                    wrecv_sem.at[p * 32 + offset * 2 + core],
                    chip + side,
                )
        launch(
            stage.at[p, 1 - core],
            row_slot(p, a1, a2, core),
            wsend_sem.at[p * 32],
            wrecv_sem.at[p * 32 + core],
            partner,
        )
    for p in range(3):
        a1, a2, _ = spots[p]
        for offset in (1, 3, 2):
            chip = peer(STRIDES[p][1], offset) - core
            for side in range(2):
                launch(
                    stage.at[p, side],
                    row_slot(p, a1, a2, core),
                    wsend_sem.at[p * 32 + 8 + offset * 2 + side],
                    wrecv_sem.at[p * 32 + 8 + offset * 2 + core],
                    chip + side,
                )
    for p in range(3):
        a3 = spots[p][2]
        for offset in (1, 3, 2):
            chip = peer(STRIDES[p][2], offset) - core
            for side in range(2):
                launch(
                    nsend.at[p, (a3 + offset) % RING],
                    xbuf.at[p, a3, core],
                    xsend_sem.at[p * 8 + offset * 2 + side],
                    xrecv_sem.at[p * 8 + offset * 2 + core],
                    chip + side,
                )
        launch(
            nsend.at[p, a3],
            xbuf.at[p, a3, core],
            xsend_sem.at[p * 8],
            xrecv_sem.at[p * 8 + core],
            partner,
        )
    for p in range(3):
        a1, a2, a3 = spots[p]
        own = stage[p, core]
        if p == 2:
            wbuf[p, a1, a2, core] = own
        else:
            wbuf[p, a2, a1, core] = own
        xbuf[p, a3, core] = nsend[p, a3]

    def arrived(p, slot, index):
        remote(stage.at[p, 0], slot, wsend_sem.at[index], wrecv_sem.at[index], partner).wait_recv()

    for step in (1, 3, 2):
        for p in range(3):
            a1, a2, _ = spots[p]
            first = (a1 + RING - step) % RING
            for which in range(2):
                arrived(p, row_slot(p, first, a2, which), p * 32 + step * 2 + which)
            block = chip_slot(p, first, a2)
            for offset in (1, 3, 2):
                index = p * 32 + 16 + offset * 4 + step
                launch(
                    block,
                    block,
                    wsend_sem.at[index],
                    wrecv_sem.at[index],
                    peer(STRIDES[p][1], offset),
                )

    def put(number, values, first):
        for head in range(values.shape[1] // HEAD):
            out[number, :, first + head, :] = values[:, head * HEAD : (head + 1) * HEAD]

    heads = mix // HEAD
    flip = (((1,), (1,)), ((), ()))

    def down(matrix):
        return lax.dot_general(normed, matrix, flip, preferred_element_type=F32)

    decay_low = jnp.tanh(down(decay_down[...])).astype(BF16)
    decay_pre = decay_base[...] + dot(decay_low, decay_up[...])
    put(3, jnp.exp(-jnp.exp(-jax.nn.softplus(-decay_pre) - 0.5)), 0)
    rate_low = down(rate_down[...]).astype(BF16)
    put(4, jax.nn.sigmoid(rate_base[...] + dot(rate_low, rate_up[...])), 0)

    for p in range(3):
        a1, a2, a3 = spots[p]
        arrived(p, row_slot(p, a1, a2, 1 - core), p * 32 + 1 - core)
        for offset in (0, 1, 3, 2):
            for side in range(2):
                if offset == 0 and side == 1:
                    continue
                which = side if offset else 1 - core
                index = p * 8 + offset * 2 + which
                remote(
                    nsend.at[p, 0],
                    xbuf.at[p, (a3 + RING - offset) % RING, which],
                    xsend_sem.at[index],
                    xrecv_sem.at[index],
                    partner,
                ).wait_recv()
        for offset in (1, 3, 2):
            second = (a2 + RING - offset) % RING
            for which in range(2):
                arrived(p, row_slot(p, a1, second, which), p * 32 + 8 + offset * 2 + which)
            for step in (1, 3, 2):
                block = chip_slot(p, (a1 + RING - step) % RING, second)
                index = p * 32 + 16 + offset * 4 + step
                remote(
                    block, block, wsend_sem.at[index], wrecv_sem.at[index], partner
                ).wait_recv()
        stacked = xbuf[p].reshape(2 * RING * count, depth)
        part = dot(stacked, wbuf[p].reshape(depth, half)).astype(BF16)
        psend[p] = part.reshape(RING, 2, count, half)
        for offset in (1, 3, 2):
            chip = peer(STRIDES[p][2], offset) - core
            for side in range(2):
                launch(
                    psend.at[p, (a3 + offset) % RING, side],
                    precv.at[p, a3, core],
                    psend_sem.at[p * 8 + offset * 2 + side],
                    precv_sem.at[p * 8 + offset * 2 + core],
                    chip + side,
                )
        launch(
            psend.at[p, a3, 1 - core],
            precv.at[p, a3, core],
            psend_sem.at[p * 8],
            precv_sem.at[p * 8 + core],
            partner,
        )
        precv[p, a3, core] = psend[p, a3, core]

    for p in range(3):
        a3 = spots[p][2]
        for offset in (0, 1, 3, 2):
            for side in range(2):
                if offset == 0 and side == 1:
                    continue
                which = side if offset else 1 - core
                index = p * 8 + offset * 2 + which
                remote(
                    nsend.at[p, 0],
                    precv.at[p, (a3 + RING - offset) % RING, which],
                    psend_sem.at[index],
                    precv_sem.at[index],
                    partner,
                ).wait_recv()
        for side in range(2):
            total = precv[p, 0, side].astype(F32)
            for which in range(1, RING):
                total = total + precv[p, which, side].astype(F32)
            total = total.astype(BF16).astype(F32)
            put(p, total, side * (heads // 2))
            if p == 1:
                scale = key_scale[:, side * half : (side + 1) * half]
                put(5, total * scale, side * (heads // 2))
    for made in sends:
        made.wait_send()


def project(tokens, gain, w_r, w_k, w_v, dd, du, db, rd, ru, rb, scale):
    count, width = tokens.shape
    rows, mix = w_r.shape
    half = mix // 2
    depth = width // RING
    vmem = pl.BlockSpec(memory_space=pltpu.VMEM)
    hbm = pl.BlockSpec(memory_space=pl.ANY)
    dma = pltpu.SemaphoreType.DMA
    return pl.pallas_call(
        project_kernel,
        out_shape=jax.ShapeDtypeStruct((6, count, mix // HEAD, HEAD), F32),
        in_specs=[vmem, vmem, hbm, hbm, hbm] + [vmem] * 7,
        out_specs=vmem,
        scratch_shapes=[
            pltpu.VMEM((3, 2, rows, half), BF16),
            pltpu.VMEM((3, RING, RING, 2, rows, half), BF16),
            pltpu.VMEM((3, RING, count, depth), BF16),
            pltpu.VMEM((3, RING, 2, count, depth), BF16),
            pltpu.VMEM((3, RING, 2, count, half), BF16),
            pltpu.VMEM((3, RING, 2, count, half), BF16),
            dma((6,)),
            dma((96,)),
            dma((96,)),
            dma((24,)),
            dma((24,)),
            dma((24,)),
            dma((24,)),
        ],
        compiler_params=pltpu.CompilerParams(
            collective_id=0, has_side_effects=True, vmem_limit_bytes=VMEM_BYTES
        ),
        name="project",
    )(tokens, gain, w_r, w_k, w_v, dd, du, db, rd, ru, rb, scale)


def split_sum(values, ones):
    high = values.astype(BF16)
    low = (values - high.astype(F32)).astype(BF16)
    return dot(high, ones) + dot(low, ones)


def mixer_kernel(
    steps,
    vectors,
    state,
    head_gain,
    tokens,
    w_output,
    second_gain,
    new_state,
    residual,
    second,
    wbuf,
    mixed,
    sem,
):
    step = pl.program_id(0)
    _, per_step, heads, _ = vectors.shape
    entries = state.shape[2]
    span = 256
    tiles = entries // span
    copies = span // HEAD
    copy = pltpu.make_async_copy(w_output, wbuf, sem)

    @pl.when(step == 0)
    def _():
        copy.start()

    row = lax.broadcasted_iota(jnp.int32, (span, span), 0)
    col = lax.broadcasted_iota(jnp.int32, (span, span), 1)
    ones = (row // HEAD == col // HEAD).astype(F32).astype(BF16)
    lane = lax.broadcasted_iota(jnp.int32, (heads, span), 1)

    def widen(inputs):
        return jnp.concatenate([inputs] * copies, axis=1)

    for number in range(per_step):
        reader, keys, values, decay, learn, scaled = [vectors[w, number] for w in range(6)]
        direction = scaled / jnp.sqrt(jnp.sum(scaled * scaled, axis=-1, keepdims=True) + 1.0)
        wide_direction = widen(direction)
        wide_decay = widen(decay)
        wide_learn = widen(direction * learn)
        wide_keys = widen(keys)
        wide_reader = widen(reader)
        wide_values = widen(values)
        blocks = [state[number, :, i * span : (i + 1) * span] for i in range(tiles)]
        picks = [(lane % HEAD) == i * copies + lane // HEAD for i in range(tiles)]
        removed = dot(
            jnp.concatenate([(b * wide_direction).astype(BF16) for b in blocks], 0), ones
        )
        spread_values = dot(
            jnp.concatenate([jnp.where(p, wide_values, 0.0) for p in picks], 0).astype(BF16), ones
        )
        later = []
        for i in range(tiles):
            part = slice(i * heads, (i + 1) * heads)
            fresh = (
                blocks[i] * wide_decay
                - removed[part] * wide_learn
                + spread_values[part] * wide_keys
            )
            new_state[number, :, i * span : (i + 1) * span] = fresh
            later.append(fresh * wide_reader)
        read = split_sum(jnp.concatenate(later, 0), ones)
        gathered = jnp.where(picks[0], read[:heads], 0.0)
        for i in range(1, tiles):
            gathered = gathered + jnp.where(picks[i], read[i * heads : (i + 1) * heads], 0.0)
        readout = gathered[:, :HEAD]
        for i in range(1, copies):
            readout = readout + gathered[:, i * HEAD : (i + 1) * HEAD]
        centre = jnp.mean(readout, axis=-1, keepdims=True)
        spread = jnp.mean(jnp.square(readout - centre), axis=-1, keepdims=True)
        mixed[step * per_step + number] = (
            readout - centre
        ) * lax.rsqrt(spread + GROUP_EPS)

    @pl.when(step == steps - 1)
    def _():
        count = mixed.shape[0]
        channels = heads * HEAD
        flat = mixed[...].reshape(count * heads, HEAD)
        source = lax.broadcasted_iota(jnp.int32, (HEAD, channels), 0)
        target = lax.broadcasted_iota(jnp.int32, (HEAD, channels), 1)
        tiled = split_sum(flat, (target % HEAD == source).astype(F32).astype(BF16))
        head = lax.broadcasted_iota(jnp.int32, (count * heads, channels), 0) % heads
        channel = lax.broadcasted_iota(jnp.int32, (count * heads, channels), 1) // HEAD
        kept = (jnp.where(head == channel, tiled, 0.0) * head_gain[...]).astype(BF16)
        owner = lax.broadcasted_iota(jnp.int32, (count, count * heads), 1) // heads
        token = lax.broadcasted_iota(jnp.int32, (count, count * heads), 0)
        rows = dot((owner == token).astype(F32).astype(BF16), kept).astype(BF16)
        copy.wait()
        after = (tokens[...].astype(F32) + dot(rows, wbuf[...])).astype(BF16)
        residual[...] = after
        second[...] = rms_scale(after, second_gain[...]).astype(BF16)


def mixer(vectors, state, head_gain, tokens, w_output, second_gain):
    _, count, heads, _ = vectors.shape
    width = tokens.shape[1]
    entries = state.shape[2]
    per_step = 2 if count % 2 == 0 else 1
    steps = count // per_step
    whole = lambda array: pl.BlockSpec(array.shape, lambda i: (0,) * array.ndim)
    block = pl.BlockSpec((per_step, heads, entries), lambda i: (i, 0, 0))
    flat = pl.BlockSpec((count, width), lambda i: (0, 0))
    return pl.pallas_call(
        functools.partial(mixer_kernel, steps),
        grid=(steps,),
        out_shape=[
            jax.ShapeDtypeStruct(state.shape, F32),
            jax.ShapeDtypeStruct((count, width), BF16),
            jax.ShapeDtypeStruct((count, width), BF16),
        ],
        in_specs=[
            pl.BlockSpec((6, per_step, heads, HEAD), lambda i: (0, i, 0, 0)),
            block,
            whole(head_gain),
            flat,
            pl.BlockSpec(memory_space=pl.ANY),
            whole(second_gain),
        ],
        out_specs=[block, flat, flat],
        scratch_shapes=[
            pltpu.VMEM(w_output.shape, BF16),
            pltpu.VMEM((count, heads, HEAD), F32),
            pltpu.SemaphoreType.DMA,
        ],
        compiler_params=pltpu.CompilerParams(
            dimension_semantics=("arbitrary",), vmem_limit_bytes=VMEM_BYTES
        ),
        name="mixer",
    )(vectors, state, head_gain, tokens, w_output, second_gain)


def onehot(flags):
    return flags.astype(F32).astype(BF16)


def onehot_values(values):
    return values.astype(F32).astype(BF16)


def part_widths(width):
    tiles = width // 128
    counts = [tiles // 3 + (1 if number < tiles % 3 else 0) for number in range(3)]
    return [number * 128 for number in counts]


def experts_kernel(
    widths,
    second,
    residual,
    routes,
    route_weights,
    shared_gate,
    shared_up,
    shared_down,
    expert_gate,
    expert_up,
    expert_down,
    out,
    sg,
    su,
    sd,
    eg,
    eu,
    ed,
    *rest,
):
    near, chosen, inbox, answer, back, total, gather, line, final = [
        rest[3 * i : 3 * i + 3] for i in range(9)
    ]
    local_sem = rest[27]
    s1, r1, s2, r2, s3, r3, t3, u3, t2, u2, t1, u1 = rest[28:40]
    count = second.shape[0]
    tokens = routes.shape[1]
    starts = [sum(widths[:p]) for p in range(3)]
    cuts = [slice(starts[p], starts[p] + widths[p]) for p in range(3)]
    blocks = RING * RING
    plane = blocks * count
    note = blocks * MOST
    me = lax.axis_index("ep")
    core = me % 2
    partner = me + 1 - 2 * core

    def place(stride):
        return (me // stride) % RING

    def peer(stride, offset):
        return me + ((place(stride) + offset) % RING - place(stride)) * stride

    spots = [[place(stride) for stride in STRIDES[p]] for p in range(3)]
    barrier = pltpu.get_barrier_semaphore()
    greet = [partner]
    for stride in STRIDES[0]:
        for offset in range(1, RING):
            mate = peer(stride, offset)
            greet = greet + [mate, mate + 1 - 2 * core]
    for mate in greet:
        pl.semaphore_signal(barrier, inc=1, device_id=(mate,), device_id_type=MESH)
    loads = [
        pltpu.make_async_copy(source, target, local_sem.at[number])
        for number, (source, target) in enumerate(
            (
                (shared_gate, sg),
                (shared_up, su),
                (expert_gate.at[0], eg),
                (expert_up.at[0], eu),
                (shared_down, sd),
                (expert_down.at[0], ed),
            )
        )
    ]
    for load in loads:
        load.start()
    pl.semaphore_wait(barrier, len(greet))

    sends = []

    def copy(source, target, send, receive, device):
        return pltpu.make_async_remote_copy(
            src_ref=source,
            dst_ref=target,
            send_sem=send,
            recv_sem=receive,
            device_id=(device,),
            device_id_type=MESH,
        )

    def launch(*args):
        made = copy(*args)
        made.start()
        sends.append(made)

    mine = [second.at[:, pl.ds(starts[p], widths[p])] for p in range(3)]

    def onward(p, step, source):
        a1, a2, _ = spots[p]
        for offset in (1, 3, 2):
            index = p * 16 + offset * 4 + step
            launch(
                source,
                near[p].at[a2, (a1 + RING - step) % RING],
                s2.at[index],
                r2.at[index],
                peer(STRIDES[p][1], offset),
            )

    for p in range(3):
        a1, a2, _ = spots[p]
        for offset in (1, 3, 2):
            launch(
                mine[p],
                near[p].at[a2, a1],
                s1.at[p * 4 + offset],
                r1.at[p * 4 + offset],
                peer(STRIDES[p][0], offset),
            )
    for p in range(3):
        onward(p, 0, mine[p])
    rows = second[...]
    for p in range(3):
        a1, a2, _ = spots[p]
        near[p][a2, a1] = rows[:, cuts[p]]

    def iota(shape, dim):
        return lax.broadcasted_iota(jnp.int32, shape, dim)

    def token_of(p, number):
        first, second_stride, third = STRIDES[p]
        device = (
            spots[p][2] * third
            + core
            + number // (RING * count) * second_stride
            + number // count % RING * first
        )
        return device * count + number % count

    def expert_of(p, number):
        third = STRIDES[p][2]
        return me - spots[p][2] * third - core + number // 2 * third + number % 2

    routes_low = onehot_values(routes[...])
    weights_low = route_weights[...].astype(BF16)
    up_row = iota((plane, plane), 0)
    up_col = iota((plane, plane), 1)
    same = up_row // count == up_col // count
    upper = onehot(same & (up_row < up_col))
    lower = onehot(same & (up_col < up_row))
    slot_row = iota((note, plane), 0)
    slot_col = iota((note, plane), 1)
    wanted = jnp.where(slot_col // count == slot_row // MOST, slot_row % MOST, -2).astype(F32)
    peers = 2 * RING

    def selector(p):
        pick = onehot(iota((tokens, plane), 0) == token_of(p, iota((tokens, plane), 1)))
        here = dot(routes_low, pick)
        names = expert_of(p, iota((peers, plane), 0)).astype(F32)
        named = names < 0.0
        for j in range(TOPK):
            named = named | (here[j : j + 1, :] == names)
        before = dot(onehot(named), upper)
        rank = jnp.where(named, before, -1.0)
        parts = [
            onehot(jnp.broadcast_to(rank[i : i + 1, :], (note, plane)) == wanted)
            for i in range(peers)
        ]
        return jnp.concatenate(parts, 0)

    selectors = [selector(p) for p in range(3)]

    for offset in (1, 3, 2):
        for p in range(3):
            a1, a2, _ = spots[p]
            slot = near[p].at[a2, (a1 + RING - offset) % RING]
            copy(mine[p], slot, s1.at[p * 4 + offset], r1.at[p * 4 + offset], partner).wait_recv()
            onward(p, offset, slot)

    for p in (1, 2, 0):
        a1, a2, a3 = spots[p]
        for offset in (1, 3, 2):
            for step in (0, 1, 3, 2):
                slot = near[p].at[(a2 + RING - offset) % RING, (a1 + RING - step) % RING]
                index = p * 16 + offset * 4 + step
                copy(mine[p], slot, s2.at[index], r2.at[index], partner).wait_recv()
        held = near[p][...].reshape(plane, widths[p])
        picked = dot(selectors[p], held).astype(BF16)
        chosen[p][...] = picked.reshape(peers, note, widths[p])
        for offset in (1, 3, 2):
            chip = peer(STRIDES[p][2], offset) - core
            for side in range(2):
                launch(
                    chosen[p].at[(a3 + offset) % RING * 2 + side],
                    inbox[p].at[core, a3],
                    s3.at[p * 8 + offset * 2 + side],
                    r3.at[p * 8 + offset * 2 + core],
                    chip + side,
                )
        launch(
            chosen[p].at[a3 * 2 + 1 - core],
            inbox[p].at[core, a3],
            s3.at[p * 8],
            r3.at[p * 8 + core],
            partner,
        )
        inbox[p][core, a3] = chosen[p][a3 * 2 + core]

    def gated(gate_part, up_part):
        return (jax.nn.silu(gate_part) * up_part).astype(BF16)

    loads[0].wait()
    loads[1].wait()
    shared_hidden = gated(dot(rows, sg[...]), dot(rows, su[...]))
    loads[4].wait()
    kept = residual[...].astype(F32) + dot(shared_hidden, sd[...])

    turned = (((1,), (1,)), ((), ()))
    tall_row = iota((plane, peers * note), 0)
    tall_col = iota((plane, peers * note), 1)
    expand = onehot(iota((128, peers * note), 0) == iota((128, peers * note), 1) // note)
    wanted_t = jnp.where(
        tall_row // count == tall_col % note // MOST, tall_col % MOST, -2
    ).astype(F32)

    def mixing(p):
        pick = onehot(iota((plane, tokens), 1) == token_of(p, iota((plane, tokens), 0)))
        here = lax.dot_general(pick, routes_low, turned, preferred_element_type=F32)
        weigh = lax.dot_general(pick, weights_low, turned, preferred_element_type=F32)
        number = iota((plane, 128), 1)
        names = jnp.where(number < peers, expert_of(p, number), -1).astype(F32)
        named = names < -2.0
        weight = jnp.zeros((plane, 128), F32)
        for j in range(TOPK):
            hit = here[:, j : j + 1] == names
            named = named | hit
            weight = weight + jnp.where(hit, weigh[:, j : j + 1], 0.0)
        before = dot(lower, onehot(named))
        rank = dot(jnp.where(named, before, -1.0).astype(BF16), expand)
        spread = dot(weight.astype(BF16), expand)
        return jnp.where(rank == wanted_t, spread, 0.0).astype(BF16)

    mixers = [mixing(p) for p in range(3)]

    each = RING * note
    turn_row = iota((each, each), 0)
    turn_col = iota((each, each), 1)

    def digits(number):
        return number // 64, number // 16 % 4, number // 4 % 4, number % 4

    def joined(a, b, c, d):
        return ((a * RING + b) * RING + c) * MOST + d

    def orders(number):
        z, y, x, s = digits(number)
        return [None, joined(x, z, y, s), joined(y, x, z, s)]

    def restored(number):
        first, middle, last, s = digits(number)
        return [None, joined(middle, last, first, s), joined(last, first, middle, s)]

    turns = [None] + [onehot(turn_col == orders(turn_row)[p]) for p in (1, 2)]
    returns = [None] + [onehot(turn_col == restored(turn_row)[p]) for p in (1, 2)]

    gate_part = None
    up_part = None
    loads[2].wait()
    loads[3].wait()
    for p in (1, 2, 0):
        a3 = spots[p][2]
        for offset in (0, 1, 3, 2):
            for side in range(2):
                if offset == 0 and side == 1:
                    continue
                which = side if offset else 1 - core
                slot = inbox[p].at[which, (a3 + RING - offset) % RING]
                index = p * 8 + offset * 2 + which
                copy(chosen[p].at[0], slot, s3.at[index], r3.at[index], partner).wait_recv()
        if p == 0:
            inputs = inbox[p][...].reshape(2 * each, widths[p])
        else:
            inputs = jnp.concatenate(
                [
                    dot(turns[p], inbox[p][side].reshape(each, widths[p])).astype(BF16)
                    for side in range(2)
                ],
                0,
            )
        gate_more = dot(inputs, eg[cuts[p], :])
        up_more = dot(inputs, eu[cuts[p], :])
        gate_part = gate_more if gate_part is None else gate_part + gate_more
        up_part = up_more if up_part is None else up_part + up_more
    hidden = gated(gate_part, up_part)
    loads[5].wait()

    for p in range(3):
        a3 = spots[p][2]
        if p == 0:
            inputs = hidden
        else:
            inputs = jnp.concatenate(
                [
                    dot(returns[p], hidden[side * each : (side + 1) * each]).astype(BF16)
                    for side in range(2)
                ],
                0,
            )
        result = dot(inputs, ed[:, cuts[p]]).astype(BF16)
        answer[p][...] = result.reshape(2, RING, note, widths[p])
        for offset in (1, 3, 2):
            chip = peer(STRIDES[p][2], offset) - core
            for side in range(2):
                launch(
                    answer[p].at[side, (a3 + offset) % RING],
                    back[p].at[a3, core],
                    t3.at[p * 8 + offset * 2 + side],
                    u3.at[p * 8 + offset * 2 + core],
                    chip + side,
                )
        launch(
            answer[p].at[1 - core, a3],
            back[p].at[a3, core],
            t3.at[p * 8],
            u3.at[p * 8 + core],
            partner,
        )
        back[p][a3, core] = answer[p][core, a3]

    for p in (1, 2, 0):
        a1, a2, a3 = spots[p]
        for offset in (0, 1, 3, 2):
            for side in range(2):
                if offset == 0 and side == 1:
                    continue
                which = side if offset else 1 - core
                slot = back[p].at[(a3 + RING - offset) % RING, which]
                index = p * 8 + offset * 2 + which
                copy(chosen[p].at[0], slot, t3.at[index], u3.at[index], partner).wait_recv()
        summed = dot(mixers[p], back[p][...].reshape(peers * note, widths[p])).astype(BF16)
        total[p][...] = summed.reshape(RING, RING, count, widths[p])
        for offset in (1, 3, 2):
            launch(
                total[p].at[(a2 + offset) % RING],
                gather[p].at[offset],
                t2.at[p * 4 + offset],
                u2.at[p * 4 + offset],
                peer(STRIDES[p][1], offset),
            )
    for p in (1, 2, 0):
        a1, a2, a3 = spots[p]
        summed = total[p][a2].astype(F32)
        for offset in (1, 3, 2):
            index = p * 4 + offset
            slot = gather[p].at[offset]
            copy(total[p].at[0], slot, t2.at[index], u2.at[index], partner).wait_recv()
            summed = summed + gather[p][offset].astype(F32)
        line[p][...] = summed.astype(BF16)
        for offset in (1, 3, 2):
            launch(
                line[p].at[(a1 + offset) % RING],
                final[p].at[offset],
                t1.at[p * 4 + offset],
                u1.at[p * 4 + offset],
                peer(STRIDES[p][0], offset),
            )
    for p in (1, 2, 0):
        a1 = spots[p][0]
        summed = line[p][a1].astype(F32)
        for offset in (1, 3, 2):
            index = p * 4 + offset
            slot = final[p].at[offset]
            copy(line[p].at[0], slot, t1.at[index], u1.at[index], partner).wait_recv()
            summed = summed + final[p][offset].astype(F32)
        out[:, cuts[p]] = (kept[:, cuts[p]] + summed).astype(BF16)
    for made in sends:
        made.wait_send()


def experts(second, residual, routes, weights, *matrices):
    count, width = second.shape
    widths = part_widths(width)
    vmem = pl.BlockSpec(memory_space=pltpu.VMEM)
    hbm = pl.BlockSpec(memory_space=pl.ANY)
    dma = pltpu.SemaphoreType.DMA
    blocks = RING * RING
    note = blocks * MOST
    shapes = (
        (RING, RING, count),
        (2 * RING, note),
        (2, RING, note),
        (2, RING, note),
        (RING, 2, note),
        (RING, RING, count),
        (RING, RING, count),
        (RING, count),
        (RING, count),
    )
    shapes = [pltpu.VMEM(shape + (w,), BF16) for shape in shapes for w in widths]
    sizes = (6, 12, 12, 48, 48, 24, 24, 24, 24, 12, 12, 12, 12)
    return pl.pallas_call(
        functools.partial(experts_kernel, widths),
        out_shape=jax.ShapeDtypeStruct((count, width), BF16),
        in_specs=[vmem] * 4 + [hbm] * 6,
        out_specs=vmem,
        scratch_shapes=[pltpu.VMEM(m.shape[-2:], BF16) for m in matrices]
        + shapes
        + [dma((size,)) for size in sizes],
        compiler_params=pltpu.CompilerParams(
            collective_id=1, has_side_effects=True, vmem_limit_bytes=VMEM_BYTES
        ),
        name="experts",
    )(second, residual, routes, weights, *matrices)


def per_device(
    tokens,
    recurrent_state,
    first_gain,
    w_receptance,
    w_key,
    w_value,
    decay_down,
    decay_up,
    decay_base,
    rate_down,
    rate_up,
    rate_base,
    key_scale,
    head_gain,
    w_output,
    second_gain,
    shared_gate,
    shared_up,
    shared_down,
    expert_gate,
    expert_up,
    expert_down,
    routes,
    route_weights,
):
    vectors = project(
        tokens,
        first_gain[None, :],
        w_receptance,
        w_key,
        w_value,
        decay_down.T,
        decay_up,
        decay_base[None, :],
        rate_down.T,
        rate_up,
        rate_base[None, :],
        key_scale[None, :],
    )
    new_state, residual, second = mixer(
        vectors,
        recurrent_state,
        head_gain[None, :],
        tokens,
        w_output,
        second_gain[None, :],
    )
    new_tokens = experts(
        second,
        residual,
        routes.T,
        route_weights.T,
        shared_gate,
        shared_up,
        shared_down,
        expert_gate,
        expert_up,
        expert_down,
    )
    return (new_tokens, new_state)


def solution(mesh):
    in_specs = (
        P("ep", None),
        P("ep", None, None),
        P(),
        P("ep", None),
        P("ep", None),
        P("ep", None),
        P(),
        P(),
        P(),
        P(),
        P(),
        P(),
        P(),
        P(),
        P(),
        P(),
        P(),
        P(),
        P(),
        P("ep", None, None),
        P("ep", None, None),
        P("ep", None, None),
        P(),
        P(),
    )
    out_specs = (P("ep", None), P("ep", None, None))
    return jax.shard_map(
        per_device, mesh=mesh, in_specs=in_specs, out_specs=out_specs, check_vma=False
    )
```

```python
import functools

import jax
import jax.numpy as jnp
from jax import lax
from jax.experimental import pallas as pl
from jax.experimental.pallas import tpu as pltpu
from jax.sharding import PartitionSpec as P

HEAD = 64
TOPK = 4
MOST = 4
RING = 4
SLICES = 6
STRIDES = ((2, 8, 32), (8, 32, 2), (32, 2, 8))
NORM_EPS = 1e-06
GROUP_EPS = 0.00064
MESH = pl.DeviceIdType.MESH
F32 = jnp.float32
BF16 = jnp.bfloat16
VMEM_BYTES = 60 * 1024 * 1024


def dot(a, b):
    return jnp.dot(a, b, preferred_element_type=F32)


def rms_scale(inputs, gain):
    widened = inputs.astype(F32)
    return (
        widened * lax.rsqrt(jnp.mean(widened * widened, axis=-1, keepdims=True) + NORM_EPS) * gain
    )


def project_kernel(
    tokens,
    gain,
    w_r,
    w_k,
    w_v,
    decay_down,
    decay_up,
    decay_base,
    rate_down,
    rate_up,
    rate_base,
    key_scale,
    out,
    stage,
    wbuf,
    nsend,
    xbuf,
    psend,
    precv,
    local_sem,
    wsend_sem,
    wrecv_sem,
    xsend_sem,
    xrecv_sem,
    psend_sem,
    precv_sem,
):
    rows, mix = w_r.shape
    half = mix // 2
    count, width = tokens.shape
    pair = 2 * rows
    depth = width // RING
    me = lax.axis_index("ep")
    core = me % 2
    partner = me + 1 - 2 * core

    def place(stride):
        return (me // stride) % RING

    def peer(stride, offset):
        return me + ((place(stride) + offset) % RING - place(stride)) * stride

    spots = [[place(stride) for stride in STRIDES[p]] for p in range(3)]
    local = []
    for p, weight in enumerate((w_r, w_k, w_v)):
        for side in range(2):
            local.append(
                pltpu.make_async_copy(
                    weight.at[:, pl.ds(side * half, half)],
                    stage.at[p, side],
                    local_sem.at[p * 2 + side],
                )
            )
    for copy in local:
        copy.start()

    barrier = pltpu.get_barrier_semaphore()
    greet = [partner]
    for stride in STRIDES[0]:
        for offset in range(1, RING):
            mate = peer(stride, offset)
            greet = greet + [mate, mate + 1 - 2 * core]
    for mate in greet:
        pl.semaphore_signal(barrier, inc=1, device_id=(mate,), device_id_type=MESH)

    normed = rms_scale(tokens[...], gain[...]).astype(BF16)
    for q in range(RING):
        nsend[0, q] = normed[:, q * depth : (q + 1) * depth]
        chunks = [z * depth + y * RING * pair + q * pair for z in range(RING) for y in range(RING)]
        nsend[1, q] = jnp.concatenate([normed[:, s : s + pair] for s in chunks], axis=1)
        chunks = [z * depth + q * RING * pair for z in range(RING)]
        nsend[2, q] = jnp.concatenate([normed[:, s : s + RING * pair] for s in chunks], axis=1)
    for copy in local:
        copy.wait()
    pl.semaphore_wait(barrier, len(greet))

    sends = []

    def remote(source, target, send, receive, device):
        return pltpu.make_async_remote_copy(
            src_ref=source,
            dst_ref=target,
            send_sem=send,
            recv_sem=receive,
            device_id=(device,),
            device_id_type=MESH,
        )

    def launch(*args):
        made = remote(*args)
        made.start()
        sends.append(made)

    def chip_slot(p, first, second):
        return wbuf.at[p, first, second] if p == 2 else wbuf.at[p, second, first]

    def row_slot(p, first, second, which):
        return chip_slot(p, first, second).at[which]

    for p in range(3):
        a1, a2, _ = spots[p]
        for offset in (1, 3, 2):
            chip = peer(STRIDES[p][0], offset) - core
            for side in range(2):
                launch(
                    stage.at[p, side],
                    row_slot(p, a1, a2, core),
                    wsend_sem.at[p * 32 + offset * 2 + side],
                    wrecv_sem.at[p * 32 + offset * 2 + core],
                    chip + side,
                )
        launch(
            stage.at[p, 1 - core],
            row_slot(p, a1, a2, core),
            wsend_sem.at[p * 32],
            wrecv_sem.at[p * 32 + core],
            partner,
        )
    for p in range(3):
        a1, a2, _ = spots[p]
        for offset in (1, 3, 2):
            chip = peer(STRIDES[p][1], offset) - core
            for side in range(2):
                launch(
                    stage.at[p, side],
                    row_slot(p, a1, a2, core),
                    wsend_sem.at[p * 32 + 8 + offset * 2 + side],
                    wrecv_sem.at[p * 32 + 8 + offset * 2 + core],
                    chip + side,
                )
    for p in range(3):
        a3 = spots[p][2]
        for offset in (1, 3, 2):
            chip = peer(STRIDES[p][2], offset) - core
            for side in range(2):
                launch(
                    nsend.at[p, (a3 + offset) % RING],
                    xbuf.at[p, a3, core],
                    xsend_sem.at[p * 8 + offset * 2 + side],
                    xrecv_sem.at[p * 8 + offset * 2 + core],
                    chip + side,
                )
        launch(
            nsend.at[p, a3],
            xbuf.at[p, a3, core],
            xsend_sem.at[p * 8],
            xrecv_sem.at[p * 8 + core],
            partner,
        )
    for p in range(3):
        a1, a2, a3 = spots[p]
        own = stage[p, core]
        if p == 2:
            wbuf[p, a1, a2, core] = own
        else:
            wbuf[p, a2, a1, core] = own
        xbuf[p, a3, core] = nsend[p, a3]

    def arrived(p, slot, index):
        remote(stage.at[p, 0], slot, wsend_sem.at[index], wrecv_sem.at[index], partner).wait_recv()

    for step in (1, 3, 2):
        for p in range(3):
            a1, a2, _ = spots[p]
            first = (a1 + RING - step) % RING
            for which in range(2):
                arrived(p, row_slot(p, first, a2, which), p * 32 + step * 2 + which)
            block = chip_slot(p, first, a2)
            for offset in (1, 3, 2):
                index = p * 32 + 16 + offset * 4 + step
                launch(
                    block,
                    block,
                    wsend_sem.at[index],
                    wrecv_sem.at[index],
                    peer(STRIDES[p][1], offset),
                )

    def put(number, values, first):
        for head in range(values.shape[1] // HEAD):
            out[number, :, first + head, :] = values[:, head * HEAD : (head + 1) * HEAD]

    heads = mix // HEAD
    flip = (((1,), (1,)), ((), ()))

    def down(matrix):
        return lax.dot_general(normed, matrix, flip, preferred_element_type=F32)

    decay_low = jnp.tanh(down(decay_down[...])).astype(BF16)
    decay_pre = decay_base[...] + dot(decay_low, decay_up[...])
    put(3, jnp.exp(-jnp.exp(-jax.nn.softplus(-decay_pre) - 0.5)), 0)
    rate_low = down(rate_down[...]).astype(BF16)
    put(4, jax.nn.sigmoid(rate_base[...] + dot(rate_low, rate_up[...])), 0)

    for p in range(3):
        a1, a2, a3 = spots[p]
        arrived(p, row_slot(p, a1, a2, 1 - core), p * 32 + 1 - core)
        for offset in (0, 1, 3, 2):
            for side in range(2):
                if offset == 0 and side == 1:
                    continue
                which = side if offset else 1 - core
                index = p * 8 + offset * 2 + which
                remote(
                    nsend.at[p, 0],
                    xbuf.at[p, (a3 + RING - offset) % RING, which],
                    xsend_sem.at[index],
                    xrecv_sem.at[index],
                    partner,
                ).wait_recv()
        for offset in (1, 3, 2):
            second = (a2 + RING - offset) % RING
            for which in range(2):
                arrived(p, row_slot(p, a1, second, which), p * 32 + 8 + offset * 2 + which)
            for step in (1, 3, 2):
                block = chip_slot(p, (a1 + RING - step) % RING, second)
                index = p * 32 + 16 + offset * 4 + step
                remote(
                    block, block, wsend_sem.at[index], wrecv_sem.at[index], partner
                ).wait_recv()
        stacked = xbuf[p].reshape(2 * RING * count, depth)
        part = dot(stacked, wbuf[p].reshape(depth, half)).astype(BF16)
        psend[p] = part.reshape(RING, 2, count, half)
        for offset in (1, 3, 2):
            chip = peer(STRIDES[p][2], offset) - core
            for side in range(2):
                launch(
                    psend.at[p, (a3 + offset) % RING, side],
                    precv.at[p, a3, core],
                    psend_sem.at[p * 8 + offset * 2 + side],
                    precv_sem.at[p * 8 + offset * 2 + core],
                    chip + side,
                )
        launch(
            psend.at[p, a3, 1 - core],
            precv.at[p, a3, core],
            psend_sem.at[p * 8],
            precv_sem.at[p * 8 + core],
            partner,
        )
        precv[p, a3, core] = psend[p, a3, core]

    for p in range(3):
        a3 = spots[p][2]
        for offset in (0, 1, 3, 2):
            for side in range(2):
                if offset == 0 and side == 1:
                    continue
                which = side if offset else 1 - core
                index = p * 8 + offset * 2 + which
                remote(
                    nsend.at[p, 0],
                    precv.at[p, (a3 + RING - offset) % RING, which],
                    psend_sem.at[index],
                    precv_sem.at[index],
                    partner,
                ).wait_recv()
        for side in range(2):
            total = precv[p, 0, side].astype(F32)
            for which in range(1, RING):
                total = total + precv[p, which, side].astype(F32)
            total = total.astype(BF16).astype(F32)
            put(p, total, side * (heads // 2))
            if p == 1:
                scale = key_scale[:, side * half : (side + 1) * half]
                put(5, total * scale, side * (heads // 2))
    for made in sends:
        made.wait_send()


def project(tokens, gain, w_r, w_k, w_v, dd, du, db, rd, ru, rb, scale):
    count, width = tokens.shape
    rows, mix = w_r.shape
    half = mix // 2
    depth = width // RING
    vmem = pl.BlockSpec(memory_space=pltpu.VMEM)
    hbm = pl.BlockSpec(memory_space=pl.ANY)
    dma = pltpu.SemaphoreType.DMA
    return pl.pallas_call(
        project_kernel,
        out_shape=jax.ShapeDtypeStruct((6, count, mix // HEAD, HEAD), F32),
        in_specs=[vmem, vmem, hbm, hbm, hbm] + [vmem] * 7,
        out_specs=vmem,
        scratch_shapes=[
            pltpu.VMEM((3, 2, rows, half), BF16),
            pltpu.VMEM((3, RING, RING, 2, rows, half), BF16),
            pltpu.VMEM((3, RING, count, depth), BF16),
            pltpu.VMEM((3, RING, 2, count, depth), BF16),
            pltpu.VMEM((3, RING, 2, count, half), BF16),
            pltpu.VMEM((3, RING, 2, count, half), BF16),
            dma((6,)),
            dma((96,)),
            dma((96,)),
            dma((24,)),
            dma((24,)),
            dma((24,)),
            dma((24,)),
        ],
        compiler_params=pltpu.CompilerParams(
            collective_id=0, has_side_effects=True, vmem_limit_bytes=VMEM_BYTES
        ),
        name="project",
    )(tokens, gain, w_r, w_k, w_v, dd, du, db, rd, ru, rb, scale)


def split_sum(values, ones):
    high = values.astype(BF16)
    low = (values - high.astype(F32)).astype(BF16)
    return dot(high, ones) + dot(low, ones)


def mixer_kernel(
    steps,
    vectors,
    state,
    head_gain,
    tokens,
    w_output,
    second_gain,
    new_state,
    residual,
    second,
    wbuf,
    mixed,
    sem,
):
    step = pl.program_id(0)
    _, per_step, heads, _ = vectors.shape
    entries = state.shape[2]
    span = 256
    tiles = entries // span
    copies = span // HEAD
    copy = pltpu.make_async_copy(w_output, wbuf, sem)

    @pl.when(step == 0)
    def _():
        copy.start()

    row = lax.broadcasted_iota(jnp.int32, (span, span), 0)
    col = lax.broadcasted_iota(jnp.int32, (span, span), 1)
    ones = (row // HEAD == col // HEAD).astype(F32).astype(BF16)
    lane = lax.broadcasted_iota(jnp.int32, (heads, span), 1)

    def widen(inputs):
        return jnp.concatenate([inputs] * copies, axis=1)

    for number in range(per_step):
        reader, keys, values, decay, learn, scaled = [vectors[w, number] for w in range(6)]
        direction = scaled / jnp.sqrt(jnp.sum(scaled * scaled, axis=-1, keepdims=True) + 1.0)
        wide_direction = widen(direction)
        wide_decay = widen(decay)
        wide_learn = widen(direction * learn)
        wide_keys = widen(keys)
        wide_reader = widen(reader)
        wide_values = widen(values)
        blocks = [state[number, :, i * span : (i + 1) * span] for i in range(tiles)]
        picks = [(lane % HEAD) == i * copies + lane // HEAD for i in range(tiles)]
        removed = dot(
            jnp.concatenate([(b * wide_direction).astype(BF16) for b in blocks], 0), ones
        )
        spread_values = dot(
            jnp.concatenate([jnp.where(p, wide_values, 0.0) for p in picks], 0).astype(BF16), ones
        )
        later = []
        for i in range(tiles):
            part = slice(i * heads, (i + 1) * heads)
            fresh = (
                blocks[i] * wide_decay
                - removed[part] * wide_learn
                + spread_values[part] * wide_keys
            )
            new_state[number, :, i * span : (i + 1) * span] = fresh
            later.append(fresh * wide_reader)
        read = split_sum(jnp.concatenate(later, 0), ones)
        gathered = jnp.where(picks[0], read[:heads], 0.0)
        for i in range(1, tiles):
            gathered = gathered + jnp.where(picks[i], read[i * heads : (i + 1) * heads], 0.0)
        readout = gathered[:, :HEAD]
        for i in range(1, copies):
            readout = readout + gathered[:, i * HEAD : (i + 1) * HEAD]
        centre = jnp.mean(readout, axis=-1, keepdims=True)
        spread = jnp.mean(jnp.square(readout - centre), axis=-1, keepdims=True)
        mixed[step * per_step + number] = (
            readout - centre
        ) * lax.rsqrt(spread + GROUP_EPS)

    @pl.when(step == steps - 1)
    def _():
        count = mixed.shape[0]
        channels = heads * HEAD
        flat = mixed[...].reshape(count * heads, HEAD)
        source = lax.broadcasted_iota(jnp.int32, (HEAD, channels), 0)
        target = lax.broadcasted_iota(jnp.int32, (HEAD, channels), 1)
        tiled = split_sum(flat, (target % HEAD == source).astype(F32).astype(BF16))
        head = lax.broadcasted_iota(jnp.int32, (count * heads, channels), 0) % heads
        channel = lax.broadcasted_iota(jnp.int32, (count * heads, channels), 1) // HEAD
        kept = (jnp.where(head == channel, tiled, 0.0) * head_gain[...]).astype(BF16)
        owner = lax.broadcasted_iota(jnp.int32, (count, count * heads), 1) // heads
        token = lax.broadcasted_iota(jnp.int32, (count, count * heads), 0)
        rows = dot((owner == token).astype(F32).astype(BF16), kept).astype(BF16)
        copy.wait()
        after = (tokens[...].astype(F32) + dot(rows, wbuf[...])).astype(BF16)
        residual[...] = after
        second[...] = rms_scale(after, second_gain[...]).astype(BF16)


def mixer(vectors, state, head_gain, tokens, w_output, second_gain):
    _, count, heads, _ = vectors.shape
    width = tokens.shape[1]
    entries = state.shape[2]
    per_step = 8 if count % 8 == 0 else 1
    steps = count // per_step
    whole = lambda array: pl.BlockSpec(array.shape, lambda i: (0,) * array.ndim)
    block = pl.BlockSpec((per_step, heads, entries), lambda i: (i, 0, 0))
    flat = pl.BlockSpec((count, width), lambda i: (0, 0))
    return pl.pallas_call(
        functools.partial(mixer_kernel, steps),
        grid=(steps,),
        out_shape=[
            jax.ShapeDtypeStruct(state.shape, F32),
            jax.ShapeDtypeStruct((count, width), BF16),
            jax.ShapeDtypeStruct((count, width), BF16),
        ],
        in_specs=[
            pl.BlockSpec((6, per_step, heads, HEAD), lambda i: (0, i, 0, 0)),
            block,
            whole(head_gain),
            flat,
            pl.BlockSpec(memory_space=pl.ANY),
            whole(second_gain),
        ],
        out_specs=[block, flat, flat],
        scratch_shapes=[
            pltpu.VMEM(w_output.shape, BF16),
            pltpu.VMEM((count, heads, HEAD), F32),
            pltpu.SemaphoreType.DMA,
        ],
        compiler_params=pltpu.CompilerParams(
            dimension_semantics=("arbitrary",), vmem_limit_bytes=VMEM_BYTES
        ),
        name="mixer",
    )(vectors, state, head_gain, tokens, w_output, second_gain)


def onehot(flags):
    return flags.astype(F32).astype(BF16)


def onehot_values(values):
    return values.astype(F32).astype(BF16)


def part_widths(width):
    tiles = width // 128
    counts = [tiles // SLICES + (1 if number < tiles % SLICES else 0) for number in range(SLICES)]
    return [number * 128 for number in counts]


def experts_kernel(
    widths,
    second,
    residual,
    routes,
    route_weights,
    shared_gate,
    shared_up,
    shared_down,
    expert_gate,
    expert_up,
    expert_down,
    out,
    sg,
    su,
    sd,
    eg,
    eu,
    ed,
    *rest,
):
    near, chosen, inbox, answer, back, total, gather, line, final = [
        rest[SLICES * i : SLICES * (i + 1)] for i in range(9)
    ]
    local_sem = rest[9 * SLICES]
    s1, r1, s2, r2, s3, r3, t3, u3, t2, u2, t1, u1 = rest[9 * SLICES + 1 :]
    count = second.shape[0]
    tokens = routes.shape[1]
    starts = [sum(widths[:p]) for p in range(SLICES)]
    cuts = [slice(starts[p], starts[p] + widths[p]) for p in range(SLICES)]
    blocks = RING * RING
    plane = blocks * count
    note = blocks * MOST
    me = lax.axis_index("ep")
    core = me % 2
    partner = me + 1 - 2 * core

    def place(stride):
        return (me // stride) % RING

    def peer(stride, offset):
        return me + ((place(stride) + offset) % RING - place(stride)) * stride

    strides = [STRIDES[p % 3] for p in range(SLICES)]
    spots = [[place(stride) for stride in strides[p]] for p in range(SLICES)]
    barrier = pltpu.get_barrier_semaphore()
    greet = [partner]
    for stride in STRIDES[0]:
        for offset in range(1, RING):
            mate = peer(stride, offset)
            greet = greet + [mate, mate + 1 - 2 * core]
    for mate in greet:
        pl.semaphore_signal(barrier, inc=1, device_id=(mate,), device_id_type=MESH)
    loads = [
        pltpu.make_async_copy(source, target, local_sem.at[number])
        for number, (source, target) in enumerate(
            (
                (shared_gate, sg),
                (shared_up, su),
                (expert_gate.at[0], eg),
                (expert_up.at[0], eu),
                (shared_down, sd),
                (expert_down.at[0], ed),
            )
        )
    ]
    for load in loads:
        load.start()
    pl.semaphore_wait(barrier, len(greet))

    sends = []

    def copy(source, target, send, receive, device):
        return pltpu.make_async_remote_copy(
            src_ref=source,
            dst_ref=target,
            send_sem=send,
            recv_sem=receive,
            device_id=(device,),
            device_id_type=MESH,
        )

    def launch(*args):
        made = copy(*args)
        made.start()
        sends.append(made)

    mine = [second.at[:, pl.ds(starts[p], widths[p])] for p in range(SLICES)]

    def onward(p, step, source):
        a1, a2, _ = spots[p]
        for offset in (1, 3, 2):
            index = p * 16 + offset * 4 + step
            launch(
                source,
                near[p].at[a2, (a1 + RING - step) % RING],
                s2.at[index],
                r2.at[index],
                peer(strides[p][1], offset),
            )

    def enter(p):
        a1, a2, _ = spots[p]
        for offset in (1, 3, 2):
            launch(
                mine[p],
                near[p].at[a2, a1],
                s1.at[p * 4 + offset],
                r1.at[p * 4 + offset],
                peer(strides[p][0], offset),
            )

    groups = [range(first, first + 3) for first in range(0, SLICES, 3)]
    for p in groups[0]:
        enter(p)
    for p in groups[0]:
        onward(p, 0, mine[p])
    for group in groups[1:]:
        for p in group:
            enter(p)
    rows = second[...]
    for p in range(SLICES):
        a1, a2, _ = spots[p]
        near[p][a2, a1] = rows[:, cuts[p]]

    def iota(shape, dim):
        return lax.broadcasted_iota(jnp.int32, shape, dim)

    def token_of(p, number):
        first, second_stride, third = strides[p]
        device = (
            spots[p][2] * third
            + core
            + number // (RING * count) * second_stride
            + number // count % RING * first
        )
        return device * count + number % count

    def expert_of(p, number):
        third = strides[p][2]
        return me - spots[p][2] * third - core + number // 2 * third + number % 2

    routes_low = onehot_values(routes[...])
    weights_low = route_weights[...].astype(BF16)
    up_row = iota((plane, plane), 0)
    up_col = iota((plane, plane), 1)
    same = up_row // count == up_col // count
    upper = onehot(same & (up_row < up_col))
    lower = onehot(same & (up_col < up_row))
    slot_row = iota((note, plane), 0)
    slot_col = iota((note, plane), 1)
    wanted = jnp.where(slot_col // count == slot_row // MOST, slot_row % MOST, -2).astype(F32)
    peers = 2 * RING

    def selector(p):
        pick = onehot(iota((tokens, plane), 0) == token_of(p, iota((tokens, plane), 1)))
        here = dot(routes_low, pick)
        names = expert_of(p, iota((peers, plane), 0)).astype(F32)
        named = names < 0.0
        for j in range(TOPK):
            named = named | (here[j : j + 1, :] == names)
        before = dot(onehot(named), upper)
        rank = jnp.where(named, before, -1.0)
        parts = [
            onehot(jnp.broadcast_to(rank[i : i + 1, :], (note, plane)) == wanted)
            for i in range(peers)
        ]
        return jnp.concatenate(parts, 0)

    selectors = [selector(p) for p in range(3)]

    for group in groups:
        if group != groups[0]:
            for p in group:
                onward(p, 0, mine[p])
        for offset in (1, 3, 2):
            for p in group:
                a1, a2, _ = spots[p]
                slot = near[p].at[a2, (a1 + RING - offset) % RING]
                index = p * 4 + offset
                copy(mine[p], slot, s1.at[index], r1.at[index], partner).wait_recv()
                onward(p, offset, slot)

    for p in range(SLICES):
        a1, a2, a3 = spots[p]
        for offset in (1, 3, 2):
            for step in (0, 1, 3, 2):
                slot = near[p].at[(a2 + RING - offset) % RING, (a1 + RING - step) % RING]
                index = p * 16 + offset * 4 + step
                copy(mine[p], slot, s2.at[index], r2.at[index], partner).wait_recv()
        held = near[p][...].reshape(plane, widths[p])
        picked = dot(selectors[p % 3], held).astype(BF16)
        chosen[p][...] = picked.reshape(peers, note, widths[p])
        for offset in (1, 3, 2):
            chip = peer(strides[p][2], offset) - core
            for side in range(2):
                launch(
                    chosen[p].at[(a3 + offset) % RING * 2 + side],
                    inbox[p].at[core, a3],
                    s3.at[p * 8 + offset * 2 + side],
                    r3.at[p * 8 + offset * 2 + core],
                    chip + side,
                )
        launch(
            chosen[p].at[a3 * 2 + 1 - core],
            inbox[p].at[core, a3],
            s3.at[p * 8],
            r3.at[p * 8 + core],
            partner,
        )
        inbox[p][core, a3] = chosen[p][a3 * 2 + core]

    def gated(gate_part, up_part):
        return (jax.nn.silu(gate_part) * up_part).astype(BF16)

    each = RING * note
    turn_row = iota((each, each), 0)
    turn_col = iota((each, each), 1)

    def digits(number):
        return number // 64, number // 16 % 4, number // 4 % 4, number % 4

    def joined(a, b, c, d):
        return ((a * RING + b) * RING + c) * MOST + d

    def orders(number):
        z, y, x, s = digits(number)
        return [None, joined(x, z, y, s), joined(y, x, z, s)]

    def restored(number):
        first, middle, last, s = digits(number)
        return [None, joined(middle, last, first, s), joined(last, first, middle, s)]

    turns = [None] + [onehot(turn_col == orders(turn_row)[p]) for p in (1, 2)]
    returns = [None] + [onehot(turn_col == restored(turn_row)[p]) for p in (1, 2)]

    gate_part = None
    up_part = None
    loads[2].wait()
    loads[3].wait()
    for p in range(SLICES):
        a3 = spots[p][2]
        for offset in (0, 1, 3, 2):
            for side in range(2):
                if offset == 0 and side == 1:
                    continue
                which = side if offset else 1 - core
                slot = inbox[p].at[which, (a3 + RING - offset) % RING]
                index = p * 8 + offset * 2 + which
                copy(chosen[p].at[0], slot, s3.at[index], r3.at[index], partner).wait_recv()
        if p % 3 == 0:
            inputs = inbox[p][...].reshape(2 * each, widths[p])
        else:
            inputs = jnp.concatenate(
                [
                    dot(turns[p % 3], inbox[p][side].reshape(each, widths[p])).astype(BF16)
                    for side in range(2)
                ],
                0,
            )
        gate_more = dot(inputs, eg[cuts[p], :])
        up_more = dot(inputs, eu[cuts[p], :])
        gate_part = gate_more if gate_part is None else gate_part + gate_more
        up_part = up_more if up_part is None else up_part + up_more
    hidden = gated(gate_part, up_part)
    loads[5].wait()

    for p in range(SLICES):
        a3 = spots[p][2]
        if p % 3 == 0:
            inputs = hidden
        else:
            inputs = jnp.concatenate(
                [
                    dot(returns[p % 3], hidden[side * each : (side + 1) * each]).astype(BF16)
                    for side in range(2)
                ],
                0,
            )
        result = dot(inputs, ed[:, cuts[p]]).astype(BF16)
        answer[p][...] = result.reshape(2, RING, note, widths[p])
        for offset in (1, 3, 2):
            chip = peer(strides[p][2], offset) - core
            for side in range(2):
                launch(
                    answer[p].at[side, (a3 + offset) % RING],
                    back[p].at[a3, core],
                    t3.at[p * 8 + offset * 2 + side],
                    u3.at[p * 8 + offset * 2 + core],
                    chip + side,
                )
        launch(
            answer[p].at[1 - core, a3],
            back[p].at[a3, core],
            t3.at[p * 8],
            u3.at[p * 8 + core],
            partner,
        )
        back[p][a3, core] = answer[p][core, a3]

    loads[0].wait()
    loads[1].wait()
    shared_hidden = gated(dot(rows, sg[...]), dot(rows, su[...]))
    loads[4].wait()
    kept = residual[...].astype(F32) + dot(shared_hidden, sd[...])

    turned = (((1,), (1,)), ((), ()))
    tall_row = iota((plane, peers * note), 0)
    tall_col = iota((plane, peers * note), 1)
    expand = onehot(iota((128, peers * note), 0) == iota((128, peers * note), 1) // note)
    wanted_t = jnp.where(
        tall_row // count == tall_col % note // MOST, tall_col % MOST, -2
    ).astype(F32)

    def mixing(p):
        pick = onehot(iota((plane, tokens), 1) == token_of(p, iota((plane, tokens), 0)))
        here = lax.dot_general(pick, routes_low, turned, preferred_element_type=F32)
        weigh = lax.dot_general(pick, weights_low, turned, preferred_element_type=F32)
        number = iota((plane, 128), 1)
        names = jnp.where(number < peers, expert_of(p, number), -1).astype(F32)
        named = names < -2.0
        weight = jnp.zeros((plane, 128), F32)
        for j in range(TOPK):
            hit = here[:, j : j + 1] == names
            named = named | hit
            weight = weight + jnp.where(hit, weigh[:, j : j + 1], 0.0)
        before = dot(lower, onehot(named))
        rank = dot(jnp.where(named, before, -1.0).astype(BF16), expand)
        spread = dot(weight.astype(BF16), expand)
        return jnp.where(rank == wanted_t, spread, 0.0).astype(BF16)

    mixers = [mixing(p) for p in range(3)]

    for p in range(SLICES):
        a1, a2, a3 = spots[p]
        for offset in (0, 1, 3, 2):
            for side in range(2):
                if offset == 0 and side == 1:
                    continue
                which = side if offset else 1 - core
                slot = back[p].at[(a3 + RING - offset) % RING, which]
                index = p * 8 + offset * 2 + which
                copy(chosen[p].at[0], slot, t3.at[index], u3.at[index], partner).wait_recv()
        summed = dot(mixers[p % 3], back[p][...].reshape(peers * note, widths[p])).astype(BF16)
        total[p][...] = summed.reshape(RING, RING, count, widths[p])
        for offset in (1, 3, 2):
            launch(
                total[p].at[(a2 + offset) % RING],
                gather[p].at[offset],
                t2.at[p * 4 + offset],
                u2.at[p * 4 + offset],
                peer(strides[p][1], offset),
            )
    for p in range(SLICES):
        a1, a2, a3 = spots[p]
        summed = total[p][a2].astype(F32)
        for offset in (1, 3, 2):
            index = p * 4 + offset
            slot = gather[p].at[offset]
            copy(total[p].at[0], slot, t2.at[index], u2.at[index], partner).wait_recv()
            summed = summed + gather[p][offset].astype(F32)
        line[p][...] = summed.astype(BF16)
        for offset in (1, 3, 2):
            launch(
                line[p].at[(a1 + offset) % RING],
                final[p].at[offset],
                t1.at[p * 4 + offset],
                u1.at[p * 4 + offset],
                peer(strides[p][0], offset),
            )
    for p in range(SLICES):
        a1 = spots[p][0]
        summed = line[p][a1].astype(F32)
        for offset in (1, 3, 2):
            index = p * 4 + offset
            slot = final[p].at[offset]
            copy(line[p].at[0], slot, t1.at[index], u1.at[index], partner).wait_recv()
            summed = summed + final[p][offset].astype(F32)
        out[:, cuts[p]] = (kept[:, cuts[p]] + summed).astype(BF16)
    for made in sends:
        made.wait_send()


def experts(second, residual, routes, weights, *matrices):
    count, width = second.shape
    widths = part_widths(width)
    vmem = pl.BlockSpec(memory_space=pltpu.VMEM)
    hbm = pl.BlockSpec(memory_space=pl.ANY)
    dma = pltpu.SemaphoreType.DMA
    blocks = RING * RING
    note = blocks * MOST
    shapes = (
        (RING, RING, count),
        (2 * RING, note),
        (2, RING, note),
        (2, RING, note),
        (RING, 2, note),
        (RING, RING, count),
        (RING, RING, count),
        (RING, count),
        (RING, count),
    )
    shapes = [pltpu.VMEM(shape + (w,), BF16) for shape in shapes for w in widths]
    sizes = [6] + [SLICES * size for size in (4, 4, 16, 16, 8, 8, 8, 8, 4, 4, 4, 4)]
    return pl.pallas_call(
        functools.partial(experts_kernel, widths),
        out_shape=jax.ShapeDtypeStruct((count, width), BF16),
        in_specs=[vmem] * 4 + [hbm] * 6,
        out_specs=vmem,
        scratch_shapes=[pltpu.VMEM(m.shape[-2:], BF16) for m in matrices]
        + shapes
        + [dma((size,)) for size in sizes],
        compiler_params=pltpu.CompilerParams(
            collective_id=1, has_side_effects=True, vmem_limit_bytes=VMEM_BYTES
        ),
        name="experts",
    )(second, residual, routes, weights, *matrices)


def per_device(
    tokens,
    recurrent_state,
    first_gain,
    w_receptance,
    w_key,
    w_value,
    decay_down,
    decay_up,
    decay_base,
    rate_down,
    rate_up,
    rate_base,
    key_scale,
    head_gain,
    w_output,
    second_gain,
    shared_gate,
    shared_up,
    shared_down,
    expert_gate,
    expert_up,
    expert_down,
    routes,
    route_weights,
):
    vectors = project(
        tokens,
        first_gain[None, :],
        w_receptance,
        w_key,
        w_value,
        decay_down.T,
        decay_up,
        decay_base[None, :],
        rate_down.T,
        rate_up,
        rate_base[None, :],
        key_scale[None, :],
    )
    new_state, residual, second = mixer(
        vectors,
        recurrent_state,
        head_gain[None, :],
        tokens,
        w_output,
        second_gain[None, :],
    )
    new_tokens = experts(
        second,
        residual,
        routes.T,
        route_weights.T,
        shared_gate,
        shared_up,
        shared_down,
        expert_gate,
        expert_up,
        expert_down,
    )
    return (new_tokens, new_state)


def solution(mesh):
    in_specs = (
        P("ep", None),
        P("ep", None, None),
        P(),
        P("ep", None),
        P("ep", None),
        P("ep", None),
        P(),
        P(),
        P(),
        P(),
        P(),
        P(),
        P(),
        P(),
        P(),
        P(),
        P(),
        P(),
        P(),
        P("ep", None, None),
        P("ep", None, None),
        P("ep", None, None),
        P(),
        P(),
    )
    out_specs = (P("ep", None), P("ep", None, None))
    return jax.shard_map(
        per_device, mesh=mesh, in_specs=in_specs, out_specs=out_specs, check_vma=False
    )
```

```python
import functools

import jax
import jax.numpy as jnp
from jax import lax
from jax.experimental import pallas as pl
from jax.experimental.pallas import tpu as pltpu
from jax.sharding import PartitionSpec as P

HEAD = 64
TOPK = 4
MOST = 4
RING = 4
SLICES = 6
STRIDES = ((2, 8, 32), (8, 32, 2), (32, 2, 8))
NORM_EPS = 1e-06
GROUP_EPS = 0.00064
MESH = pl.DeviceIdType.MESH
F32 = jnp.float32
BF16 = jnp.bfloat16
VMEM_BYTES = 60 * 1024 * 1024


def dot(a, b):
    return jnp.dot(a, b, preferred_element_type=F32)


def rms_scale(inputs, gain):
    widened = inputs.astype(F32)
    return (
        widened * lax.rsqrt(jnp.mean(widened * widened, axis=-1, keepdims=True) + NORM_EPS) * gain
    )


def onehot(flags):
    return flags.astype(F32).astype(BF16)


def onehot_values(values):
    return values.astype(F32).astype(BF16)


def part_widths(width):
    tiles = width // 128
    counts = [tiles // SLICES + (1 if number < tiles % SLICES else 0) for number in range(SLICES)]
    return [number * 128 for number in counts]


def layer_kernel(
    widths,
    tokens,
    gain,
    decay_down,
    decay_up,
    decay_base,
    rate_down,
    rate_up,
    rate_base,
    key_scale,
    head_gain,
    second_gain,
    routes,
    route_weights,
    w_r,
    w_k,
    w_v,
    state,
    w_output,
    shared_gate,
    shared_up,
    shared_down,
    expert_gate,
    expert_up,
    expert_down,
    out,
    wide_out,
    low_out,
    stage,
    wbuf,
    nsend,
    xbuf,
    psend,
    precv,
    vecs,
    old,
    wo,
    sg,
    su,
    sd,
    eg,
    eu,
    ed,
    fold,
    second,
    selectors,
    mixers,
    *rest,
):
    near, chosen, inbox, answer, back, total, gather, line, final = [
        rest[SLICES * i : SLICES * (i + 1)] for i in range(9)
    ]
    local_sem, load_sem = rest[9 * SLICES : 9 * SLICES + 2]
    wsend_sem, wrecv_sem, xsend_sem, xrecv_sem, psend_sem, precv_sem = rest[
        9 * SLICES + 2 : 9 * SLICES + 8
    ]
    s1, r1, r2, s3, r3, t3, u3, t2, u2, t1, u1 = rest[9 * SLICES + 8 :]
    rows, mix = w_r.shape
    half = mix // 2
    count, width = tokens.shape
    pair = 2 * rows
    depth = width // RING
    me = lax.axis_index("ep")
    core = me % 2
    partner = me + 1 - 2 * core

    def place(stride):
        return (me // stride) % RING

    def peer(stride, offset):
        return me + ((place(stride) + offset) % RING - place(stride)) * stride

    spots = [[place(stride) for stride in STRIDES[p % 3]] for p in range(SLICES)]
    local = []
    for p, weight in enumerate((w_r, w_k, w_v)):
        for side in range(2):
            local.append(
                pltpu.make_async_copy(
                    weight.at[:, pl.ds(side * half, half)],
                    stage.at[p, side],
                    local_sem,
                )
            )
    for copy in local:
        copy.start()

    barrier = pltpu.get_barrier_semaphore()
    greet = [partner]
    for stride in STRIDES[0]:
        for offset in range(1, RING):
            mate = peer(stride, offset)
            greet = greet + [mate, mate + 1 - 2 * core]
    for mate in greet:
        pl.semaphore_signal(barrier, inc=1, device_id=(mate,), device_id_type=MESH)

    loads = [
        pltpu.make_async_copy(source, target, load_sem.at[number])
        for number, (source, target) in enumerate(
            (
                (shared_gate, sg),
                (shared_up, su),
                (expert_gate.at[0], eg),
                (expert_up.at[0], eu),
                (shared_down, sd),
                (expert_down.at[0], ed),
                (state, old),
                (w_output, wo),
            )
        )
    ]
    for number in (6, 7, 2, 3, 5, 0, 1, 4):
        loads[number].start()

    normed = rms_scale(tokens[...], gain[...]).astype(BF16)
    for q in range(RING):
        nsend[0, q] = normed[:, q * depth : (q + 1) * depth]
        chunks = [z * depth + y * RING * pair + q * pair for z in range(RING) for y in range(RING)]
        nsend[1, q] = jnp.concatenate([normed[:, s : s + pair] for s in chunks], axis=1)
        chunks = [z * depth + q * RING * pair for z in range(RING)]
        nsend[2, q] = jnp.concatenate([normed[:, s : s + RING * pair] for s in chunks], axis=1)
    def remote(source, target, send, receive, device):
        return pltpu.make_async_remote_copy(
            src_ref=source,
            dst_ref=target,
            send_sem=send,
            recv_sem=receive,
            device_id=(device,),
            device_id_type=MESH,
        )

    def launch(*args):
        remote(*args).start()

    def settle(view, semaphore):
        remote(view, view, semaphore, semaphore, partner).wait_recv()

    def chip_index(p, first, second):
        return first * RING + second if p == 2 else second * RING + first

    def row_slot(p, first, second, which):
        return wbuf.at[p, chip_index(p, first, second) * 2 + which]

    settle(stage, local_sem)
    pl.semaphore_wait(barrier, len(greet))

    for p in range(3):
        a1, a2, _ = spots[p]
        for offset in (1, 3, 2):
            chip = peer(STRIDES[p][0], offset) - core
            for side in range(2):
                launch(
                    stage.at[p, side],
                    row_slot(p, a1, a2, core),
                    wsend_sem.at[p],
                    wrecv_sem.at[p * RING + offset],
                    chip + side,
                )
        launch(
            stage.at[p, 1 - core],
            row_slot(p, a1, a2, core),
            wsend_sem.at[p],
            wrecv_sem.at[p * RING],
            partner,
        )
    for p in range(3):
        a1, a2, _ = spots[p]
        for offset in (1, 3, 2):
            chip = peer(STRIDES[p][1], offset) - core
            for side in range(2):
                launch(
                    stage.at[p, side],
                    row_slot(p, a1, a2, core),
                    wsend_sem.at[p],
                    wrecv_sem.at[p * RING],
                    chip + side,
                )
    for p in range(3):
        a3 = spots[p][2]
        for offset in (1, 3, 2):
            chip = peer(STRIDES[p][2], offset) - core
            for side in range(2):
                launch(
                    nsend.at[p, (a3 + offset) % RING],
                    xbuf.at[p, a3 * 2 + core],
                    xsend_sem.at[p],
                    xrecv_sem.at[p],
                    chip + side,
                )
        launch(
            nsend.at[p, a3],
            xbuf.at[p, a3 * 2 + core],
            xsend_sem.at[p],
            xrecv_sem.at[p],
            partner,
        )
    for p in range(3):
        a1, a2, a3 = spots[p]
        own = stage[p, core]
        wbuf[p, chip_index(p, a1, a2) * 2 + core] = own
        xbuf[p, a3 * 2 + core] = nsend[p, a3]

    for step in (1, 3, 2):
        for p in range(3):
            a1, a2, _ = spots[p]
            first = (a1 + RING - step) % RING
            block = wbuf.at[p, pl.ds(chip_index(p, first, a2) * 2, 2)]
            settle(block, wrecv_sem.at[p * RING + step])
            for offset in (1, 3, 2):
                launch(
                    block,
                    block,
                    wsend_sem.at[p],
                    wrecv_sem.at[p * RING],
                    peer(STRIDES[p][1], offset),
                )

    def put(number, values, first):
        for head in range(values.shape[1] // HEAD):
            vecs[number, :, first + head, :] = values[:, head * HEAD : (head + 1) * HEAD]

    heads = mix // HEAD
    flip = (((1,), (1,)), ((), ()))

    def down(matrix):
        return lax.dot_general(normed, matrix, flip, preferred_element_type=F32)

    decay_low = jnp.tanh(down(decay_down[...])).astype(BF16)
    decay_pre = decay_base[...] + dot(decay_low, decay_up[...])
    put(3, jnp.exp(-jnp.exp(-jax.nn.softplus(-decay_pre) - 0.5)), 0)
    rate_low = down(rate_down[...]).astype(BF16)
    put(4, jax.nn.sigmoid(rate_base[...] + dot(rate_low, rate_up[...])), 0)

    strides = [STRIDES[p % 3] for p in range(SLICES)]
    note = RING * RING * MOST
    plane = RING * RING * count
    every = routes.shape[1]
    entries = old.shape[2]

    def iota(shape, dim):
        return lax.broadcasted_iota(jnp.int32, shape, dim)

    def token_of(p, number):
        first, second_stride, third = strides[p]
        device = (
            spots[p][2] * third
            + core
            + number // (RING * count) * second_stride
            + number // count % RING * first
        )
        return device * count + number % count

    def expert_of(p, number):
        third = strides[p][2]
        return me - spots[p][2] * third - core + number // 2 * third + number % 2

    routes_low = onehot_values(routes[...])
    weights_low = route_weights[...].astype(BF16)
    up_row = iota((plane, plane), 0)
    up_col = iota((plane, plane), 1)
    same = up_row // count == up_col // count
    upper = onehot(same & (up_row < up_col))
    lower = onehot(same & (up_col < up_row))
    slot_row = iota((note, plane), 0)
    slot_col = iota((note, plane), 1)
    wanted = jnp.where(slot_col // count == slot_row // MOST, slot_row % MOST, -2).astype(F32)
    peers = 2 * RING

    def selector(p):
        pick = onehot(iota((every, plane), 0) == token_of(p, iota((every, plane), 1)))
        here = dot(routes_low, pick)
        names = expert_of(p, iota((peers, plane), 0)).astype(F32)
        named = names < 0.0
        for j in range(TOPK):
            named = named | (here[j : j + 1, :] == names)
        before = dot(onehot(named), upper)
        rank = jnp.where(named, before, -1.0)
        parts = [
            onehot(jnp.broadcast_to(rank[i : i + 1, :], (note, plane)) == wanted)
            for i in range(peers)
        ]
        return jnp.concatenate(parts, 0)

    for p in range(3):
        selectors[p] = selector(p)

    fold[...] = onehot(iota((entries, HEAD), 0) // HEAD == iota((entries, HEAD), 1))
    each = RING * note
    turn_row = iota((each, each), 0)
    turn_col = iota((each, each), 1)

    def digits(number):
        return number // 64, number // 16 % 4, number // 4 % 4, number % 4

    def joined(a, b, c, d):
        return ((a * RING + b) * RING + c) * MOST + d

    def orders(number):
        z, y, x, s = digits(number)
        return [None, joined(x, z, y, s), joined(y, x, z, s)]

    def restored(number):
        first, middle, last, s = digits(number)
        return [None, joined(middle, last, first, s), joined(last, first, middle, s)]

    turns = [None] + [onehot(turn_col == orders(turn_row)[p]) for p in (1, 2)]
    returns = [None] + [onehot(turn_col == restored(turn_row)[p]) for p in (1, 2)]

    for p in range(3):
        a1, a2, a3 = spots[p]
        settle(xbuf.at[p, pl.ds(0, 7)], xrecv_sem.at[p])
        settle(wbuf.at[p, pl.ds(0, 25)], wrecv_sem.at[p * RING])
        stacked = xbuf[p].reshape(2 * RING * count, depth)
        part = dot(stacked, wbuf[p].reshape(depth, half)).astype(BF16)
        psend[p] = part.reshape(2 * RING, count, half)
        for offset in (1, 3, 2):
            chip = peer(STRIDES[p][2], offset) - core
            for side in range(2):
                launch(
                    psend.at[p, (a3 + offset) % RING * 2 + side],
                    precv.at[p, a3 * 2 + core],
                    psend_sem.at[p],
                    precv_sem.at[p],
                    chip + side,
                )
        launch(
            psend.at[p, a3 * 2 + 1 - core],
            precv.at[p, a3 * 2 + core],
            psend_sem.at[p],
            precv_sem.at[p],
            partner,
        )
        precv[p, a3 * 2 + core] = psend[p, a3 * 2 + core]

    for p in range(3):
        settle(precv.at[p, pl.ds(0, 7)], precv_sem.at[p])
        for side in range(2):
            added = precv[p, side].astype(F32)
            for which in range(1, RING):
                added = added + precv[p, which * 2 + side].astype(F32)
            added = added.astype(BF16).astype(F32)
            put(p, added, side * (heads // 2))
            if p == 1:
                scale = key_scale[:, side * half : (side + 1) * half]
                put(5, added * scale, side * (heads // 2))

    tall = count * heads
    reader, keys, values, decay, learn, scaled = [vecs[w].reshape(tall, HEAD) for w in range(6)]
    direction = scaled / jnp.sqrt(jnp.sum(scaled * scaled, axis=-1, keepdims=True) + 1.0)
    learned = direction * learn

    def twice(inputs):
        return jnp.concatenate([inputs, inputs], axis=1)

    along = twice(direction)
    reading = twice(decay * reader)
    loads[6].wait()
    cells = [
        old[:, :, lane : lane + 2 * HEAD].reshape(tall, 2 * HEAD)
        for lane in range(0, entries, 2 * HEAD)
    ]
    removed = dot(jnp.concatenate([(c * along).astype(BF16) for c in cells], 1), fold[...])
    readout = dot(jnp.concatenate([(c * reading).astype(BF16) for c in cells], 1), fold[...])
    readout = (
        readout
        - removed * jnp.sum(learned * reader, axis=-1, keepdims=True)
        + values * jnp.sum(keys * reader, axis=-1, keepdims=True)
    )
    centre = jnp.mean(readout, axis=-1, keepdims=True)
    spread = jnp.mean(jnp.square(readout - centre), axis=-1, keepdims=True)
    mixed = (readout - centre) * lax.rsqrt(spread + GROUP_EPS)
    vecs[5] = mixed.reshape(count, heads, HEAD)
    flat = jnp.concatenate([vecs[5, :, head, :] for head in range(heads)], axis=1)
    flat = (flat * head_gain[...]).astype(BF16)
    loads[7].wait()
    after = (tokens[...].astype(F32) + dot(flat, wo[...])).astype(BF16)
    second[...] = rms_scale(after, second_gain[...]).astype(BF16)

    starts = [sum(widths[:p]) for p in range(SLICES)]
    cuts = [slice(starts[p], starts[p] + widths[p]) for p in range(SLICES)]
    mine = [second.at[:, pl.ds(starts[p], widths[p])] for p in range(SLICES)]

    def onward(p, step, source):
        a1, a2, _ = spots[p]
        for offset in (1, 3, 2):
            launch(
                source,
                near[p].at[a2 * RING + (a1 + RING - step) % RING],
                s1.at[p],
                r2.at[p],
                peer(strides[p][1], offset),
            )

    def enter(p):
        a1, a2, _ = spots[p]
        for offset in (1, 3, 2):
            launch(
                mine[p],
                near[p].at[a2 * RING + a1],
                s1.at[p],
                r1.at[p * 3 + offset - 1],
                peer(strides[p][0], offset),
            )

    groups = [range(first, first + 3) for first in range(0, SLICES, 3)]
    for p in groups[0]:
        enter(p)
    for p in groups[0]:
        onward(p, 0, mine[p])
    for group in groups[1:]:
        for p in group:
            enter(p)
    sent = second[...]
    for p in range(SLICES):
        a1, a2, _ = spots[p]
        near[p][a2 * RING + a1] = sent[:, cuts[p]]

    wide_out[0] = twice(decay)
    wide_out[1] = twice(learned)
    wide_out[2] = twice(keys)
    high = removed.astype(BF16)
    low = (removed - high.astype(F32)).astype(BF16)
    low_out[0] = jnp.concatenate([high, low], axis=1)
    low_out[1] = jnp.concatenate([values, jnp.zeros_like(values)], axis=1).astype(BF16)

    for group in groups:
        if group != groups[0]:
            for p in group:
                onward(p, 0, mine[p])
        for offset in (1, 3, 2):
            for p in group:
                a1, a2, _ = spots[p]
                slot = near[p].at[a2 * RING + (a1 + RING - offset) % RING]
                settle(slot, r1.at[p * 3 + offset - 1])
                onward(p, offset, slot)

    for p in range(SLICES):
        a1, a2, a3 = spots[p]
        settle(near[p].at[pl.ds(0, 12)], r2.at[p])
        held = near[p][...].reshape(plane, widths[p])
        picked = dot(selectors[p % 3], held).astype(BF16)
        chosen[p][...] = picked.reshape(peers, note, widths[p])
        for offset in (1, 3, 2):
            chip = peer(strides[p][2], offset) - core
            for side in range(2):
                launch(
                    chosen[p].at[(a3 + offset) % RING * 2 + side],
                    inbox[p].at[core * RING + a3],
                    s3.at[p],
                    r3.at[p],
                    chip + side,
                )
        launch(
            chosen[p].at[a3 * 2 + 1 - core],
            inbox[p].at[core * RING + a3],
            s3.at[p],
            r3.at[p],
            partner,
        )
        inbox[p][core * RING + a3] = chosen[p][a3 * 2 + core]

    turned = (((1,), (1,)), ((), ()))
    tall_row = iota((plane, peers * note), 0)
    tall_col = iota((plane, peers * note), 1)
    expand = onehot(iota((128, peers * note), 0) == iota((128, peers * note), 1) // note)
    wanted_t = jnp.where(
        tall_row // count == tall_col % note // MOST, tall_col % MOST, -2
    ).astype(F32)

    def mixing(p):
        pick = onehot(iota((plane, every), 1) == token_of(p, iota((plane, every), 0)))
        here = lax.dot_general(pick, routes_low, turned, preferred_element_type=F32)
        weigh = lax.dot_general(pick, weights_low, turned, preferred_element_type=F32)
        number = iota((plane, 128), 1)
        names = jnp.where(number < peers, expert_of(p, number), -1).astype(F32)
        named = names < -2.0
        weight = jnp.zeros((plane, 128), F32)
        for j in range(TOPK):
            hit = here[:, j : j + 1] == names
            named = named | hit
            weight = weight + jnp.where(hit, weigh[:, j : j + 1], 0.0)
        before = dot(lower, onehot(named))
        rank = dot(jnp.where(named, before, -1.0).astype(BF16), expand)
        spread = dot(weight.astype(BF16), expand)
        return jnp.where(rank == wanted_t, spread, 0.0).astype(BF16)

    for p in range(3):
        mixers[p] = mixing(p)

    def gated(gate_part, up_part):
        return (jax.nn.silu(gate_part) * up_part).astype(BF16)

    gate_part = None
    up_part = None
    loads[2].wait()
    loads[3].wait()
    for p in range(SLICES):
        settle(inbox[p].at[pl.ds(0, 7)], r3.at[p])
        if p % 3 == 0:
            inputs = inbox[p][...].reshape(2 * each, widths[p])
        else:
            inputs = jnp.concatenate(
                [
                    dot(
                        turns[p % 3],
                        inbox[p][side * RING : (side + 1) * RING].reshape(each, widths[p]),
                    ).astype(BF16)
                    for side in range(2)
                ],
                0,
            )
        gate_more = dot(inputs, eg[cuts[p], :])
        up_more = dot(inputs, eu[cuts[p], :])
        gate_part = gate_more if gate_part is None else gate_part + gate_more
        up_part = up_more if up_part is None else up_part + up_more
    hidden = gated(gate_part, up_part)
    loads[5].wait()

    for p in range(SLICES):
        a3 = spots[p][2]
        if p % 3 == 0:
            inputs = hidden
        else:
            inputs = jnp.concatenate(
                [
                    dot(returns[p % 3], hidden[side * each : (side + 1) * each]).astype(BF16)
                    for side in range(2)
                ],
                0,
            )
        result = dot(inputs, ed[:, cuts[p]]).astype(BF16)
        answer[p][...] = result.reshape(2 * RING, note, widths[p])
        for offset in (1, 3, 2):
            chip = peer(strides[p][2], offset) - core
            for side in range(2):
                launch(
                    answer[p].at[side * RING + (a3 + offset) % RING],
                    back[p].at[a3 * 2 + core],
                    t3.at[p],
                    u3.at[p],
                    chip + side,
                )
        launch(
            answer[p].at[(1 - core) * RING + a3],
            back[p].at[a3 * 2 + core],
            t3.at[p],
            u3.at[p],
            partner,
        )
        back[p][a3 * 2 + core] = answer[p][core * RING + a3]

    loads[0].wait()
    loads[1].wait()
    shared_hidden = gated(dot(sent, sg[...]), dot(sent, su[...]))
    loads[4].wait()
    kept = after.astype(F32) + dot(shared_hidden, sd[...])

    for p in range(SLICES):
        a1, a2, a3 = spots[p]
        settle(back[p].at[pl.ds(0, 7)], u3.at[p])
        summed = dot(mixers[p % 3], back[p][...].reshape(peers * note, widths[p])).astype(BF16)
        total[p][...] = summed.reshape(RING * RING, count, widths[p])
        for offset in (1, 3, 2):
            launch(
                total[p].at[pl.ds((a2 + offset) % RING * RING, RING)],
                gather[p].at[pl.ds(offset * RING, RING)],
                t2.at[p],
                u2.at[p],
                peer(strides[p][1], offset),
            )
    for p in range(SLICES):
        a1, a2, a3 = spots[p]
        summed = total[p][pl.ds(a2 * RING, RING)].astype(F32)
        settle(gather[p].at[pl.ds(RING, 3 * RING)], u2.at[p])
        for offset in (1, 3, 2):
            summed = summed + gather[p][offset * RING : (offset + 1) * RING].astype(F32)
        line[p][...] = summed.astype(BF16)
        for offset in (1, 3, 2):
            launch(
                line[p].at[(a1 + offset) % RING],
                final[p].at[offset],
                t1.at[p],
                u1.at[p],
                peer(strides[p][0], offset),
            )
    for p in range(SLICES):
        a1 = spots[p][0]
        summed = line[p][a1].astype(F32)
        settle(final[p].at[pl.ds(1, 3)], u1.at[p])
        for offset in (1, 3, 2):
            summed = summed + final[p][offset].astype(F32)
        out[:, cuts[p]] = (kept[:, cuts[p]] + summed).astype(BF16)
    for p in range(3):
        settle(wbuf.at[p, pl.ds(0, 31)], wsend_sem.at[p])
        settle(xbuf.at[p, pl.ds(0, 7)], xsend_sem.at[p])
        settle(precv.at[p, pl.ds(0, 7)], psend_sem.at[p])
    for p in range(SLICES):
        settle(near[p].at[pl.ds(0, 15)], s1.at[p])
        settle(inbox[p].at[pl.ds(0, 7)], s3.at[p])
        settle(back[p].at[pl.ds(0, 7)], t3.at[p])
        settle(gather[p].at[pl.ds(0, 3 * RING)], t2.at[p])
        settle(final[p].at[pl.ds(0, 3)], t1.at[p])


def layer(vmems, hbms):
    tokens, routes = vmems[0], vmems[11]
    w_r, state, matrices = hbms[0], hbms[3], hbms[5:]
    count, width = tokens.shape
    rows, mix = w_r.shape
    half = mix // 2
    depth = width // RING
    heads, entries = state.shape[1:]
    widths = part_widths(width)
    vmem = pl.BlockSpec(memory_space=pltpu.VMEM)
    hbm = pl.BlockSpec(memory_space=pl.ANY)
    dma = pltpu.SemaphoreType.DMA
    blocks = RING * RING
    note = blocks * MOST
    plane = blocks * count
    shapes = (
        (RING * RING, count),
        (2 * RING, note),
        (2 * RING, note),
        (2 * RING, note),
        (2 * RING, note),
        (RING * RING, count),
        (RING * RING, count),
        (RING, count),
        (RING, count),
    )
    shapes = [pltpu.VMEM(shape + (w,), BF16) for shape in shapes for w in widths]
    sizes = [8, 3, 3 * RING, 3, 3, 3, 3]
    sizes = sizes + [SLICES * size for size in (1, 3, 1, 1, 1, 1, 1, 1, 1, 1, 1)]
    return pl.pallas_call(
        functools.partial(layer_kernel, widths),
        out_shape=[
            jax.ShapeDtypeStruct((count, width), BF16),
            jax.ShapeDtypeStruct((3, count * heads, 2 * HEAD), F32),
            jax.ShapeDtypeStruct((2, count * heads, 2 * HEAD), BF16),
        ],
        in_specs=[vmem] * len(vmems) + [hbm] * len(hbms),
        out_specs=[vmem] * 3,
        scratch_shapes=[
            pltpu.VMEM((3, 2, rows, half), BF16),
            pltpu.VMEM((3, 2 * RING * RING, rows, half), BF16),
            pltpu.VMEM((3, RING, count, depth), BF16),
            pltpu.VMEM((3, 2 * RING, count, depth), BF16),
            pltpu.VMEM((3, 2 * RING, count, half), BF16),
            pltpu.VMEM((3, 2 * RING, count, half), BF16),
            pltpu.VMEM((6, count, heads, HEAD), F32),
            pltpu.VMEM(state.shape, F32),
            pltpu.VMEM(hbms[4].shape, BF16),
        ]
        + [pltpu.VMEM(m.shape[-2:], BF16) for m in matrices]
        + [
            pltpu.VMEM((entries, HEAD), BF16),
            pltpu.VMEM((count, width), BF16),
            pltpu.VMEM((3, 2 * RING * note, plane), BF16),
            pltpu.VMEM((3, plane, 2 * RING * note), BF16),
        ]
        + shapes
        + [dma]
        + [dma((size,)) for size in sizes],
        compiler_params=pltpu.CompilerParams(
            collective_id=0, has_side_effects=True, vmem_limit_bytes=VMEM_BYTES
        ),
        name="layer",
    )(*vmems, *hbms)


def finish_kernel(wide, low, state, ready, new_state, new_tokens, spread):
    per_step, heads, entries = state.shape
    tall = per_step * heads
    span = 2 * HEAD

    @pl.when(pl.program_id(0) == 0)
    def _():
        row = lax.broadcasted_iota(jnp.int32, (span, entries), 0)
        col = lax.broadcasted_iota(jnp.int32, (span, entries), 1)
        spread[...] = onehot(col // HEAD == row % HEAD)
        new_tokens[...] = ready[...]

    decay, learned, keys = [wide[w] for w in range(3)]
    removed = dot(low[0], spread[...])
    values = dot(low[1], spread[...])
    for lane in range(0, entries, span):
        cut = slice(lane, lane + span)
        fresh = (
            state[:, :, cut].reshape(tall, span) * decay
            - removed[:, cut] * learned
            + values[:, cut] * keys
        )
        new_state[:, :, cut] = fresh.reshape(per_step, heads, span)


def finish(wide, low, state, ready):
    count, heads, entries = state.shape
    per_step = 8 if count % 8 == 0 else 1
    tall = per_step * heads
    span = 2 * HEAD
    block = pl.BlockSpec((per_step, heads, entries), lambda i: (i, 0, 0))
    flat = pl.BlockSpec(ready.shape, lambda i: (0, 0))
    return pl.pallas_call(
        finish_kernel,
        grid=(count // per_step,),
        out_shape=[
            jax.ShapeDtypeStruct(state.shape, F32),
            jax.ShapeDtypeStruct(ready.shape, BF16),
        ],
        in_specs=[
            pl.BlockSpec((3, tall, span), lambda i: (0, i, 0)),
            pl.BlockSpec((2, tall, span), lambda i: (0, i, 0)),
            block,
            flat,
        ],
        out_specs=[block, flat],
        scratch_shapes=[pltpu.VMEM((span, entries), BF16)],
        compiler_params=pltpu.CompilerParams(
            dimension_semantics=("arbitrary",), vmem_limit_bytes=VMEM_BYTES
        ),
        name="finish",
    )(wide, low, state, ready)


def per_device(
    tokens,
    recurrent_state,
    first_gain,
    w_receptance,
    w_key,
    w_value,
    decay_down,
    decay_up,
    decay_base,
    rate_down,
    rate_up,
    rate_base,
    key_scale,
    head_gain,
    w_output,
    second_gain,
    shared_gate,
    shared_up,
    shared_down,
    expert_gate,
    expert_up,
    expert_down,
    routes,
    route_weights,
):
    vmems = (
        tokens,
        first_gain[None, :],
        decay_down.T,
        decay_up,
        decay_base[None, :],
        rate_down.T,
        rate_up,
        rate_base[None, :],
        key_scale[None, :],
        head_gain[None, :],
        second_gain[None, :],
        routes.T,
        route_weights.T,
    )
    hbms = (
        w_receptance,
        w_key,
        w_value,
        recurrent_state,
        w_output,
        shared_gate,
        shared_up,
        shared_down,
        expert_gate,
        expert_up,
        expert_down,
    )
    ready, wide, low = layer(vmems, hbms)
    new_state, new_tokens = finish(wide, low, recurrent_state, ready)
    return (new_tokens, new_state)


def solution(mesh):
    in_specs = (
        P("ep", None),
        P("ep", None, None),
        P(),
        P("ep", None),
        P("ep", None),
        P("ep", None),
        P(),
        P(),
        P(),
        P(),
        P(),
        P(),
        P(),
        P(),
        P(),
        P(),
        P(),
        P(),
        P(),
        P("ep", None, None),
        P("ep", None, None),
        P("ep", None, None),
        P(),
        P(),
    )
    out_specs = (P("ep", None), P("ep", None, None))
    return jax.shard_map(
        per_device, mesh=mesh, in_specs=in_specs, out_specs=out_specs, check_vma=False
    )
```

```python
import functools

import jax
import jax.numpy as jnp
from jax import lax
from jax.experimental import pallas as pl
from jax.experimental.pallas import tpu as pltpu
from jax.sharding import PartitionSpec as P

HEAD = 64
TOPK = 4
MOST = 4
RING = 4
SLICES = 6
STRIDES = ((2, 8, 32), (8, 32, 2), (32, 2, 8))
NORM_EPS = 1e-06
GROUP_EPS = 0.00064
MESH = pl.DeviceIdType.MESH
F32 = jnp.float32
BF16 = jnp.bfloat16
VMEM_BYTES = 60 * 1024 * 1024


def dot(a, b):
    return jnp.dot(a, b, preferred_element_type=F32)


def rms_scale(inputs, gain):
    widened = inputs.astype(F32)
    return (
        widened * lax.rsqrt(jnp.mean(widened * widened, axis=-1, keepdims=True) + NORM_EPS) * gain
    )


def onehot(flags):
    return flags.astype(F32).astype(BF16)


def onehot_values(values):
    return values.astype(F32).astype(BF16)


def part_widths(width):
    tiles = width // 128
    counts = [tiles // SLICES + (1 if number < tiles % SLICES else 0) for number in range(SLICES)]
    return [number * 128 for number in counts]


def layer_kernel(widths, small, *refs):
    given = refs[:small]
    (
        w_r,
        w_k,
        w_v,
        state,
        w_output,
        shared_gate,
        shared_up,
        shared_down,
        expert_gate,
        expert_up,
        expert_down,
        out,
        wide_out,
        low_out,
        stage,
        wbuf,
        nsend,
        xbuf,
        psend,
        precv,
        vecs,
        old,
        wo,
        sg,
        su,
        sd,
        eg,
        eu,
        ed,
        fold,
        second,
        selectors,
        mixers,
    ) = refs[small : small + 33]
    rest = refs[small + 33 + small :]
    held = refs[small + 33 : small + 33 + small]
    (
        tokens,
        gain,
        decay_down,
        decay_up,
        decay_base,
        rate_down,
        rate_up,
        rate_base,
        key_scale,
        head_gain,
        second_gain,
        routes,
        route_weights,
    ) = held
    near, chosen, inbox, answer, back, total, gather, line, final = [
        rest[SLICES * i : SLICES * (i + 1)] for i in range(9)
    ]
    local_sem, load_sem, small_sem = rest[9 * SLICES : 9 * SLICES + 3]
    wide_buf, low_buf, out_sem = rest[-3:]
    wrecv_sem, xrecv_sem, precv_sem = rest[9 * SLICES + 3 : 9 * SLICES + 6]
    wsend_sem, psend_sem, esend_sem, rsend_sem = rest[9 * SLICES + 6 : 9 * SLICES + 10]
    r1, r2, r3, u3, u2, u1 = rest[9 * SLICES + 10 : -3]
    rows, mix = w_r.shape
    half = mix // 2
    count, width = tokens.shape
    pair = 2 * rows
    depth = width // RING
    me = lax.axis_index("ep")
    core = me % 2
    partner = me + 1 - 2 * core

    def place(stride):
        return (me // stride) % RING

    def peer(stride, offset):
        return me + ((place(stride) + offset) % RING - place(stride)) * stride

    spots = [[place(stride) for stride in STRIDES[p % 3]] for p in range(SLICES)]
    barrier = pltpu.get_barrier_semaphore()
    greet = [partner]
    for stride in STRIDES[0]:
        for offset in range(1, RING):
            mate = peer(stride, offset)
            greet = greet + [mate, mate + 1 - 2 * core]
    for mate in greet:
        pl.semaphore_signal(barrier, inc=1, device_id=(mate,), device_id_type=MESH)
    intake = [
        pltpu.make_async_copy(source, target, small_sem.at[number])
        for number, (source, target) in enumerate(zip(given, held))
    ]
    for copy in intake[:2]:
        copy.start()
    local = []
    for p, weight in enumerate((w_r, w_k, w_v)):
        for side in range(2):
            local.append(
                pltpu.make_async_copy(
                    weight.at[:, pl.ds(side * half, half)],
                    stage.at[p, side],
                    local_sem,
                )
            )
    for copy in local:
        copy.start()
    for copy in intake[2:]:
        copy.start()
    loads = [
        pltpu.make_async_copy(source, target, load_sem.at[number])
        for number, (source, target) in enumerate(
            (
                (shared_gate, sg),
                (shared_up, su),
                (expert_gate.at[0], eg),
                (expert_up.at[0], eu),
                (shared_down, sd),
                (expert_down.at[0], ed),
                (state, old),
                (w_output, wo),
            )
        )
    ]
    for copy in intake[:2]:
        copy.wait()
    normed = rms_scale(tokens[...], gain[...]).astype(BF16)
    for q in range(RING):
        nsend[0, q] = normed[:, q * depth : (q + 1) * depth]
        chunks = [z * depth + y * RING * pair + q * pair for z in range(RING) for y in range(RING)]
        nsend[1, q] = jnp.concatenate([normed[:, s : s + pair] for s in chunks], axis=1)
        chunks = [z * depth + q * RING * pair for z in range(RING)]
        nsend[2, q] = jnp.concatenate([normed[:, s : s + RING * pair] for s in chunks], axis=1)
    def remote(source, target, send, receive, device):
        return pltpu.make_async_remote_copy(
            src_ref=source,
            dst_ref=target,
            send_sem=send,
            recv_sem=receive,
            device_id=(device,),
            device_id_type=MESH,
        )

    def launch(*args):
        remote(*args).start()

    def settle(view, semaphore):
        remote(view, view, semaphore, semaphore, partner).wait_recv()

    def chip_index(p, first, second):
        return first * RING + second if p == 2 else second * RING + first

    def row_slot(p, first, second, which):
        return wbuf.at[p, chip_index(p, first, second) * 2 + which]

    settle(stage, local_sem)
    pl.semaphore_wait(barrier, len(greet))

    for p in range(3):
        a1, a2, _ = spots[p]
        for offset in (1, 3, 2):
            chip = peer(STRIDES[p][0], offset) - core
            for side in range(2):
                launch(
                    stage.at[p, side],
                    row_slot(p, a1, a2, core),
                    wsend_sem,
                    wrecv_sem.at[p * RING + offset],
                    chip + side,
                )
        launch(
            stage.at[p, 1 - core],
            row_slot(p, a1, a2, core),
            wsend_sem,
            wrecv_sem.at[p * RING],
            partner,
        )
    for p in range(3):
        a1, a2, _ = spots[p]
        for offset in (1, 3, 2):
            chip = peer(STRIDES[p][1], offset) - core
            for side in range(2):
                launch(
                    stage.at[p, side],
                    row_slot(p, a1, a2, core),
                    wsend_sem,
                    wrecv_sem.at[p * RING],
                    chip + side,
                )
    for p in range(3):
        a3 = spots[p][2]
        for offset in (1, 3, 2):
            chip = peer(STRIDES[p][2], offset) - core
            for side in range(2):
                launch(
                    nsend.at[p, (a3 + offset) % RING],
                    xbuf.at[p, a3 * 2 + core],
                    wsend_sem,
                    xrecv_sem.at[p],
                    chip + side,
                )
        launch(
            nsend.at[p, a3],
            xbuf.at[p, a3 * 2 + core],
            wsend_sem,
            xrecv_sem.at[p],
            partner,
        )
    for p in range(3):
        a1, a2, a3 = spots[p]
        own = stage[p, core]
        wbuf[p, chip_index(p, a1, a2) * 2 + core] = own
        xbuf[p, a3 * 2 + core] = nsend[p, a3]

    for number in (6, 7, 2, 3, 5, 0, 1, 4):
        loads[number].start()

    for step in (1, 3, 2):
        for p in range(3):
            a1, a2, _ = spots[p]
            first = (a1 + RING - step) % RING
            block = wbuf.at[p, pl.ds(chip_index(p, first, a2) * 2, 2)]
            settle(block, wrecv_sem.at[p * RING + step])
            for offset in (1, 3, 2):
                launch(
                    block,
                    block,
                    wsend_sem,
                    wrecv_sem.at[p * RING],
                    peer(STRIDES[p][1], offset),
                )

    for copy in intake[2:]:
        copy.wait()

    def put(number, values, first):
        for head in range(values.shape[1] // HEAD):
            vecs[number, :, first + head, :] = values[:, head * HEAD : (head + 1) * HEAD]

    heads = mix // HEAD
    flip = (((1,), (1,)), ((), ()))

    def down(matrix):
        return lax.dot_general(normed, matrix, flip, preferred_element_type=F32)

    decay_low = jnp.tanh(down(decay_down[...])).astype(BF16)
    decay_pre = decay_base[...] + dot(decay_low, decay_up[...])
    put(3, jnp.exp(-jnp.exp(-jax.nn.softplus(-decay_pre) - 0.5)), 0)
    rate_low = down(rate_down[...]).astype(BF16)
    put(4, jax.nn.sigmoid(rate_base[...] + dot(rate_low, rate_up[...])), 0)

    strides = [STRIDES[p % 3] for p in range(SLICES)]
    note = RING * RING * MOST
    plane = RING * RING * count
    every = routes.shape[1]
    entries = old.shape[2]

    def iota(shape, dim):
        return lax.broadcasted_iota(jnp.int32, shape, dim)

    def token_of(p, number):
        first, second_stride, third = strides[p]
        device = (
            spots[p][2] * third
            + core
            + number // (RING * count) * second_stride
            + number // count % RING * first
        )
        return device * count + number % count

    def expert_of(p, number):
        third = strides[p][2]
        return me - spots[p][2] * third - core + number // 2 * third + number % 2

    routes_low = onehot_values(routes[...])
    weights_low = route_weights[...].astype(BF16)
    up_row = iota((plane, plane), 0)
    up_col = iota((plane, plane), 1)
    same = up_row // count == up_col // count
    upper = onehot(same & (up_row < up_col))
    lower = onehot(same & (up_col < up_row))
    slot_row = iota((note, plane), 0)
    slot_col = iota((note, plane), 1)
    wanted = jnp.where(slot_col // count == slot_row // MOST, slot_row % MOST, -2).astype(F32)
    peers = 2 * RING

    def selector(p):
        pick = onehot(iota((every, plane), 0) == token_of(p, iota((every, plane), 1)))
        here = dot(routes_low, pick)
        names = expert_of(p, iota((peers, plane), 0)).astype(F32)
        named = names < 0.0
        for j in range(TOPK):
            named = named | (here[j : j + 1, :] == names)
        before = dot(onehot(named), upper)
        rank = jnp.where(named, before, -1.0)
        parts = [
            onehot(jnp.broadcast_to(rank[i : i + 1, :], (note, plane)) == wanted)
            for i in range(peers)
        ]
        return jnp.concatenate(parts, 0)

    for p in range(3):
        selectors[p] = selector(p)

    fold[...] = onehot(iota((entries, HEAD), 0) // HEAD == iota((entries, HEAD), 1))
    each = RING * note
    turn_row = iota((each, each), 0)
    turn_col = iota((each, each), 1)

    def digits(number):
        return number // 64, number // 16 % 4, number // 4 % 4, number % 4

    def joined(a, b, c, d):
        return ((a * RING + b) * RING + c) * MOST + d

    def orders(number):
        z, y, x, s = digits(number)
        return [None, joined(x, z, y, s), joined(y, x, z, s)]

    def restored(number):
        first, middle, last, s = digits(number)
        return [None, joined(middle, last, first, s), joined(last, first, middle, s)]

    turns = [None] + [onehot(turn_col == orders(turn_row)[p]) for p in (1, 2)]
    returns = [None] + [onehot(turn_col == restored(turn_row)[p]) for p in (1, 2)]

    for p in range(3):
        a1, a2, a3 = spots[p]
        settle(xbuf.at[p, pl.ds(0, 7)], xrecv_sem.at[p])
        settle(wbuf.at[p, pl.ds(0, 25)], wrecv_sem.at[p * RING])
        stacked = xbuf[p].reshape(2 * RING * count, depth)
        part = dot(stacked, wbuf[p].reshape(depth, half)).astype(BF16)
        psend[p] = part.reshape(2 * RING, count, half)
        for offset in (1, 3, 2):
            chip = peer(STRIDES[p][2], offset) - core
            for side in range(2):
                launch(
                    psend.at[p, (a3 + offset) % RING * 2 + side],
                    precv.at[p, a3 * 2 + core],
                    psend_sem,
                    precv_sem.at[p],
                    chip + side,
                )
        launch(
            psend.at[p, a3 * 2 + 1 - core],
            precv.at[p, a3 * 2 + core],
            psend_sem,
            precv_sem.at[p],
            partner,
        )
        precv[p, a3 * 2 + core] = psend[p, a3 * 2 + core]

    for p in range(3):
        settle(precv.at[p, pl.ds(0, 7)], precv_sem.at[p])
        for side in range(2):
            added = precv[p, side].astype(F32)
            for which in range(1, RING):
                added = added + precv[p, which * 2 + side].astype(F32)
            added = added.astype(BF16).astype(F32)
            put(p, added, side * (heads // 2))
            if p == 1:
                scale = key_scale[:, side * half : (side + 1) * half]
                put(5, added * scale, side * (heads // 2))

    tall = count * heads
    reader, keys, values, decay, learn, scaled = [vecs[w].reshape(tall, HEAD) for w in range(6)]
    direction = scaled / jnp.sqrt(jnp.sum(scaled * scaled, axis=-1, keepdims=True) + 1.0)
    learned = direction * learn

    def twice(inputs):
        return jnp.concatenate([inputs, inputs], axis=1)

    along = twice(direction)
    reading = twice(decay * reader)
    loads[6].wait()
    cells = [
        old[:, :, lane : lane + 2 * HEAD].reshape(tall, 2 * HEAD)
        for lane in range(0, entries, 2 * HEAD)
    ]
    removed = dot(jnp.concatenate([(c * along).astype(BF16) for c in cells], 1), fold[...])
    readout = dot(jnp.concatenate([(c * reading).astype(BF16) for c in cells], 1), fold[...])
    readout = (
        readout
        - removed * jnp.sum(learned * reader, axis=-1, keepdims=True)
        + values * jnp.sum(keys * reader, axis=-1, keepdims=True)
    )
    centre = jnp.mean(readout, axis=-1, keepdims=True)
    spread = jnp.mean(jnp.square(readout - centre), axis=-1, keepdims=True)
    mixed = (readout - centre) * lax.rsqrt(spread + GROUP_EPS)
    vecs[5] = mixed.reshape(count, heads, HEAD)
    flat = jnp.concatenate([vecs[5, :, head, :] for head in range(heads)], axis=1)
    flat = (flat * head_gain[...]).astype(BF16)
    loads[7].wait()
    after = (tokens[...].astype(F32) + dot(flat, wo[...])).astype(BF16)
    second[...] = rms_scale(after, second_gain[...]).astype(BF16)

    starts = [sum(widths[:p]) for p in range(SLICES)]
    cuts = [slice(starts[p], starts[p] + widths[p]) for p in range(SLICES)]
    mine = [second.at[:, pl.ds(starts[p], widths[p])] for p in range(SLICES)]

    def onward(p, step, source):
        a1, a2, _ = spots[p]
        for offset in (1, 3, 2):
            launch(
                source,
                near[p].at[a2 * RING + (a1 + RING - step) % RING],
                esend_sem,
                r2.at[p],
                peer(strides[p][1], offset),
            )

    def enter(p):
        a1, a2, _ = spots[p]
        for offset in (1, 3, 2):
            launch(
                mine[p],
                near[p].at[a2 * RING + a1],
                esend_sem,
                r1.at[p * 3 + offset - 1],
                peer(strides[p][0], offset),
            )

    groups = [range(first, first + 3) for first in range(0, SLICES, 3)]
    for p in groups[0]:
        enter(p)
    for p in groups[0]:
        onward(p, 0, mine[p])
    for group in groups[1:]:
        for p in group:
            enter(p)
    sent = second[...]
    for p in range(SLICES):
        a1, a2, _ = spots[p]
        near[p][a2 * RING + a1] = sent[:, cuts[p]]

    wide_buf[0] = twice(decay)
    wide_buf[1] = twice(learned)
    wide_buf[2] = twice(keys)
    high = removed.astype(BF16)
    low = (removed - high.astype(F32)).astype(BF16)
    low_buf[0] = jnp.concatenate([high, low], axis=1)
    low_buf[1] = jnp.concatenate([values, jnp.zeros_like(values)], axis=1).astype(BF16)
    outward = [
        pltpu.make_async_copy(wide_buf, wide_out, out_sem.at[0]),
        pltpu.make_async_copy(low_buf, low_out, out_sem.at[1]),
    ]
    for copy in outward:
        copy.start()

    for group in groups:
        if group != groups[0]:
            for p in group:
                onward(p, 0, mine[p])
        for offset in (1, 3, 2):
            for p in group:
                a1, a2, _ = spots[p]
                slot = near[p].at[a2 * RING + (a1 + RING - offset) % RING]
                settle(slot, r1.at[p * 3 + offset - 1])
                onward(p, offset, slot)

    for p in range(SLICES):
        a1, a2, a3 = spots[p]
        settle(near[p].at[pl.ds(0, 12)], r2.at[p])
        held = near[p][...].reshape(plane, widths[p])
        picked = dot(selectors[p % 3], held).astype(BF16)
        chosen[p][...] = picked.reshape(peers, note, widths[p])
        for offset in (1, 3, 2):
            chip = peer(strides[p][2], offset) - core
            for side in range(2):
                launch(
                    chosen[p].at[(a3 + offset) % RING * 2 + side],
                    inbox[p].at[core * RING + a3],
                    esend_sem,
                    r3.at[p],
                    chip + side,
                )
        launch(
            chosen[p].at[a3 * 2 + 1 - core],
            inbox[p].at[core * RING + a3],
            esend_sem,
            r3.at[p],
            partner,
        )
        inbox[p][core * RING + a3] = chosen[p][a3 * 2 + core]

    turned = (((1,), (1,)), ((), ()))
    tall_row = iota((plane, peers * note), 0)
    tall_col = iota((plane, peers * note), 1)
    expand = onehot(iota((128, peers * note), 0) == iota((128, peers * note), 1) // note)
    wanted_t = jnp.where(
        tall_row // count == tall_col % note // MOST, tall_col % MOST, -2
    ).astype(F32)

    def mixing(p):
        pick = onehot(iota((plane, every), 1) == token_of(p, iota((plane, every), 0)))
        here = lax.dot_general(pick, routes_low, turned, preferred_element_type=F32)
        weigh = lax.dot_general(pick, weights_low, turned, preferred_element_type=F32)
        number = iota((plane, 128), 1)
        names = jnp.where(number < peers, expert_of(p, number), -1).astype(F32)
        named = names < -2.0
        weight = jnp.zeros((plane, 128), F32)
        for j in range(TOPK):
            hit = here[:, j : j + 1] == names
            named = named | hit
            weight = weight + jnp.where(hit, weigh[:, j : j + 1], 0.0)
        before = dot(lower, onehot(named))
        rank = dot(jnp.where(named, before, -1.0).astype(BF16), expand)
        spread = dot(weight.astype(BF16), expand)
        return jnp.where(rank == wanted_t, spread, 0.0).astype(BF16)

    for p in range(3):
        mixers[p] = mixing(p)

    def gated(gate_part, up_part):
        return (jax.nn.silu(gate_part) * up_part).astype(BF16)

    gate_part = None
    up_part = None
    loads[2].wait()
    loads[3].wait()
    for p in range(SLICES):
        settle(inbox[p].at[pl.ds(0, 7)], r3.at[p])
        if p % 3 == 0:
            inputs = inbox[p][...].reshape(2 * each, widths[p])
        else:
            inputs = jnp.concatenate(
                [
                    dot(
                        turns[p % 3],
                        inbox[p][side * RING : (side + 1) * RING].reshape(each, widths[p]),
                    ).astype(BF16)
                    for side in range(2)
                ],
                0,
            )
        gate_more = dot(inputs, eg[cuts[p], :])
        up_more = dot(inputs, eu[cuts[p], :])
        gate_part = gate_more if gate_part is None else gate_part + gate_more
        up_part = up_more if up_part is None else up_part + up_more
    hidden = gated(gate_part, up_part)
    loads[5].wait()

    for p in range(SLICES):
        a3 = spots[p][2]
        if p % 3 == 0:
            inputs = hidden
        else:
            inputs = jnp.concatenate(
                [
                    dot(returns[p % 3], hidden[side * each : (side + 1) * each]).astype(BF16)
                    for side in range(2)
                ],
                0,
            )
        result = dot(inputs, ed[:, cuts[p]]).astype(BF16)
        answer[p][...] = result.reshape(2 * RING, note, widths[p])
        for offset in (1, 3, 2):
            chip = peer(strides[p][2], offset) - core
            for side in range(2):
                launch(
                    answer[p].at[side * RING + (a3 + offset) % RING],
                    back[p].at[a3 * 2 + core],
                    rsend_sem,
                    u3.at[p],
                    chip + side,
                )
        launch(
            answer[p].at[(1 - core) * RING + a3],
            back[p].at[a3 * 2 + core],
            rsend_sem,
            u3.at[p],
            partner,
        )
        back[p][a3 * 2 + core] = answer[p][core * RING + a3]

    loads[0].wait()
    loads[1].wait()
    shared_hidden = gated(dot(sent, sg[...]), dot(sent, su[...]))
    loads[4].wait()
    kept = after.astype(F32) + dot(shared_hidden, sd[...])

    for p in range(SLICES):
        a1, a2, a3 = spots[p]
        settle(back[p].at[pl.ds(0, 7)], u3.at[p])
        summed = dot(mixers[p % 3], back[p][...].reshape(peers * note, widths[p])).astype(BF16)
        total[p][...] = summed.reshape(RING * RING, count, widths[p])
        for offset in (1, 3, 2):
            launch(
                total[p].at[pl.ds((a2 + offset) % RING * RING, RING)],
                gather[p].at[pl.ds(offset * RING, RING)],
                rsend_sem,
                u2.at[p],
                peer(strides[p][1], offset),
            )
    for p in range(SLICES):
        a1, a2, a3 = spots[p]
        summed = total[p][pl.ds(a2 * RING, RING)].astype(F32)
        settle(gather[p].at[pl.ds(RING, 3 * RING)], u2.at[p])
        for offset in (1, 3, 2):
            summed = summed + gather[p][offset * RING : (offset + 1) * RING].astype(F32)
        line[p][...] = summed.astype(BF16)
        for offset in (1, 3, 2):
            launch(
                line[p].at[(a1 + offset) % RING],
                final[p].at[offset],
                rsend_sem,
                u1.at[p],
                peer(strides[p][0], offset),
            )
    for p in range(SLICES):
        a1 = spots[p][0]
        summed = line[p][a1].astype(F32)
        settle(final[p].at[pl.ds(1, 3)], u1.at[p])
        for offset in (1, 3, 2):
            summed = summed + final[p][offset].astype(F32)
        out[:, cuts[p]] = (kept[:, cuts[p]] + summed).astype(BF16)
    sent_units = (3 * (31 + 7), 3 * 7)
    settle(eg.at[pl.ds(0, sent_units[0] * rows)], wsend_sem)
    settle(eg.at[pl.ds(0, sent_units[1] * rows)], psend_sem)
    settle(wo.at[pl.ds(0, (15 + 7 * RING) * count)], esend_sem)
    settle(wo.at[pl.ds(0, (15 + 7 * RING) * count)], rsend_sem)
    for copy in outward:
        copy.wait()


def layer(vmems, hbms):
    tokens, routes = vmems[0], vmems[11]
    w_r, state, matrices = hbms[0], hbms[3], hbms[5:]
    count, width = tokens.shape
    rows, mix = w_r.shape
    half = mix // 2
    depth = width // RING
    heads, entries = state.shape[1:]
    widths = part_widths(width)
    vmem = pl.BlockSpec(memory_space=pltpu.VMEM)
    hbm = pl.BlockSpec(memory_space=pl.ANY)
    dma = pltpu.SemaphoreType.DMA
    blocks = RING * RING
    note = blocks * MOST
    plane = blocks * count
    shapes = (
        (RING * RING, count),
        (2 * RING, note),
        (2 * RING, note),
        (2 * RING, note),
        (2 * RING, note),
        (RING * RING, count),
        (RING * RING, count),
        (RING, count),
        (RING, count),
    )
    shapes = [pltpu.VMEM(shape + (w,), BF16) for shape in shapes for w in widths]
    sizes = [8, len(vmems), 3 * RING, 3, 3]
    later = [SLICES * size for size in (3, 1, 1, 1, 1, 1)]
    return pl.pallas_call(
        functools.partial(layer_kernel, widths, len(vmems)),
        out_shape=[
            jax.ShapeDtypeStruct((count, width), BF16),
            jax.ShapeDtypeStruct((3, count * heads, 2 * HEAD), F32),
            jax.ShapeDtypeStruct((2, count * heads, 2 * HEAD), BF16),
        ],
        in_specs=[hbm] * (len(vmems) + len(hbms)),
        out_specs=[vmem, hbm, hbm],
        scratch_shapes=[
            pltpu.VMEM((3, 2, rows, half), BF16),
            pltpu.VMEM((3, 2 * RING * RING, rows, half), BF16),
            pltpu.VMEM((3, RING, count, depth), BF16),
            pltpu.VMEM((3, 2 * RING, count, depth), BF16),
            pltpu.VMEM((3, 2 * RING, count, half), BF16),
            pltpu.VMEM((3, 2 * RING, count, half), BF16),
            pltpu.VMEM((6, count, heads, HEAD), F32),
            pltpu.VMEM(state.shape, F32),
            pltpu.VMEM(hbms[4].shape, BF16),
        ]
        + [pltpu.VMEM(m.shape[-2:], BF16) for m in matrices]
        + [
            pltpu.VMEM((entries, HEAD), BF16),
            pltpu.VMEM((count, width), BF16),
            pltpu.VMEM((3, 2 * RING * note, plane), BF16),
            pltpu.VMEM((3, plane, 2 * RING * note), BF16),
        ]
        + [pltpu.VMEM(small.shape, small.dtype) for small in vmems]
        + shapes
        + [dma]
        + [dma((size,)) for size in sizes]
        + [dma] * 4
        + [dma((size,)) for size in later]
        + [
            pltpu.VMEM((3, count * heads, 2 * HEAD), F32),
            pltpu.VMEM((2, count * heads, 2 * HEAD), BF16),
            dma((2,)),
        ],
        compiler_params=pltpu.CompilerParams(
            collective_id=0, has_side_effects=True, vmem_limit_bytes=VMEM_BYTES
        ),
        name="layer",
    )(*vmems, *hbms)


def finish_kernel(wide, low, state, ready, new_state, new_tokens, spread):
    per_step, heads, entries = state.shape
    tall = per_step * heads
    span = 2 * HEAD

    @pl.when(pl.program_id(0) == 0)
    def _():
        row = lax.broadcasted_iota(jnp.int32, (span, entries), 0)
        col = lax.broadcasted_iota(jnp.int32, (span, entries), 1)
        spread[...] = onehot(col // HEAD == row % HEAD)
        new_tokens[...] = ready[...]

    decay, learned, keys = [wide[w] for w in range(3)]
    removed = dot(low[0], spread[...])
    values = dot(low[1], spread[...])
    for lane in range(0, entries, span):
        cut = slice(lane, lane + span)
        fresh = (
            state[:, :, cut].reshape(tall, span) * decay
            - removed[:, cut] * learned
            + values[:, cut] * keys
        )
        new_state[:, :, cut] = fresh.reshape(per_step, heads, span)


def finish(wide, low, state, ready):
    count, heads, entries = state.shape
    per_step = 8 if count % 8 == 0 else 1
    tall = per_step * heads
    span = 2 * HEAD
    block = pl.BlockSpec((per_step, heads, entries), lambda i: (i, 0, 0))
    flat = pl.BlockSpec(ready.shape, lambda i: (0, 0))
    return pl.pallas_call(
        finish_kernel,
        grid=(count // per_step,),
        out_shape=[
            jax.ShapeDtypeStruct(state.shape, F32),
            jax.ShapeDtypeStruct(ready.shape, BF16),
        ],
        in_specs=[
            pl.BlockSpec((3, tall, span), lambda i: (0, i, 0)),
            pl.BlockSpec((2, tall, span), lambda i: (0, i, 0)),
            block,
            flat,
        ],
        out_specs=[block, flat],
        scratch_shapes=[pltpu.VMEM((span, entries), BF16)],
        compiler_params=pltpu.CompilerParams(
            dimension_semantics=("arbitrary",), vmem_limit_bytes=VMEM_BYTES
        ),
        name="finish",
    )(wide, low, state, ready)


def per_device(
    tokens,
    recurrent_state,
    first_gain,
    w_receptance,
    w_key,
    w_value,
    decay_down,
    decay_up,
    decay_base,
    rate_down,
    rate_up,
    rate_base,
    key_scale,
    head_gain,
    w_output,
    second_gain,
    shared_gate,
    shared_up,
    shared_down,
    expert_gate,
    expert_up,
    expert_down,
    routes,
    route_weights,
):
    vmems = (
        tokens,
        first_gain[None, :],
        decay_down.T,
        decay_up,
        decay_base[None, :],
        rate_down.T,
        rate_up,
        rate_base[None, :],
        key_scale[None, :],
        head_gain[None, :],
        second_gain[None, :],
        routes.T,
        route_weights.T,
    )
    hbms = (
        w_receptance,
        w_key,
        w_value,
        recurrent_state,
        w_output,
        shared_gate,
        shared_up,
        shared_down,
        expert_gate,
        expert_up,
        expert_down,
    )
    ready, wide, low = layer(vmems, hbms)
    new_state, new_tokens = finish(wide, low, recurrent_state, ready)
    return (new_tokens, new_state)


def solution(mesh):
    in_specs = (
        P("ep", None),
        P("ep", None, None),
        P(),
        P("ep", None),
        P("ep", None),
        P("ep", None),
        P(),
        P(),
        P(),
        P(),
        P(),
        P(),
        P(),
        P(),
        P(),
        P(),
        P(),
        P(),
        P(),
        P("ep", None, None),
        P("ep", None, None),
        P("ep", None, None),
        P(),
        P(),
    )
    out_specs = (P("ep", None), P("ep", None, None))
    return jax.shard_map(
        per_device, mesh=mesh, in_specs=in_specs, out_specs=out_specs, check_vma=False
    )
```

```python
import functools

import jax
import jax.numpy as jnp
from jax import lax
from jax.experimental import pallas as pl
from jax.experimental.pallas import tpu as pltpu
from jax.sharding import PartitionSpec as P

HEAD = 64
TOPK = 4
MOST = 4
RING = 4
SLICES = 7
STRIDES = ((2, 8, 32), (8, 32, 2), (32, 2, 8))
NORM_EPS = 1e-06
GROUP_EPS = 0.00064
MESH = pl.DeviceIdType.MESH
F32 = jnp.float32
BF16 = jnp.bfloat16
VMEM_BYTES = 60 * 1024 * 1024


def dot(a, b):
    return jnp.dot(a, b, preferred_element_type=F32)


def rms_scale(inputs, gain):
    widened = inputs.astype(F32)
    return (
        widened * lax.rsqrt(jnp.mean(widened * widened, axis=-1, keepdims=True) + NORM_EPS) * gain
    )


def onehot(flags):
    return flags.astype(F32).astype(BF16)


def onehot_values(values):
    return values.astype(F32).astype(BF16)


def part_widths(width):
    tiles = width // 128
    even = tiles // 3
    counts = [even - even // 2] * 3 + [even // 2] * 3 + [tiles - 3 * even]
    return [number * 128 for number in counts]


def layer_kernel(widths, small, *refs):
    given = refs[:small]
    (
        w_r,
        w_k,
        w_v,
        state,
        w_output,
        shared_gate,
        shared_up,
        shared_down,
        expert_gate,
        expert_up,
        expert_down,
        out,
        wide_out,
        low_out,
        stage,
        wbuf,
        nsend,
        xbuf,
        psend,
        precv,
        vecs,
        old,
        wo,
        sg,
        su,
        sd,
        eg,
        eu,
        ed,
        fold,
        second,
        selectors,
        mixers,
    ) = refs[small : small + 33]
    rest = refs[small + 33 + small :]
    held = refs[small + 33 : small + 33 + small]
    (
        tokens,
        gain,
        decay_down,
        decay_up,
        decay_base,
        rate_down,
        rate_up,
        rate_base,
        key_scale,
        head_gain,
        second_gain,
        routes,
        route_weights,
    ) = held
    near, chosen, inbox, answer, back, total, gather, line, final = [
        rest[SLICES * i : SLICES * (i + 1)] for i in range(9)
    ]
    local_sem, load_sem, small_sem = rest[9 * SLICES : 9 * SLICES + 3]
    wide_buf, low_buf, out_sem = rest[-3:]
    wrecv_sem, xrecv_sem, precv_sem = rest[9 * SLICES + 3 : 9 * SLICES + 6]
    wsend_sem, psend_sem, esend_sem, rsend_sem = rest[9 * SLICES + 6 : 9 * SLICES + 10]
    r1, r2, r3, u3, u2, u1 = rest[9 * SLICES + 10 : -3]
    rows, mix = w_r.shape
    half = mix // 2
    count, width = tokens.shape
    pair = 2 * rows
    depth = width // RING
    me = lax.axis_index("ep")
    core = me % 2
    partner = me + 1 - 2 * core

    def place(stride):
        return (me // stride) % RING

    def peer(stride, offset):
        return me + ((place(stride) + offset) % RING - place(stride)) * stride

    spots = [[place(stride) for stride in STRIDES[p % 3]] for p in range(6)]
    spots = spots + [[spots[0][i] + core * (spots[1][i] - spots[0][i]) for i in range(3)]]

    def hop(p, level, offset):
        mate = peer(STRIDES[p % 3][level], offset)
        return mate if p < 6 else mate + core * (peer(STRIDES[1][level], offset) - mate)

    def order_of(p):
        return p % 3 if p < 6 else core
    barrier = pltpu.get_barrier_semaphore()
    greet = [partner]
    for stride in STRIDES[0]:
        for offset in range(1, RING):
            mate = peer(stride, offset)
            greet = greet + [mate, mate + 1 - 2 * core]
    for mate in greet:
        pl.semaphore_signal(barrier, inc=1, device_id=(mate,), device_id_type=MESH)
    intake = [
        pltpu.make_async_copy(source, target, small_sem.at[number])
        for number, (source, target) in enumerate(zip(given, held))
    ]
    for copy in intake[:2]:
        copy.start()
    local = []
    for p, weight in enumerate((w_r, w_k, w_v)):
        for side in range(2):
            local.append(
                pltpu.make_async_copy(
                    weight.at[:, pl.ds(side * half, half)],
                    stage.at[p, side],
                    local_sem,
                )
            )
    for copy in local:
        copy.start()
    for copy in intake[2:]:
        copy.start()
    loads = [
        pltpu.make_async_copy(source, target, load_sem.at[number])
        for number, (source, target) in enumerate(
            (
                (shared_gate, sg),
                (shared_up, su),
                (expert_gate.at[0], eg),
                (expert_up.at[0], eu),
                (shared_down, sd),
                (expert_down.at[0], ed),
                (state, old),
                (w_output, wo),
            )
        )
    ]
    for copy in intake[:2]:
        copy.wait()
    normed = rms_scale(tokens[...], gain[...]).astype(BF16)
    for q in range(RING):
        nsend[0, q] = normed[:, q * depth : (q + 1) * depth]
        chunks = [z * depth + y * RING * pair + q * pair for z in range(RING) for y in range(RING)]
        nsend[1, q] = jnp.concatenate([normed[:, s : s + pair] for s in chunks], axis=1)
        chunks = [z * depth + q * RING * pair for z in range(RING)]
        nsend[2, q] = jnp.concatenate([normed[:, s : s + RING * pair] for s in chunks], axis=1)
    def remote(source, target, send, receive, device):
        return pltpu.make_async_remote_copy(
            src_ref=source,
            dst_ref=target,
            send_sem=send,
            recv_sem=receive,
            device_id=(device,),
            device_id_type=MESH,
        )

    def launch(*args):
        remote(*args).start()

    def settle(view, semaphore):
        remote(view, view, semaphore, semaphore, partner).wait_recv()

    def chip_index(p, first, second):
        return first * RING + second if p == 2 else second * RING + first

    def row_slot(p, first, second, which):
        return wbuf.at[p, chip_index(p, first, second) * 2 + which]

    settle(stage, local_sem)
    pl.semaphore_wait(barrier, len(greet))

    for p in range(3):
        a1, a2, _ = spots[p]
        for offset in (1, 3, 2):
            chip = peer(STRIDES[p][0], offset) - core
            for side in range(2):
                launch(
                    stage.at[p, side],
                    row_slot(p, a1, a2, core),
                    wsend_sem,
                    wrecv_sem.at[p * RING + offset],
                    chip + side,
                )
        launch(
            stage.at[p, 1 - core],
            row_slot(p, a1, a2, core),
            wsend_sem,
            wrecv_sem.at[p * RING],
            partner,
        )
    for p in range(3):
        a1, a2, _ = spots[p]
        for offset in (1, 3, 2):
            chip = peer(STRIDES[p][1], offset) - core
            for side in range(2):
                launch(
                    stage.at[p, side],
                    row_slot(p, a1, a2, core),
                    wsend_sem,
                    wrecv_sem.at[p * RING],
                    chip + side,
                )
    for p in range(3):
        a3 = spots[p][2]
        for offset in (1, 3, 2):
            chip = peer(STRIDES[p][2], offset) - core
            for side in range(2):
                launch(
                    nsend.at[p, (a3 + offset) % RING],
                    xbuf.at[p, a3 * 2 + core],
                    wsend_sem,
                    xrecv_sem.at[p],
                    chip + side,
                )
        launch(
            nsend.at[p, a3],
            xbuf.at[p, a3 * 2 + core],
            wsend_sem,
            xrecv_sem.at[p],
            partner,
        )
    for p in range(3):
        a1, a2, a3 = spots[p]
        own = stage[p, core]
        wbuf[p, chip_index(p, a1, a2) * 2 + core] = own
        xbuf[p, a3 * 2 + core] = nsend[p, a3]

    for number in (6, 7, 2, 3, 5, 0, 1, 4):
        loads[number].start()

    for step in (1, 3, 2):
        for p in range(3):
            a1, a2, _ = spots[p]
            first = (a1 + RING - step) % RING
            block = wbuf.at[p, pl.ds(chip_index(p, first, a2) * 2, 2)]
            settle(block, wrecv_sem.at[p * RING + step])
            for offset in (1, 3, 2):
                launch(
                    block,
                    block,
                    wsend_sem,
                    wrecv_sem.at[p * RING],
                    peer(STRIDES[p][1], offset),
                )

    for copy in intake[2:]:
        copy.wait()

    def put(number, values, first):
        for head in range(values.shape[1] // HEAD):
            vecs[number, :, first + head, :] = values[:, head * HEAD : (head + 1) * HEAD]

    heads = mix // HEAD
    flip = (((1,), (1,)), ((), ()))

    def down(matrix):
        return lax.dot_general(normed, matrix, flip, preferred_element_type=F32)

    decay_low = jnp.tanh(down(decay_down[...])).astype(BF16)
    decay_pre = decay_base[...] + dot(decay_low, decay_up[...])
    put(3, jnp.exp(-jnp.exp(-jax.nn.softplus(-decay_pre) - 0.5)), 0)
    rate_low = down(rate_down[...]).astype(BF16)
    put(4, jax.nn.sigmoid(rate_base[...] + dot(rate_low, rate_up[...])), 0)

    strides = [STRIDES[p % 3] for p in range(SLICES)]
    note = RING * RING * MOST
    plane = RING * RING * count
    every = routes.shape[1]
    entries = old.shape[2]

    def iota(shape, dim):
        return lax.broadcasted_iota(jnp.int32, shape, dim)

    def token_of(p, number):
        first, second_stride, third = strides[p]
        device = (
            spots[p][2] * third
            + core
            + number // (RING * count) * second_stride
            + number // count % RING * first
        )
        return device * count + number % count

    def expert_of(p, number):
        third = strides[p][2]
        return me - spots[p][2] * third - core + number // 2 * third + number % 2

    routes_low = onehot_values(routes[...])
    weights_low = route_weights[...].astype(BF16)
    up_row = iota((plane, plane), 0)
    up_col = iota((plane, plane), 1)
    same = up_row // count == up_col // count
    upper = onehot(same & (up_row < up_col))
    lower = onehot(same & (up_col < up_row))
    slot_row = iota((note, plane), 0)
    slot_col = iota((note, plane), 1)
    wanted = jnp.where(slot_col // count == slot_row // MOST, slot_row % MOST, -2).astype(F32)
    peers = 2 * RING

    def selector(p):
        pick = onehot(iota((every, plane), 0) == token_of(p, iota((every, plane), 1)))
        here = dot(routes_low, pick)
        names = expert_of(p, iota((peers, plane), 0)).astype(F32)
        named = names < 0.0
        for j in range(TOPK):
            named = named | (here[j : j + 1, :] == names)
        before = dot(onehot(named), upper)
        rank = jnp.where(named, before, -1.0)
        parts = [
            onehot(jnp.broadcast_to(rank[i : i + 1, :], (note, plane)) == wanted)
            for i in range(peers)
        ]
        return jnp.concatenate(parts, 0)

    for p in range(3):
        selectors[p] = selector(p)

    fold[...] = onehot(iota((entries, HEAD), 0) // HEAD == iota((entries, HEAD), 1))
    each = RING * note
    turn_row = iota((each, each), 0)
    turn_col = iota((each, each), 1)

    def digits(number):
        return number // 64, number // 16 % 4, number // 4 % 4, number % 4

    def joined(a, b, c, d):
        return ((a * RING + b) * RING + c) * MOST + d

    def orders(number):
        z, y, x, s = digits(number)
        return [None, joined(x, z, y, s), joined(y, x, z, s)]

    def restored(number):
        first, middle, last, s = digits(number)
        return [None, joined(middle, last, first, s), joined(last, first, middle, s)]

    turns = [None] + [onehot(turn_col == orders(turn_row)[p]) for p in (1, 2)]
    returns = [None] + [onehot(turn_col == restored(turn_row)[p]) for p in (1, 2)]

    for p in range(3):
        a1, a2, a3 = spots[p]
        settle(xbuf.at[p, pl.ds(0, 7)], xrecv_sem.at[p])
        settle(wbuf.at[p, pl.ds(0, 25)], wrecv_sem.at[p * RING])
        stacked = xbuf[p].reshape(2 * RING * count, depth)
        part = dot(stacked, wbuf[p].reshape(depth, half)).astype(BF16)
        psend[p] = part.reshape(2 * RING, count, half)
        for offset in (1, 3, 2):
            chip = peer(STRIDES[p][2], offset) - core
            for side in range(2):
                launch(
                    psend.at[p, (a3 + offset) % RING * 2 + side],
                    precv.at[p, a3 * 2 + core],
                    psend_sem,
                    precv_sem.at[p],
                    chip + side,
                )
        launch(
            psend.at[p, a3 * 2 + 1 - core],
            precv.at[p, a3 * 2 + core],
            psend_sem,
            precv_sem.at[p],
            partner,
        )
        precv[p, a3 * 2 + core] = psend[p, a3 * 2 + core]

    for p in range(3):
        settle(precv.at[p, pl.ds(0, 7)], precv_sem.at[p])
        for side in range(2):
            added = precv[p, side].astype(F32)
            for which in range(1, RING):
                added = added + precv[p, which * 2 + side].astype(F32)
            added = added.astype(BF16).astype(F32)
            put(p, added, side * (heads // 2))
            if p == 1:
                scale = key_scale[:, side * half : (side + 1) * half]
                put(5, added * scale, side * (heads // 2))

    tall = count * heads
    reader, keys, values, decay, learn, scaled = [vecs[w].reshape(tall, HEAD) for w in range(6)]
    direction = scaled / jnp.sqrt(jnp.sum(scaled * scaled, axis=-1, keepdims=True) + 1.0)
    learned = direction * learn

    def twice(inputs):
        return jnp.concatenate([inputs, inputs], axis=1)

    along = twice(direction)
    reading = twice(decay * reader)
    loads[6].wait()
    cells = [
        old[:, :, lane : lane + 2 * HEAD].reshape(tall, 2 * HEAD)
        for lane in range(0, entries, 2 * HEAD)
    ]
    removed = dot(jnp.concatenate([(c * along).astype(BF16) for c in cells], 1), fold[...])
    readout = dot(jnp.concatenate([(c * reading).astype(BF16) for c in cells], 1), fold[...])
    readout = (
        readout
        - removed * jnp.sum(learned * reader, axis=-1, keepdims=True)
        + values * jnp.sum(keys * reader, axis=-1, keepdims=True)
    )
    centre = jnp.mean(readout, axis=-1, keepdims=True)
    spread = jnp.mean(jnp.square(readout - centre), axis=-1, keepdims=True)
    mixed = (readout - centre) * lax.rsqrt(spread + GROUP_EPS)
    vecs[5] = mixed.reshape(count, heads, HEAD)
    flat = jnp.concatenate([vecs[5, :, head, :] for head in range(heads)], axis=1)
    flat = (flat * head_gain[...]).astype(BF16)
    loads[7].wait()
    after = (tokens[...].astype(F32) + dot(flat, wo[...])).astype(BF16)
    second[...] = rms_scale(after, second_gain[...]).astype(BF16)

    starts = [sum(widths[:p]) for p in range(SLICES)]
    cuts = [slice(starts[p], starts[p] + widths[p]) for p in range(SLICES)]
    mine = [second.at[:, pl.ds(starts[p], widths[p])] for p in range(SLICES)]

    def onward(p, step, source):
        a1, a2, _ = spots[p]
        for offset in (1, 3, 2):
            launch(
                source,
                near[p].at[a2 * RING + (a1 + RING - step) % RING],
                esend_sem,
                r2.at[p],
                hop(p, 1, offset),
            )

    def enter(p):
        a1, a2, _ = spots[p]
        for offset in (1, 3, 2):
            launch(
                mine[p],
                near[p].at[a2 * RING + a1],
                esend_sem,
                r1.at[p * 3 + offset - 1],
                hop(p, 0, offset),
            )

    groups = [range(3), range(3, SLICES)]
    for p in groups[0]:
        enter(p)
    for p in groups[0]:
        onward(p, 0, mine[p])
    for group in groups[1:]:
        for p in group:
            enter(p)
    sent = second[...]
    for p in range(SLICES):
        a1, a2, _ = spots[p]
        near[p][a2 * RING + a1] = sent[:, cuts[p]]

    wide_buf[0] = twice(decay)
    wide_buf[1] = twice(learned)
    wide_buf[2] = twice(keys)
    high = removed.astype(BF16)
    low = (removed - high.astype(F32)).astype(BF16)
    low_buf[0] = jnp.concatenate([high, low], axis=1)
    low_buf[1] = jnp.concatenate([values, jnp.zeros_like(values)], axis=1).astype(BF16)
    outward = [
        pltpu.make_async_copy(wide_buf, wide_out, out_sem.at[0]),
        pltpu.make_async_copy(low_buf, low_out, out_sem.at[1]),
    ]
    for copy in outward:
        copy.start()

    for group in groups:
        if group != groups[0]:
            for p in group:
                onward(p, 0, mine[p])
        for offset in (1, 3, 2):
            for p in group:
                a1, a2, _ = spots[p]
                slot = near[p].at[a2 * RING + (a1 + RING - offset) % RING]
                settle(slot, r1.at[p * 3 + offset - 1])
                onward(p, offset, slot)

    for p in range(SLICES):
        a1, a2, a3 = spots[p]
        settle(near[p].at[pl.ds(0, 12)], r2.at[p])
        held = near[p][...].reshape(plane, widths[p])
        picked = dot(selectors[order_of(p)], held).astype(BF16)
        chosen[p][...] = picked.reshape(peers, note, widths[p])
        for offset in (1, 3, 2):
            chip = hop(p, 2, offset) - core
            for side in range(2):
                launch(
                    chosen[p].at[(a3 + offset) % RING * 2 + side],
                    inbox[p].at[core * RING + a3],
                    esend_sem,
                    r3.at[p],
                    chip + side,
                )
        launch(
            chosen[p].at[a3 * 2 + 1 - core],
            inbox[p].at[core * RING + a3],
            esend_sem,
            r3.at[p],
            partner,
        )
        inbox[p][core * RING + a3] = chosen[p][a3 * 2 + core]

    turned = (((1,), (1,)), ((), ()))
    tall_row = iota((plane, peers * note), 0)
    tall_col = iota((plane, peers * note), 1)
    expand = onehot(iota((128, peers * note), 0) == iota((128, peers * note), 1) // note)
    wanted_t = jnp.where(
        tall_row // count == tall_col % note // MOST, tall_col % MOST, -2
    ).astype(F32)

    def mixing(p):
        pick = onehot(iota((plane, every), 1) == token_of(p, iota((plane, every), 0)))
        here = lax.dot_general(pick, routes_low, turned, preferred_element_type=F32)
        weigh = lax.dot_general(pick, weights_low, turned, preferred_element_type=F32)
        number = iota((plane, 128), 1)
        names = jnp.where(number < peers, expert_of(p, number), -1).astype(F32)
        named = names < -2.0
        weight = jnp.zeros((plane, 128), F32)
        for j in range(TOPK):
            hit = here[:, j : j + 1] == names
            named = named | hit
            weight = weight + jnp.where(hit, weigh[:, j : j + 1], 0.0)
        before = dot(lower, onehot(named))
        rank = dot(jnp.where(named, before, -1.0).astype(BF16), expand)
        spread = dot(weight.astype(BF16), expand)
        return jnp.where(rank == wanted_t, spread, 0.0).astype(BF16)

    for p in range(3):
        mixers[p] = mixing(p)

    def gated(gate_part, up_part):
        return (jax.nn.silu(gate_part) * up_part).astype(BF16)

    def turned_by(matrices, p, side, inputs):
        which = p % 3 if p < 6 else side
        return inputs if which == 0 else dot(matrices[which], inputs).astype(BF16)

    gate_part = None
    up_part = None
    loads[2].wait()
    loads[3].wait()
    for p in range(SLICES):
        settle(inbox[p].at[pl.ds(0, 7)], r3.at[p])
        inputs = jnp.concatenate(
            [
                turned_by(
                    turns,
                    p,
                    side,
                    inbox[p][side * RING : (side + 1) * RING].reshape(each, widths[p]),
                )
                for side in range(2)
            ],
            0,
        )
        gate_more = dot(inputs, eg[cuts[p], :])
        up_more = dot(inputs, eu[cuts[p], :])
        gate_part = gate_more if gate_part is None else gate_part + gate_more
        up_part = up_more if up_part is None else up_part + up_more
    hidden = gated(gate_part, up_part)
    loads[5].wait()

    for p in range(SLICES):
        a3 = spots[p][2]
        inputs = jnp.concatenate(
            [
                turned_by(returns, p, side, hidden[side * each : (side + 1) * each])
                for side in range(2)
            ],
            0,
        )
        result = dot(inputs, ed[:, cuts[p]]).astype(BF16)
        answer[p][...] = result.reshape(2 * RING, note, widths[p])
        ends = [spots[p][2] if p < 6 else spots[side][2] for side in range(2)]
        for offset in (1, 3, 2):
            for side in range(2):
                stride = STRIDES[p % 3 if p < 6 else side][2]
                launch(
                    answer[p].at[side * RING + (ends[side] + offset) % RING],
                    back[p].at[ends[side] * 2 + core],
                    rsend_sem,
                    u3.at[p],
                    peer(stride, offset) - core + side,
                )
        end = ends[0] + core * (ends[1] - ends[0])
        far = ends[0] + ends[1] - end
        launch(
            answer[p].at[(1 - core) * RING + far],
            back[p].at[far * 2 + core],
            rsend_sem,
            u3.at[p],
            partner,
        )
        back[p][end * 2 + core] = answer[p][core * RING + end]

    loads[0].wait()
    loads[1].wait()
    shared_hidden = gated(dot(sent, sg[...]), dot(sent, su[...]))
    loads[4].wait()
    kept = after.astype(F32) + dot(shared_hidden, sd[...])

    for p in range(SLICES):
        a1, a2, a3 = spots[p]
        settle(back[p].at[pl.ds(0, 7)], u3.at[p])
        summed = dot(mixers[order_of(p)], back[p][...].reshape(peers * note, widths[p])).astype(BF16)
        total[p][...] = summed.reshape(RING * RING, count, widths[p])
        for offset in (1, 3, 2):
            launch(
                total[p].at[pl.ds((a2 + offset) % RING * RING, RING)],
                gather[p].at[pl.ds(offset * RING, RING)],
                rsend_sem,
                u2.at[p],
                hop(p, 1, offset),
            )
    for p in range(SLICES):
        a1, a2, a3 = spots[p]
        summed = total[p][pl.ds(a2 * RING, RING)].astype(F32)
        settle(gather[p].at[pl.ds(RING, 3 * RING)], u2.at[p])
        for offset in (1, 3, 2):
            summed = summed + gather[p][offset * RING : (offset + 1) * RING].astype(F32)
        line[p][...] = summed.astype(BF16)
        for offset in (1, 3, 2):
            launch(
                line[p].at[(a1 + offset) % RING],
                final[p].at[offset],
                rsend_sem,
                u1.at[p],
                hop(p, 0, offset),
            )
    for p in range(SLICES):
        a1 = spots[p][0]
        summed = line[p][a1].astype(F32)
        settle(final[p].at[pl.ds(1, 3)], u1.at[p])
        for offset in (1, 3, 2):
            summed = summed + final[p][offset].astype(F32)
        out[:, cuts[p]] = (kept[:, cuts[p]] + summed).astype(BF16)
    sent_units = (3 * (31 + 7), 3 * 7)
    settle(eg.at[pl.ds(0, sent_units[0] * rows)], wsend_sem)
    settle(eg.at[pl.ds(0, sent_units[1] * rows)], psend_sem)
    settle(wo.at[pl.ds(0, (15 + 7 * RING) * count)], esend_sem)
    settle(wo.at[pl.ds(0, (15 + 7 * RING) * count)], rsend_sem)
    for copy in outward:
        copy.wait()


def layer(vmems, hbms):
    tokens, routes = vmems[0], vmems[11]
    w_r, state, matrices = hbms[0], hbms[3], hbms[5:]
    count, width = tokens.shape
    rows, mix = w_r.shape
    half = mix // 2
    depth = width // RING
    heads, entries = state.shape[1:]
    widths = part_widths(width)
    vmem = pl.BlockSpec(memory_space=pltpu.VMEM)
    hbm = pl.BlockSpec(memory_space=pl.ANY)
    dma = pltpu.SemaphoreType.DMA
    blocks = RING * RING
    note = blocks * MOST
    plane = blocks * count
    shapes = (
        (RING * RING, count),
        (2 * RING, note),
        (2 * RING, note),
        (2 * RING, note),
        (2 * RING, note),
        (RING * RING, count),
        (RING * RING, count),
        (RING, count),
        (RING, count),
    )
    shapes = [pltpu.VMEM(shape + (w,), BF16) for shape in shapes for w in widths]
    sizes = [8, len(vmems), 3 * RING, 3, 3]
    later = [SLICES * size for size in (3, 1, 1, 1, 1, 1)]
    return pl.pallas_call(
        functools.partial(layer_kernel, widths, len(vmems)),
        out_shape=[
            jax.ShapeDtypeStruct((count, width), BF16),
            jax.ShapeDtypeStruct((3, count * heads, 2 * HEAD), F32),
            jax.ShapeDtypeStruct((2, count * heads, 2 * HEAD), BF16),
        ],
        in_specs=[hbm] * (len(vmems) + len(hbms)),
        out_specs=[vmem, hbm, hbm],
        scratch_shapes=[
            pltpu.VMEM((3, 2, rows, half), BF16),
            pltpu.VMEM((3, 2 * RING * RING, rows, half), BF16),
            pltpu.VMEM((3, RING, count, depth), BF16),
            pltpu.VMEM((3, 2 * RING, count, depth), BF16),
            pltpu.VMEM((3, 2 * RING, count, half), BF16),
            pltpu.VMEM((3, 2 * RING, count, half), BF16),
            pltpu.VMEM((6, count, heads, HEAD), F32),
            pltpu.VMEM(state.shape, F32),
            pltpu.VMEM(hbms[4].shape, BF16),
        ]
        + [pltpu.VMEM(m.shape[-2:], BF16) for m in matrices]
        + [
            pltpu.VMEM((entries, HEAD), BF16),
            pltpu.VMEM((count, width), BF16),
            pltpu.VMEM((3, 2 * RING * note, plane), BF16),
            pltpu.VMEM((3, plane, 2 * RING * note), BF16),
        ]
        + [pltpu.VMEM(small.shape, small.dtype) for small in vmems]
        + shapes
        + [dma]
        + [dma((size,)) for size in sizes]
        + [dma] * 4
        + [dma((size,)) for size in later]
        + [
            pltpu.VMEM((3, count * heads, 2 * HEAD), F32),
            pltpu.VMEM((2, count * heads, 2 * HEAD), BF16),
            dma((2,)),
        ],
        compiler_params=pltpu.CompilerParams(
            collective_id=0, has_side_effects=True, vmem_limit_bytes=VMEM_BYTES
        ),
        name="layer",
    )(*vmems, *hbms)


def finish_kernel(wide, low, state, ready, new_state, new_tokens, spread):
    per_step, heads, entries = state.shape
    tall = per_step * heads
    span = 2 * HEAD

    @pl.when(pl.program_id(0) == 0)
    def _():
        row = lax.broadcasted_iota(jnp.int32, (span, entries), 0)
        col = lax.broadcasted_iota(jnp.int32, (span, entries), 1)
        spread[...] = onehot(col // HEAD == row % HEAD)
        new_tokens[...] = ready[...]

    decay, learned, keys = [wide[w] for w in range(3)]
    removed = dot(low[0], spread[...])
    values = dot(low[1], spread[...])
    for lane in range(0, entries, span):
        cut = slice(lane, lane + span)
        fresh = (
            state[:, :, cut].reshape(tall, span) * decay
            - removed[:, cut] * learned
            + values[:, cut] * keys
        )
        new_state[:, :, cut] = fresh.reshape(per_step, heads, span)


def finish(wide, low, state, ready):
    count, heads, entries = state.shape
    per_step = 8 if count % 8 == 0 else 1
    tall = per_step * heads
    span = 2 * HEAD
    block = pl.BlockSpec((per_step, heads, entries), lambda i: (i, 0, 0))
    flat = pl.BlockSpec(ready.shape, lambda i: (0, 0))
    return pl.pallas_call(
        finish_kernel,
        grid=(count // per_step,),
        out_shape=[
            jax.ShapeDtypeStruct(state.shape, F32),
            jax.ShapeDtypeStruct(ready.shape, BF16),
        ],
        in_specs=[
            pl.BlockSpec((3, tall, span), lambda i: (0, i, 0)),
            pl.BlockSpec((2, tall, span), lambda i: (0, i, 0)),
            block,
            flat,
        ],
        out_specs=[block, flat],
        scratch_shapes=[pltpu.VMEM((span, entries), BF16)],
        compiler_params=pltpu.CompilerParams(
            dimension_semantics=("arbitrary",), vmem_limit_bytes=VMEM_BYTES
        ),
        name="finish",
    )(wide, low, state, ready)


def per_device(
    tokens,
    recurrent_state,
    first_gain,
    w_receptance,
    w_key,
    w_value,
    decay_down,
    decay_up,
    decay_base,
    rate_down,
    rate_up,
    rate_base,
    key_scale,
    head_gain,
    w_output,
    second_gain,
    shared_gate,
    shared_up,
    shared_down,
    expert_gate,
    expert_up,
    expert_down,
    routes,
    route_weights,
):
    vmems = (
        tokens,
        first_gain[None, :],
        decay_down.T,
        decay_up,
        decay_base[None, :],
        rate_down.T,
        rate_up,
        rate_base[None, :],
        key_scale[None, :],
        head_gain[None, :],
        second_gain[None, :],
        routes.T,
        route_weights.T,
    )
    hbms = (
        w_receptance,
        w_key,
        w_value,
        recurrent_state,
        w_output,
        shared_gate,
        shared_up,
        shared_down,
        expert_gate,
        expert_up,
        expert_down,
    )
    ready, wide, low = layer(vmems, hbms)
    new_state, new_tokens = finish(wide, low, recurrent_state, ready)
    return (new_tokens, new_state)


def solution(mesh):
    in_specs = (
        P("ep", None),
        P("ep", None, None),
        P(),
        P("ep", None),
        P("ep", None),
        P("ep", None),
        P(),
        P(),
        P(),
        P(),
        P(),
        P(),
        P(),
        P(),
        P(),
        P(),
        P(),
        P(),
        P(),
        P("ep", None, None),
        P("ep", None, None),
        P("ep", None, None),
        P(),
        P(),
    )
    out_specs = (P("ep", None), P("ep", None, None))
    return jax.shard_map(
        per_device, mesh=mesh, in_specs=in_specs, out_specs=out_specs, check_vma=False
    )
```

```python
import functools

import jax
import jax.numpy as jnp
from jax import lax
from jax.experimental import pallas as pl
from jax.experimental.pallas import tpu as pltpu
from jax.sharding import PartitionSpec as P

HEAD = 64
TOPK = 4
MOST = 4
RING = 4
SLICES = 7
STRIDES = ((2, 8, 32), (8, 32, 2), (32, 2, 8))
NORM_EPS = 1e-06
GROUP_EPS = 0.00064
MESH = pl.DeviceIdType.MESH
F32 = jnp.float32
BF16 = jnp.bfloat16
VMEM_BYTES = 60 * 1024 * 1024


def dot(a, b):
    return jnp.dot(a, b, preferred_element_type=F32)


def rms_scale(inputs, gain):
    widened = inputs.astype(F32)
    return (
        widened * lax.rsqrt(jnp.mean(widened * widened, axis=-1, keepdims=True) + NORM_EPS) * gain
    )


def onehot(flags):
    return flags.astype(F32).astype(BF16)


def onehot_values(values):
    return values.astype(F32).astype(BF16)


def part_widths(width):
    tiles = width // 128
    even = tiles // 3
    counts = [even - even // 2] * 3 + [even // 2] * 3 + [tiles - 3 * even]
    return [number * 128 for number in counts]


def layer_kernel(widths, small, *refs):
    given = refs[:small]
    (
        w_r,
        w_k,
        w_v,
        state,
        w_output,
        shared_gate,
        shared_up,
        shared_down,
        expert_gate,
        expert_up,
        expert_down,
        out,
        wide_out,
        low_out,
        stage,
        wbuf,
        nsend,
        xbuf,
        psend,
        precv,
        vecs,
        old,
        wo,
        sg,
        su,
        sd,
        eg,
        eu,
        ed,
        fold,
        second,
        selectors,
        mixers,
    ) = refs[small : small + 33]
    rest = refs[small + 33 + small :]
    held = refs[small + 33 : small + 33 + small]
    (
        tokens,
        gain,
        decay_down,
        decay_up,
        decay_base,
        rate_down,
        rate_up,
        rate_base,
        key_scale,
        head_gain,
        second_gain,
        routes,
        route_weights,
    ) = held
    near, chosen, inbox, answer, back, total, gather, line, final = [
        rest[SLICES * i : SLICES * (i + 1)] for i in range(9)
    ]
    local_sem, load_sem, small_sem = rest[9 * SLICES : 9 * SLICES + 3]
    wide_buf, low_buf, out_sem = rest[-3:]
    wrecv_sem, xrecv_sem, precv_sem = rest[9 * SLICES + 3 : 9 * SLICES + 6]
    wsend_sem, psend_sem, esend_sem, rsend_sem = rest[9 * SLICES + 6 : 9 * SLICES + 10]
    r1, r2, r3, u3, u2, u1 = rest[9 * SLICES + 10 : -3]
    rows, mix = w_r.shape
    half = mix // 2
    count, width = tokens.shape
    pair = 2 * rows
    depth = width // RING
    me = lax.axis_index("ep")
    core = me % 2
    partner = me + 1 - 2 * core

    def place(stride):
        return (me // stride) % RING

    def peer(stride, offset):
        return me + ((place(stride) + offset) % RING - place(stride)) * stride

    spots = [[place(stride) for stride in STRIDES[p % 3]] for p in range(6)]
    spots = spots + [[spots[0][i] + core * (spots[1][i] - spots[0][i]) for i in range(3)]]

    def hop(p, level, offset):
        mate = peer(STRIDES[p % 3][level], offset)
        return mate if p < 6 else mate + core * (peer(STRIDES[1][level], offset) - mate)

    def order_of(p):
        return p % 3 if p < 6 else core
    barrier = pltpu.get_barrier_semaphore()
    greet = [partner]
    for stride in STRIDES[0]:
        for offset in range(1, RING):
            mate = peer(stride, offset)
            greet = greet + [mate, mate + 1 - 2 * core]
    for mate in greet:
        pl.semaphore_signal(barrier, inc=1, device_id=(mate,), device_id_type=MESH)
    intake = [
        pltpu.make_async_copy(source, target, small_sem.at[number])
        for number, (source, target) in enumerate(zip(given, held))
    ]
    for copy in intake[:2]:
        copy.start()
    local = []
    for p, weight in enumerate((w_r, w_k, w_v)):
        for side in range(2):
            local.append(
                pltpu.make_async_copy(
                    weight.at[:, pl.ds(side * half, half)],
                    stage.at[p, side],
                    local_sem,
                )
            )
    for copy in local:
        copy.start()
    for copy in intake[2:]:
        copy.start()
    loads = [
        pltpu.make_async_copy(source, target, load_sem.at[number])
        for number, (source, target) in enumerate(
            (
                (shared_gate, sg),
                (shared_up, su),
                (expert_gate.at[0], eg),
                (expert_up.at[0], eu),
                (shared_down, sd),
                (expert_down.at[0], ed),
                (state, old),
                (w_output, wo),
            )
        )
    ]
    for copy in intake[:2]:
        copy.wait()
    normed = rms_scale(tokens[...], gain[...]).astype(BF16)
    for q in range(RING):
        nsend[0, q] = normed[:, q * depth : (q + 1) * depth]
        chunks = [z * depth + y * RING * pair + q * pair for z in range(RING) for y in range(RING)]
        nsend[1, q] = jnp.concatenate([normed[:, s : s + pair] for s in chunks], axis=1)
        chunks = [z * depth + q * RING * pair for z in range(RING)]
        nsend[2, q] = jnp.concatenate([normed[:, s : s + RING * pair] for s in chunks], axis=1)
    def remote(source, target, send, receive, device):
        return pltpu.make_async_remote_copy(
            src_ref=source,
            dst_ref=target,
            send_sem=send,
            recv_sem=receive,
            device_id=(device,),
            device_id_type=MESH,
        )

    def launch(*args):
        remote(*args).start()

    def settle(view, semaphore):
        remote(view, view, semaphore, semaphore, partner).wait_recv()

    def chip_index(p, first, second):
        return first * RING + second if p == 2 else second * RING + first

    def row_slot(p, first, second, which):
        return wbuf.at[p, chip_index(p, first, second) * 2 + which]

    settle(stage, local_sem)
    pl.semaphore_wait(barrier, len(greet))

    for p in range(3):
        a1, a2, _ = spots[p]
        for offset in (2, 1, 3):
            chip = peer(STRIDES[p][0], offset) - core
            for side in range(2):
                launch(
                    stage.at[p, side],
                    row_slot(p, a1, a2, core),
                    wsend_sem,
                    wrecv_sem.at[p * RING + offset],
                    chip + side,
                )
        launch(
            stage.at[p, 1 - core],
            row_slot(p, a1, a2, core),
            wsend_sem,
            wrecv_sem.at[p * RING],
            partner,
        )
    for p in range(3):
        a1, a2, _ = spots[p]
        for offset in (2, 1, 3):
            chip = peer(STRIDES[p][1], offset) - core
            for side in range(2):
                launch(
                    stage.at[p, side],
                    row_slot(p, a1, a2, core),
                    wsend_sem,
                    wrecv_sem.at[p * RING],
                    chip + side,
                )
    for p in range(3):
        a3 = spots[p][2]
        for offset in (2, 1, 3):
            chip = peer(STRIDES[p][2], offset) - core
            for side in range(2):
                launch(
                    nsend.at[p, (a3 + offset) % RING],
                    xbuf.at[p, a3 * 2 + core],
                    wsend_sem,
                    xrecv_sem.at[p],
                    chip + side,
                )
        launch(
            nsend.at[p, a3],
            xbuf.at[p, a3 * 2 + core],
            wsend_sem,
            xrecv_sem.at[p],
            partner,
        )
    for p in range(3):
        a1, a2, a3 = spots[p]
        own = stage[p, core]
        wbuf[p, chip_index(p, a1, a2) * 2 + core] = own
        xbuf[p, a3 * 2 + core] = nsend[p, a3]

    for number in (6, 7, 2, 3, 5, 0, 1, 4):
        loads[number].start()

    for step in (1, 3, 2):
        for p in range(3):
            a1, a2, _ = spots[p]
            first = (a1 + RING - step) % RING
            block = wbuf.at[p, pl.ds(chip_index(p, first, a2) * 2, 2)]
            settle(block, wrecv_sem.at[p * RING + step])
            for offset in (2, 1, 3):
                launch(
                    block,
                    block,
                    wsend_sem,
                    wrecv_sem.at[p * RING],
                    peer(STRIDES[p][1], offset),
                )

    for copy in intake[2:]:
        copy.wait()

    def put(number, values, first):
        for head in range(values.shape[1] // HEAD):
            vecs[number, :, first + head, :] = values[:, head * HEAD : (head + 1) * HEAD]

    heads = mix // HEAD
    flip = (((1,), (1,)), ((), ()))

    def down(matrix):
        return lax.dot_general(normed, matrix, flip, preferred_element_type=F32)

    decay_low = jnp.tanh(down(decay_down[...])).astype(BF16)
    decay_pre = decay_base[...] + dot(decay_low, decay_up[...])
    put(3, jnp.exp(-jnp.exp(-jax.nn.softplus(-decay_pre) - 0.5)), 0)
    rate_low = down(rate_down[...]).astype(BF16)
    put(4, jax.nn.sigmoid(rate_base[...] + dot(rate_low, rate_up[...])), 0)

    strides = [STRIDES[p % 3] for p in range(SLICES)]
    note = RING * RING * MOST
    plane = RING * RING * count
    every = routes.shape[1]
    entries = old.shape[2]

    def iota(shape, dim):
        return lax.broadcasted_iota(jnp.int32, shape, dim)

    def token_of(p, number):
        first, second_stride, third = strides[p]
        device = (
            spots[p][2] * third
            + core
            + number // (RING * count) * second_stride
            + number // count % RING * first
        )
        return device * count + number % count

    def expert_of(p, number):
        third = strides[p][2]
        return me - spots[p][2] * third - core + number // 2 * third + number % 2

    routes_low = onehot_values(routes[...])
    weights_low = route_weights[...].astype(BF16)
    up_row = iota((plane, plane), 0)
    up_col = iota((plane, plane), 1)
    same = up_row // count == up_col // count
    upper = onehot(same & (up_row < up_col))
    lower = onehot(same & (up_col < up_row))
    slot_row = iota((note, plane), 0)
    slot_col = iota((note, plane), 1)
    wanted = jnp.where(slot_col // count == slot_row // MOST, slot_row % MOST, -2).astype(F32)
    peers = 2 * RING

    def selector(p):
        pick = onehot(iota((every, plane), 0) == token_of(p, iota((every, plane), 1)))
        here = dot(routes_low, pick)
        names = expert_of(p, iota((peers, plane), 0)).astype(F32)
        named = names < 0.0
        for j in range(TOPK):
            named = named | (here[j : j + 1, :] == names)
        before = dot(onehot(named), upper)
        rank = jnp.where(named, before, -1.0)
        parts = [
            onehot(jnp.broadcast_to(rank[i : i + 1, :], (note, plane)) == wanted)
            for i in range(peers)
        ]
        return jnp.concatenate(parts, 0)

    for p in range(3):
        selectors[p] = selector(p)

    fold[...] = onehot(iota((entries, HEAD), 0) // HEAD == iota((entries, HEAD), 1))
    each = RING * note
    turn_row = iota((each, each), 0)
    turn_col = iota((each, each), 1)

    def digits(number):
        return number // 64, number // 16 % 4, number // 4 % 4, number % 4

    def joined(a, b, c, d):
        return ((a * RING + b) * RING + c) * MOST + d

    def orders(number):
        z, y, x, s = digits(number)
        return [None, joined(x, z, y, s), joined(y, x, z, s)]

    def restored(number):
        first, middle, last, s = digits(number)
        return [None, joined(middle, last, first, s), joined(last, first, middle, s)]

    turns = [None] + [onehot(turn_col == orders(turn_row)[p]) for p in (1, 2)]
    returns = [None] + [onehot(turn_col == restored(turn_row)[p]) for p in (1, 2)]

    for p in range(3):
        a1, a2, a3 = spots[p]
        settle(xbuf.at[p, pl.ds(0, 7)], xrecv_sem.at[p])
        settle(wbuf.at[p, pl.ds(0, 25)], wrecv_sem.at[p * RING])
        stacked = xbuf[p].reshape(2 * RING * count, depth)
        part = dot(stacked, wbuf[p].reshape(depth, half)).astype(BF16)
        psend[p] = part.reshape(2 * RING, count, half)
        for offset in (2, 1, 3):
            chip = peer(STRIDES[p][2], offset) - core
            for side in range(2):
                launch(
                    psend.at[p, (a3 + offset) % RING * 2 + side],
                    precv.at[p, a3 * 2 + core],
                    psend_sem,
                    precv_sem.at[p],
                    chip + side,
                )
        launch(
            psend.at[p, a3 * 2 + 1 - core],
            precv.at[p, a3 * 2 + core],
            psend_sem,
            precv_sem.at[p],
            partner,
        )
        precv[p, a3 * 2 + core] = psend[p, a3 * 2 + core]

    for p in range(3):
        settle(precv.at[p, pl.ds(0, 7)], precv_sem.at[p])
        for side in range(2):
            added = precv[p, side].astype(F32)
            for which in range(1, RING):
                added = added + precv[p, which * 2 + side].astype(F32)
            added = added.astype(BF16).astype(F32)
            put(p, added, side * (heads // 2))
            if p == 1:
                scale = key_scale[:, side * half : (side + 1) * half]
                put(5, added * scale, side * (heads // 2))

    tall = count * heads
    reader, keys, values, decay, learn, scaled = [vecs[w].reshape(tall, HEAD) for w in range(6)]
    direction = scaled / jnp.sqrt(jnp.sum(scaled * scaled, axis=-1, keepdims=True) + 1.0)
    learned = direction * learn

    def twice(inputs):
        return jnp.concatenate([inputs, inputs], axis=1)

    along = twice(direction)
    reading = twice(decay * reader)
    loads[6].wait()
    cells = [
        old[:, :, lane : lane + 2 * HEAD].reshape(tall, 2 * HEAD)
        for lane in range(0, entries, 2 * HEAD)
    ]
    removed = dot(jnp.concatenate([(c * along).astype(BF16) for c in cells], 1), fold[...])
    readout = dot(jnp.concatenate([(c * reading).astype(BF16) for c in cells], 1), fold[...])
    readout = (
        readout
        - removed * jnp.sum(learned * reader, axis=-1, keepdims=True)
        + values * jnp.sum(keys * reader, axis=-1, keepdims=True)
    )
    centre = jnp.mean(readout, axis=-1, keepdims=True)
    spread = jnp.mean(jnp.square(readout - centre), axis=-1, keepdims=True)
    mixed = (readout - centre) * lax.rsqrt(spread + GROUP_EPS)
    vecs[5] = mixed.reshape(count, heads, HEAD)
    flat = jnp.concatenate([vecs[5, :, head, :] for head in range(heads)], axis=1)
    flat = (flat * head_gain[...]).astype(BF16)
    loads[7].wait()
    after = (tokens[...].astype(F32) + dot(flat, wo[...])).astype(BF16)
    second[...] = rms_scale(after, second_gain[...]).astype(BF16)

    starts = [sum(widths[:p]) for p in range(SLICES)]
    cuts = [slice(starts[p], starts[p] + widths[p]) for p in range(SLICES)]
    mine = [second.at[:, pl.ds(starts[p], widths[p])] for p in range(SLICES)]

    def onward(p, step, source):
        a1, a2, _ = spots[p]
        for offset in (2, 1, 3):
            launch(
                source,
                near[p].at[a2 * RING + (a1 + RING - step) % RING],
                esend_sem,
                r2.at[p],
                hop(p, 1, offset),
            )

    def enter(p):
        a1, a2, _ = spots[p]
        for offset in (2, 1, 3):
            launch(
                mine[p],
                near[p].at[a2 * RING + a1],
                esend_sem,
                r1.at[p * 3 + offset - 1],
                hop(p, 0, offset),
            )

    groups = [range(3), range(3, SLICES)]
    for p in groups[0]:
        enter(p)
    for p in groups[0]:
        onward(p, 0, mine[p])
    for group in groups[1:]:
        for p in group:
            enter(p)
    sent = second[...]
    for p in range(SLICES):
        a1, a2, _ = spots[p]
        near[p][a2 * RING + a1] = sent[:, cuts[p]]

    wide_buf[0] = twice(decay)
    wide_buf[1] = twice(learned)
    wide_buf[2] = twice(keys)
    high = removed.astype(BF16)
    low = (removed - high.astype(F32)).astype(BF16)
    low_buf[0] = jnp.concatenate([high, low], axis=1)
    low_buf[1] = jnp.concatenate([values, jnp.zeros_like(values)], axis=1).astype(BF16)
    outward = [
        pltpu.make_async_copy(wide_buf, wide_out, out_sem.at[0]),
        pltpu.make_async_copy(low_buf, low_out, out_sem.at[1]),
    ]
    for copy in outward:
        copy.start()

    for group in groups:
        if group != groups[0]:
            for p in group:
                onward(p, 0, mine[p])
        for offset in (1, 3, 2):
            for p in group:
                a1, a2, _ = spots[p]
                slot = near[p].at[a2 * RING + (a1 + RING - offset) % RING]
                settle(slot, r1.at[p * 3 + offset - 1])
                onward(p, offset, slot)

    for p in range(SLICES):
        a1, a2, a3 = spots[p]
        settle(near[p].at[pl.ds(0, 12)], r2.at[p])
        held = near[p][...].reshape(plane, widths[p])
        picked = dot(selectors[order_of(p)], held).astype(BF16)
        chosen[p][...] = picked.reshape(peers, note, widths[p])
        for offset in (2, 1, 3):
            chip = hop(p, 2, offset) - core
            for side in range(2):
                launch(
                    chosen[p].at[(a3 + offset) % RING * 2 + side],
                    inbox[p].at[core * RING + a3],
                    esend_sem,
                    r3.at[p],
                    chip + side,
                )
        launch(
            chosen[p].at[a3 * 2 + 1 - core],
            inbox[p].at[core * RING + a3],
            esend_sem,
            r3.at[p],
            partner,
        )
        inbox[p][core * RING + a3] = chosen[p][a3 * 2 + core]

    turned = (((1,), (1,)), ((), ()))
    tall_row = iota((plane, peers * note), 0)
    tall_col = iota((plane, peers * note), 1)
    expand = onehot(iota((128, peers * note), 0) == iota((128, peers * note), 1) // note)
    wanted_t = jnp.where(
        tall_row // count == tall_col % note // MOST, tall_col % MOST, -2
    ).astype(F32)

    def mixing(p):
        pick = onehot(iota((plane, every), 1) == token_of(p, iota((plane, every), 0)))
        here = lax.dot_general(pick, routes_low, turned, preferred_element_type=F32)
        weigh = lax.dot_general(pick, weights_low, turned, preferred_element_type=F32)
        number = iota((plane, 128), 1)
        names = jnp.where(number < peers, expert_of(p, number), -1).astype(F32)
        named = names < -2.0
        weight = jnp.zeros((plane, 128), F32)
        for j in range(TOPK):
            hit = here[:, j : j + 1] == names
            named = named | hit
            weight = weight + jnp.where(hit, weigh[:, j : j + 1], 0.0)
        before = dot(lower, onehot(named))
        rank = dot(jnp.where(named, before, -1.0).astype(BF16), expand)
        spread = dot(weight.astype(BF16), expand)
        return jnp.where(rank == wanted_t, spread, 0.0).astype(BF16)

    for p in range(3):
        mixers[p] = mixing(p)

    def gated(gate_part, up_part):
        return (jax.nn.silu(gate_part) * up_part).astype(BF16)

    def turned_by(matrices, p, side, inputs):
        which = p % 3 if p < 6 else side
        return inputs if which == 0 else dot(matrices[which], inputs).astype(BF16)

    gate_part = None
    up_part = None
    loads[2].wait()
    loads[3].wait()
    for p in range(SLICES):
        settle(inbox[p].at[pl.ds(0, 7)], r3.at[p])
        inputs = jnp.concatenate(
            [
                turned_by(
                    turns,
                    p,
                    side,
                    inbox[p][side * RING : (side + 1) * RING].reshape(each, widths[p]),
                )
                for side in range(2)
            ],
            0,
        )
        gate_more = dot(inputs, eg[cuts[p], :])
        up_more = dot(inputs, eu[cuts[p], :])
        gate_part = gate_more if gate_part is None else gate_part + gate_more
        up_part = up_more if up_part is None else up_part + up_more
    hidden = gated(gate_part, up_part)
    loads[5].wait()

    for p in range(SLICES):
        a3 = spots[p][2]
        inputs = jnp.concatenate(
            [
                turned_by(returns, p, side, hidden[side * each : (side + 1) * each])
                for side in range(2)
            ],
            0,
        )
        result = dot(inputs, ed[:, cuts[p]]).astype(BF16)
        answer[p][...] = result.reshape(2 * RING, note, widths[p])
        ends = [spots[p][2] if p < 6 else spots[side][2] for side in range(2)]
        for offset in (2, 1, 3):
            for side in range(2):
                stride = STRIDES[p % 3 if p < 6 else side][2]
                launch(
                    answer[p].at[side * RING + (ends[side] + offset) % RING],
                    back[p].at[ends[side] * 2 + core],
                    rsend_sem,
                    u3.at[p],
                    peer(stride, offset) - core + side,
                )
        end = ends[0] + core * (ends[1] - ends[0])
        far = ends[0] + ends[1] - end
        launch(
            answer[p].at[(1 - core) * RING + far],
            back[p].at[far * 2 + core],
            rsend_sem,
            u3.at[p],
            partner,
        )
        back[p][end * 2 + core] = answer[p][core * RING + end]

    loads[0].wait()
    loads[1].wait()
    shared_hidden = gated(dot(sent, sg[...]), dot(sent, su[...]))
    loads[4].wait()
    kept = after.astype(F32) + dot(shared_hidden, sd[...])

    for p in range(SLICES):
        a1, a2, a3 = spots[p]
        settle(back[p].at[pl.ds(0, 7)], u3.at[p])
        summed = dot(mixers[order_of(p)], back[p][...].reshape(peers * note, widths[p])).astype(BF16)
        total[p][...] = summed.reshape(RING * RING, count, widths[p])
        for offset in (2, 1, 3):
            launch(
                total[p].at[pl.ds((a2 + offset) % RING * RING, RING)],
                gather[p].at[pl.ds(offset * RING, RING)],
                rsend_sem,
                u2.at[p],
                hop(p, 1, offset),
            )
    for p in range(SLICES):
        a1, a2, a3 = spots[p]
        summed = total[p][pl.ds(a2 * RING, RING)].astype(F32)
        settle(gather[p].at[pl.ds(RING, 3 * RING)], u2.at[p])
        for offset in (1, 3, 2):
            summed = summed + gather[p][offset * RING : (offset + 1) * RING].astype(F32)
        line[p][...] = summed.astype(BF16)
        for offset in (2, 1, 3):
            launch(
                line[p].at[(a1 + offset) % RING],
                final[p].at[offset],
                rsend_sem,
                u1.at[p],
                hop(p, 0, offset),
            )
    for p in range(SLICES):
        a1 = spots[p][0]
        summed = line[p][a1].astype(F32)
        settle(final[p].at[pl.ds(1, 3)], u1.at[p])
        for offset in (1, 3, 2):
            summed = summed + final[p][offset].astype(F32)
        out[:, cuts[p]] = (kept[:, cuts[p]] + summed).astype(BF16)
    sent_units = (3 * (31 + 7), 3 * 7)
    settle(eg.at[pl.ds(0, sent_units[0] * rows)], wsend_sem)
    settle(eg.at[pl.ds(0, sent_units[1] * rows)], psend_sem)
    settle(wo.at[pl.ds(0, (15 + 7 * RING) * count)], esend_sem)
    settle(wo.at[pl.ds(0, (15 + 7 * RING) * count)], rsend_sem)
    for copy in outward:
        copy.wait()


def layer(vmems, hbms):
    tokens, routes = vmems[0], vmems[11]
    w_r, state, matrices = hbms[0], hbms[3], hbms[5:]
    count, width = tokens.shape
    rows, mix = w_r.shape
    half = mix // 2
    depth = width // RING
    heads, entries = state.shape[1:]
    widths = part_widths(width)
    vmem = pl.BlockSpec(memory_space=pltpu.VMEM)
    hbm = pl.BlockSpec(memory_space=pl.ANY)
    dma = pltpu.SemaphoreType.DMA
    blocks = RING * RING
    note = blocks * MOST
    plane = blocks * count
    shapes = (
        (RING * RING, count),
        (2 * RING, note),
        (2 * RING, note),
        (2 * RING, note),
        (2 * RING, note),
        (RING * RING, count),
        (RING * RING, count),
        (RING, count),
        (RING, count),
    )
    shapes = [pltpu.VMEM(shape + (w,), BF16) for shape in shapes for w in widths]
    sizes = [8, len(vmems), 3 * RING, 3, 3]
    later = [SLICES * size for size in (3, 1, 1, 1, 1, 1)]
    return pl.pallas_call(
        functools.partial(layer_kernel, widths, len(vmems)),
        out_shape=[
            jax.ShapeDtypeStruct((count, width), BF16),
            jax.ShapeDtypeStruct((3, count * heads, 2 * HEAD), F32),
            jax.ShapeDtypeStruct((2, count * heads, 2 * HEAD), BF16),
        ],
        in_specs=[hbm] * (len(vmems) + len(hbms)),
        out_specs=[vmem, hbm, hbm],
        scratch_shapes=[
            pltpu.VMEM((3, 2, rows, half), BF16),
            pltpu.VMEM((3, 2 * RING * RING, rows, half), BF16),
            pltpu.VMEM((3, RING, count, depth), BF16),
            pltpu.VMEM((3, 2 * RING, count, depth), BF16),
            pltpu.VMEM((3, 2 * RING, count, half), BF16),
            pltpu.VMEM((3, 2 * RING, count, half), BF16),
            pltpu.VMEM((6, count, heads, HEAD), F32),
            pltpu.VMEM(state.shape, F32),
            pltpu.VMEM(hbms[4].shape, BF16),
        ]
        + [pltpu.VMEM(m.shape[-2:], BF16) for m in matrices]
        + [
            pltpu.VMEM((entries, HEAD), BF16),
            pltpu.VMEM((count, width), BF16),
            pltpu.VMEM((3, 2 * RING * note, plane), BF16),
            pltpu.VMEM((3, plane, 2 * RING * note), BF16),
        ]
        + [pltpu.VMEM(small.shape, small.dtype) for small in vmems]
        + shapes
        + [dma]
        + [dma((size,)) for size in sizes]
        + [dma] * 4
        + [dma((size,)) for size in later]
        + [
            pltpu.VMEM((3, count * heads, 2 * HEAD), F32),
            pltpu.VMEM((2, count * heads, 2 * HEAD), BF16),
            dma((2,)),
        ],
        compiler_params=pltpu.CompilerParams(
            collective_id=0, has_side_effects=True, vmem_limit_bytes=VMEM_BYTES
        ),
        name="layer",
    )(*vmems, *hbms)


def finish_kernel(wide, low, state, ready, new_state, new_tokens, spread):
    per_step, heads, entries = state.shape
    tall = per_step * heads
    span = 2 * HEAD

    @pl.when(pl.program_id(0) == 0)
    def _():
        row = lax.broadcasted_iota(jnp.int32, (span, entries), 0)
        col = lax.broadcasted_iota(jnp.int32, (span, entries), 1)
        spread[...] = onehot(col // HEAD == row % HEAD)
        new_tokens[...] = ready[...]

    decay, learned, keys = [wide[w] for w in range(3)]
    removed = dot(low[0], spread[...])
    values = dot(low[1], spread[...])
    for lane in range(0, entries, span):
        cut = slice(lane, lane + span)
        fresh = (
            state[:, :, cut].reshape(tall, span) * decay
            - removed[:, cut] * learned
            + values[:, cut] * keys
        )
        new_state[:, :, cut] = fresh.reshape(per_step, heads, span)


def finish(wide, low, state, ready):
    count, heads, entries = state.shape
    per_step = 8 if count % 8 == 0 else 1
    tall = per_step * heads
    span = 2 * HEAD
    block = pl.BlockSpec((per_step, heads, entries), lambda i: (i, 0, 0))
    flat = pl.BlockSpec(ready.shape, lambda i: (0, 0))
    return pl.pallas_call(
        finish_kernel,
        grid=(count // per_step,),
        out_shape=[
            jax.ShapeDtypeStruct(state.shape, F32),
            jax.ShapeDtypeStruct(ready.shape, BF16),
        ],
        in_specs=[
            pl.BlockSpec((3, tall, span), lambda i: (0, i, 0)),
            pl.BlockSpec((2, tall, span), lambda i: (0, i, 0)),
            block,
            flat,
        ],
        out_specs=[block, flat],
        scratch_shapes=[pltpu.VMEM((span, entries), BF16)],
        compiler_params=pltpu.CompilerParams(
            dimension_semantics=("arbitrary",), vmem_limit_bytes=VMEM_BYTES
        ),
        name="finish",
    )(wide, low, state, ready)


def per_device(
    tokens,
    recurrent_state,
    first_gain,
    w_receptance,
    w_key,
    w_value,
    decay_down,
    decay_up,
    decay_base,
    rate_down,
    rate_up,
    rate_base,
    key_scale,
    head_gain,
    w_output,
    second_gain,
    shared_gate,
    shared_up,
    shared_down,
    expert_gate,
    expert_up,
    expert_down,
    routes,
    route_weights,
):
    vmems = (
        tokens,
        first_gain[None, :],
        decay_down.T,
        decay_up,
        decay_base[None, :],
        rate_down.T,
        rate_up,
        rate_base[None, :],
        key_scale[None, :],
        head_gain[None, :],
        second_gain[None, :],
        routes.T,
        route_weights.T,
    )
    hbms = (
        w_receptance,
        w_key,
        w_value,
        recurrent_state,
        w_output,
        shared_gate,
        shared_up,
        shared_down,
        expert_gate,
        expert_up,
        expert_down,
    )
    ready, wide, low = layer(vmems, hbms)
    new_state, new_tokens = finish(wide, low, recurrent_state, ready)
    return (new_tokens, new_state)


def solution(mesh):
    in_specs = (
        P("ep", None),
        P("ep", None, None),
        P(),
        P("ep", None),
        P("ep", None),
        P("ep", None),
        P(),
        P(),
        P(),
        P(),
        P(),
        P(),
        P(),
        P(),
        P(),
        P(),
        P(),
        P(),
        P(),
        P("ep", None, None),
        P("ep", None, None),
        P("ep", None, None),
        P(),
        P(),
    )
    out_specs = (P("ep", None), P("ep", None, None))
    return jax.shard_map(
        per_device, mesh=mesh, in_specs=in_specs, out_specs=out_specs, check_vma=False
    )
```
